32 devices in a mesh: sp: 8 (over z, x), tp: 4 (over y, core).
Axes of the slice: x: 2, y: 2, z: 4, core: 2. Of those that a mesh axis runs over, the one named last changes fastest.
Arguments:
- q_first: bfloat16 [1536, 512], P('sp', 'tp'), may hold values from -6 to 6
- k_first: bfloat16 [1536, 512], P('sp', 'tp'), may hold values from -6 to 6
- q_second: bfloat16 [1536, 512], P('sp', 'tp'), may hold values from -6 to 6
- k_second: bfloat16 [1536, 512], P('sp', 'tp'), may hold values from -6 to 6
- values: bfloat16 [1536, 1024], P('sp', 'tp'), may hold values from -6 to 6
- lambdas: float32 [8], P('tp'), may hold values from 0.3 to 0.8
- head_gain: float32 [128], replicated, may hold values from 0.1 to 1.9
- out_weight: bfloat16 [1024, 2048], P('tp'), may hold values from -0.1875 to 0.1875
- residual_in: bfloat16 [1536, 2048], P('sp'), may hold values from -6 to 6
- mix_gain: float32 [2048], replicated, may hold values from 0.1 to 1.9
- gate_weight: bfloat16 [2048, 5632], P('sp', 'tp'), may hold values from -0.125 to 0.125
- up_weight: bfloat16 [2048, 5632], P('sp', 'tp'), may hold values from -0.125 to 0.125
- gate_taps: float32 [3, 5632], P(None, 'tp'), may hold values from -3.5 to 3.5
- up_taps: float32 [3, 5632], P(None, 'tp'), may hold values from -3.5 to 3.5
- down_weight: bfloat16 [5632, 2048], P('tp'), may hold values from -0.078125 to 0.078125
Outputs:
- mixed: bfloat16 [1536, 2048], P(('sp', 'tp'))
The draws below stay inside these ranges and needn't reach their ends.
All inputs are finite; a program needn't handle non-finite values.
Results may differ from the reference program's by a relative error of at most 0.017.
Values may be sent and summed in bfloat16 or wider, within the bound.
A program may use at most 128 MiB of HBM per device.

```python
import math
import jax
import jax.numpy as jnp
from jax import lax

D = 2048
HEADS = 8
HEAD_DIM = 64
VALUE_DIM = 128
FF = 5632
KERNEL = 3
TOKENS = 1536


def aligned_pair(key):
    shape = (TOKENS, HEADS * HEAD_DIM)
    query_key = jax.random.fold_in(key, 71)
    other_key = jax.random.fold_in(key, 72)
    queries = jnp.clip(1.35 * jax.random.normal(query_key, shape, jnp.float32), -6.0, 6.0)
    keys = jnp.clip(1.35 * jax.random.normal(other_key, shape, jnp.float32), -6.0, 6.0)
    return (queries.astype(jnp.bfloat16), keys.astype(jnp.bfloat16))


def draw_q_first(key, part):
    return aligned_pair(key)[0]


def draw_k_first(key, part):
    return aligned_pair(key)[1]


def shard_levels(own_key, extent, pieces, low, top_value):
    loudness = 1.0
    for position, shards_of in pieces:
        heights = jax.random.uniform(jax.random.fold_in(jax.random.fold_in(own_key, 6), position), (shards_of,), jnp.float32, low / len(pieces), top_value / len(pieces))
        loudness = loudness * jnp.repeat(jnp.exp(heights), extent[position] // shards_of).reshape((-1,) + (1,) * (len(extent) - 1 - position))
    return loudness


def normal_values(key, dims, spread, limit, split=(), kind=jnp.bfloat16):
    entries = spread * jax.random.normal(key, dims, jnp.float32)
    if split:
        entries = entries * shard_levels(key, dims, split, -0.22, 0.18)
    return jnp.clip(entries, -limit, limit).astype(kind)


def setup_inputs(seed: int = 0) -> dict:
    arg_keys = jax.random.split(jax.random.key(seed), 16)
    return {
        "q_first": draw_q_first(jax.random.fold_in(arg_keys[15], 71), 0),
        "k_first": draw_k_first(jax.random.fold_in(arg_keys[15], 71), 0),
        "q_second": normal_values(arg_keys[2], (TOKENS, HEADS * HEAD_DIM), 1.35, 6.0, ((0, 8), (1, 4))),
        "k_second": normal_values(arg_keys[3], (TOKENS, HEADS * HEAD_DIM), 1.35, 6.0, ((0, 8), (1, 4))),
        "values": normal_values(arg_keys[4], (TOKENS, HEADS * VALUE_DIM), 1.0, 6.0, ((0, 8), (1, 4))),
        "lambdas": jnp.clip(0.3 + 0.5 * jax.random.uniform(arg_keys[5], (HEADS,), jnp.float32) ** shard_levels(arg_keys[5], (HEADS,), ((0, 4),), -0.2, 0.2), 0.3, 0.8),
        "head_gain": jnp.clip(1.0 + 0.18 * jax.random.normal(arg_keys[6], (VALUE_DIM,), jnp.float32), 0.1, 1.9),
        "out_weight": normal_values(arg_keys[7], (HEADS * VALUE_DIM, D), (HEADS * VALUE_DIM) ** -0.5, 0.1875, ((0, 4),)),
        "residual_in": normal_values(arg_keys[8], (TOKENS, D), 1.0, 6.0, ((0, 8),)),
        "mix_gain": jnp.clip(1.0 + 0.18 * jax.random.normal(arg_keys[9], (D,), jnp.float32), 0.1, 1.9),
        "gate_weight": normal_values(arg_keys[10], (D, FF), D ** -0.5, 0.125, ((0, 8), (1, 4))),
        "up_weight": normal_values(arg_keys[11], (D, FF), D ** -0.5, 0.125, ((0, 8), (1, 4))),
        "gate_taps": normal_values(arg_keys[12], (KERNEL, FF), KERNEL ** -0.5, 3.5, ((1, 4),), jnp.float32),
        "up_taps": normal_values(arg_keys[13], (KERNEL, FF), KERNEL ** -0.5, 3.5, ((1, 4),), jnp.float32),
        "down_weight": normal_values(arg_keys[14], (FF, D), FF ** -0.5, 0.078125, ((0, 4),)),
    }


norm_eps = 1e-06
far_below = -1e+30

def reference(q_first, k_first, q_second, k_second, values, lambdas, head_gain, out_weight, residual_in, mix_gain, gate_weight, up_weight, gate_taps, up_taps, down_weight):
    total = q_first.shape[0]
    scale = HEAD_DIM ** (-0.5)
    query_a = q_first.astype(jnp.float32).reshape(total, HEADS, HEAD_DIM)
    query_b = q_second.astype(jnp.float32).reshape(total, HEADS, HEAD_DIM)
    keys_a = k_first.astype(jnp.float32).reshape(total, HEADS, HEAD_DIM)
    keys_b = k_second.astype(jnp.float32).reshape(total, HEADS, HEAD_DIM)
    vals = values.astype(jnp.float32).reshape(total, HEADS, VALUE_DIM)
    block_rows = math.gcd(total, 512)
    key_pos = jnp.arange(total, dtype=jnp.int32)

    def weigh(queries, keys, visible):
        scores = jnp.einsum('qhd,khd->hqk', queries, keys, precision=lax.Precision.HIGHEST) * scale
        masked = jnp.where(visible, scores, far_below)
        peak = lax.optimization_barrier(jnp.max(masked, axis=-1, keepdims=True))
        expo = jnp.where(visible, jnp.exp(masked - peak), 0.0)
        totals = lax.optimization_barrier(jnp.sum(expo, axis=-1))
        rounded = expo.astype(jnp.bfloat16).astype(jnp.float32)
        accum = jnp.einsum('hqk,khv->qhv', rounded, vals, precision=lax.Precision.HIGHEST)
        return accum / totals.T[..., None]

    def attend(block_index):
        row_start = (block_index * block_rows).astype(jnp.int32)
        query_pos = row_start + jnp.arange(block_rows, dtype=jnp.int32)
        visible = (key_pos[None, :] <= query_pos[:, None])[None]
        first = weigh(lax.dynamic_slice_in_dim(query_a, row_start, block_rows, 0), keys_a, visible)
        second = weigh(lax.dynamic_slice_in_dim(query_b, row_start, block_rows, 0), keys_b, visible)
        diff_heads = first - lambdas[None, :, None] * second
        normed = diff_heads * lax.rsqrt(lax.optimization_barrier(jnp.mean(diff_heads * diff_heads, axis=-1, keepdims=True)) + norm_eps) * head_gain
        return normed.astype(jnp.bfloat16).reshape(block_rows, HEADS * VALUE_DIM)
    head_out = lax.map(attend, jnp.arange(total // block_rows, dtype=jnp.int32)).reshape(total, HEADS * VALUE_DIM)
    attended = jnp.dot(head_out, out_weight, preferred_element_type=jnp.float32)
    stream = residual_in.astype(jnp.float32) + attended
    ffn_in = (stream * lax.rsqrt(lax.optimization_barrier(jnp.mean(stream * stream, axis=-1, keepdims=True)) + norm_eps) * mix_gain).astype(jnp.bfloat16)
    gate_pre = jnp.dot(ffn_in, gate_weight, preferred_element_type=jnp.float32).astype(jnp.bfloat16)
    up_pre = jnp.dot(ffn_in, up_weight, preferred_element_type=jnp.float32).astype(jnp.bfloat16)

    def convolve(projected, taps):
        padded = jnp.pad(projected.astype(jnp.float32), ((KERNEL - 1, 0), (0, 0)))
        result = taps[0][None, :] * padded[0:total]
        for offset in range(1, KERNEL):
            result = result + taps[offset][None, :] * padded[offset:offset + total]
        return result
    gate_conv = convolve(gate_pre, gate_taps)
    up_conv = convolve(up_pre, up_taps)
    hidden = (jax.nn.silu(gate_conv) * up_conv).astype(jnp.bfloat16)
    return (stream + jnp.dot(hidden, down_weight, preferred_element_type=jnp.float32)).astype(jnp.bfloat16)
```

```python
import functools

import jax
import jax.numpy as jnp
from jax import lax
from jax.experimental import pallas as pl
from jax.experimental.pallas import tpu as pltpu
from jax.sharding import PartitionSpec as P

norm_eps = 1e-06
far_below = -1e30
halo = 16
lanes = 2
f32 = jnp.float32
bf16 = jnp.bfloat16


def rms_scale(field, gain):
    return field * lax.rsqrt(jnp.mean(field * field, axis=-1, keepdims=True) + norm_eps) * gain


def layer(
    sp_count,
    tp_count,
    team,
    q_a,
    k_a,
    q_b,
    k_b,
    vals,
    lambdas,
    head_gain,
    out_weight,
    residual,
    mix_gain,
    gate_weight,
    up_weight,
    gate_taps,
    up_taps,
    down_weight,
    out,
    kv,
    w_own,
    w,
    down,
    out_w,
    res,
    heads,
    part_out,
    part_in,
    stream,
    ffn,
    acc,
    hidden,
    pair_out,
    pair_in,
    y_out,
    y_in,
    z_out,
    z_in,
    local,
    kvz_send,
    kvz_recv,
    kvx_send,
    kvx_recv,
    wz_send,
    wz_recv,
    wx_send,
    wx_recv,
    rs_send,
    rs_recv,
    ag_send,
    ag_recv,
    halo_send,
    halo_recv,
    pair_send,
    pair_recv,
    y_send,
    y_recv,
    z_send,
    z_recv,
    team_send,
    team_recv,
):
    s = lax.axis_index("sp")
    t = lax.axis_index("tp")
    x = lax.rem(s, lanes)
    z = s // lanes
    lines = sp_count // lanes
    mate = z * lanes + (1 - x)
    rows = q_a.shape[0]
    key_width = q_a.shape[1]
    value_width = vals.shape[1]
    head_count = lambdas.shape[0]
    head_dim = key_width // head_count
    value_dim = value_width // head_count
    part = rows // tp_count
    width = out.shape[1]
    w_rows = gate_weight.shape[0]
    ff = gate_weight.shape[1]
    taps = gate_taps.shape[0]
    piece = w.shape[2]
    fresh = ff - (team - 1) * piece
    g = lax.rem(z, team)
    base = z - g
    slot_rows = halo + rows

    def member(slot):
        return (base + slot) * lanes + x

    def columns(line):
        return pl.multiple_of(jnp.minimum(lax.rem(line, team) * piece, ff - piece), 128)

    def by_width(line, act):
        if fresh == piece:
            act(0)
        else:
            last = lax.rem(line, team) == team - 1

            @pl.when(last)
            def _():
                act(piece - fresh)

            @pl.when(jnp.logical_not(last))
            def _():
                act(0)

    def remote(src, dst, send, recv, sp, tp):
        return pltpu.make_async_remote_copy(
            src_ref=src,
            dst_ref=dst,
            send_sem=send,
            recv_sem=recv,
            device_id=(sp, tp),
            device_id_type=pl.DeviceIdType.MESH,
        )

    def kv_block(block):
        return kv.at[pl.ds(pl.multiple_of(block * rows, 16), rows)]

    def w_block(c, block, skip=0):
        at = pl.ds(pl.multiple_of(block * w_rows, 16), w_rows)
        return w.at[c, at, pl.ds(skip, piece - skip)]

    own = pl.ds(pl.multiple_of(s * rows, 16), rows)
    kv_loads = (
        pltpu.make_async_copy(k_a, kv.at[own, pl.ds(0, key_width)], local.at[0]),
        pltpu.make_async_copy(k_b, kv.at[own, pl.ds(key_width, key_width)], local.at[1]),
        pltpu.make_async_copy(vals, kv.at[own, pl.ds(2 * key_width, value_width)], local.at[2]),
    )
    w_loads = (
        pltpu.make_async_copy(gate_weight, w_own.at[0], local.at[3]),
        pltpu.make_async_copy(up_weight, w_own.at[1], local.at[4]),
        pltpu.make_async_copy(gate_weight.at[:, pl.ds(columns(z), piece)], w_block(0, s), local.at[8]),
        pltpu.make_async_copy(up_weight.at[:, pl.ds(columns(z), piece)], w_block(1, s), local.at[9]),
    )
    out_load = pltpu.make_async_copy(out_weight, out_w, local.at[5])
    res_load = pltpu.make_async_copy(
        residual.at[pl.ds(pl.multiple_of(t * part, 16), part)], res, local.at[6]
    )
    down_load = pltpu.make_async_copy(down_weight.at[pl.ds(columns(z), piece)], down, local.at[7])
    for load in kv_loads + w_loads + (out_load, res_load, down_load):
        load.start()

    barrier = pltpu.get_barrier_semaphore()

    @pl.loop(1, sp_count)
    def _(i):
        pl.semaphore_signal(
            barrier,
            inc=1,
            device_id=(lax.rem(s + i, sp_count), t),
            device_id_type=pl.DeviceIdType.MESH,
        )

    @pl.loop(1, tp_count)
    def _(i):
        pl.semaphore_signal(
            barrier,
            inc=1,
            device_id=(s, lax.rem(t + i, tp_count)),
            device_id_type=pl.DeviceIdType.MESH,
        )

    @pl.loop(1, team)
    def _(j):
        @pl.loop(1, tp_count)
        def _(i):
            pl.semaphore_signal(
                barrier,
                inc=1,
                device_id=(member(lax.rem(g + j, team)), lax.rem(t + i, tp_count)),
                device_id_type=pl.DeviceIdType.MESH,
            )

    pl.semaphore_wait(barrier, sp_count - 1 + team * (tp_count - 1))

    def kvz(line, to, index):
        block = kv_block(line * lanes + x)
        return remote(block, block, kvz_send.at[index], kvz_recv.at[line], to * lanes + x, t)

    def kvx(line, lane):
        block = kv_block(line * lanes + lane)
        return remote(block, block, kvx_send.at[line], kvx_recv.at[line], mate, t)

    def wz(c, line, to, index, skip):
        block = w_block(c, line * lanes + x, skip)
        at = pl.ds(pl.multiple_of(columns(to) + skip, 128), piece - skip)
        return remote(
            w_own.at[c, :, at], block, wz_send.at[c, index], wz_recv.at[c, line], to * lanes + x, t
        )

    def wx(c, line, lane, skip):
        block = w_block(c, line * lanes + lane, skip)
        return remote(block, block, wx_send.at[c, line], wx_recv.at[c, line], mate, t)

    for load in kv_loads:
        load.wait()

    @pl.loop(0, lines - 1 - z)
    def _(i):
        to = lines - 1 - i
        kvz(z, to, to).start()

    kvx(z, x).start()
    for load in w_loads:
        load.wait()

    def near(distance, act):
        for line, there in ((z + distance, z + distance < lines), (z - distance, z >= distance)):

            @pl.when(there)
            def _():
                act(line)

    def send_weights(to):
        def act(skip):
            for c in range(2):
                wz(c, z, to, to, skip).start()

        by_width(to, act)

    @pl.loop(1, lines)
    def _(distance):
        near(distance, send_weights)

    scale = head_dim**-0.5
    column = lax.broadcasted_iota(jnp.int32, (rows, key_width), 1) // head_dim
    queries = [
        jnp.where(column == h, q[...], jnp.zeros((), bf16))
        for q in (q_a, q_b)
        for h in range(head_count)
    ]
    span = lanes * rows
    query_pos = s * rows + lax.broadcasted_iota(jnp.int32, (rows, span), 0)
    key_step = lax.broadcasted_iota(jnp.int32, (rows, span), 1)

    def attend(i, state):
        line = z - i

        @pl.when(i < z)
        def _():
            kvz(line - 1, mate // lanes, line - 1).wait_recv()
            kvx(line - 1, x).start()

        @pl.when(i == jnp.maximum(z - 1, 0))
        def _():
            def act(skip):
                for c in range(2):
                    wx(c, z, x, skip).start()

            by_width(z, act)

        kvx(line, 1 - x).wait_recv()
        keys_at = pl.ds(pl.multiple_of(line * span, 16), span)
        visible = line * span + key_step <= query_pos
        following = []
        for m in range(2):
            keys = kv[keys_at, pl.ds(m * key_width, key_width)]
            for h in range(head_count):
                peak, total, sums = state[m * head_count + h]
                value = kv[keys_at, pl.ds(2 * key_width + h * value_dim, value_dim)]
                scores = (
                    lax.dot_general(
                        queries[m * head_count + h],
                        keys,
                        (((1,), (1,)), ((), ())),
                        preferred_element_type=f32,
                    )
                    * scale
                )
                scores = jnp.where(visible, scores, far_below)
                new_peak = jnp.maximum(peak, jnp.max(scores, axis=-1, keepdims=True))
                fade = jnp.exp(peak - new_peak)
                expo = jnp.exp(scores - new_peak)
                total = total * fade + jnp.sum(expo, axis=-1, keepdims=True)
                sums = sums * fade + jnp.dot(expo.astype(bf16), value, preferred_element_type=f32)
                following.append((new_peak, total, sums))
        return tuple(following)

    start = tuple(
        (
            jnp.full((rows, 1), far_below, f32),
            jnp.zeros((rows, 1), f32),
            jnp.zeros((rows, value_dim), f32),
        )
        for _ in range(2 * head_count)
    )
    state = lax.fori_loop(0, z + 1, attend, start)
    for h in range(head_count):
        _, total_a, sums_a = state[h]
        _, total_b, sums_b = state[head_count + h]
        diff = sums_a / total_a - lambdas[h] * (sums_b / total_b)
        heads[:, h * value_dim : (h + 1) * value_dim] = rms_scale(diff, head_gain[...]).astype(bf16)

    def forward(line):
        def act(skip):
            for c in range(2):
                wz(c, line, mate // lanes, line, skip).wait_recv()
                wx(c, line, x, skip).start()

        by_width(z, act)

    early = min(3, lines - 1)
    if early > 0:
        near(1, forward)

    out_load.wait()
    res_load.wait()
    stream[...] = res[...].astype(f32)

    def part_copy(i):
        to = lax.rem(t + i, tp_count)
        return remote(part_out.at[to], part_in.at[t], rs_send.at[to], rs_recv.at[t], s, to)

    for i in range(1, tp_count + 1):
        to = lax.rem(t + i, tp_count)
        product = jnp.dot(
            heads[pl.ds(pl.multiple_of(to * part, 16), part), :],
            out_w[...],
            preferred_element_type=f32,
        )
        if i < tp_count:
            part_out[to] = product.astype(bf16)
            part_copy(i).start()
        else:
            stream[...] += product
    for i in range(1, tp_count):
        source = lax.rem(t + i, tp_count)
        remote(
            part_out.at[source], part_in.at[source], rs_send.at[source], rs_recv.at[source], s, source
        ).wait_recv()
        stream[...] += part_in[source].astype(f32)

    def ffn_rows(slot, rank):
        return pl.ds(pl.multiple_of(slot * slot_rows + halo + rank * part, 16), part)

    ffn[ffn_rows(g, t), :] = rms_scale(stream[...], mix_gain[...]).astype(bf16)

    def team_copy(slot, to):
        rows_here = ffn.at[ffn_rows(slot, t)]
        return remote(rows_here, rows_here, team_send.at[to], team_recv.at[slot], member(to), t)

    def gather_copy(i, slot, rank):
        to = lax.rem(t + i, tp_count)
        rows_here = ffn.at[ffn_rows(slot, rank)]
        return remote(rows_here, rows_here, ag_send.at[slot, to], ag_recv.at[slot, rank], s, to)

    for i in range(1, team):
        team_copy(g, lax.rem(g + i, team)).start()
    for i in range(1, tp_count):
        gather_copy(i, g, t).start()
    if early > 1:
        near(2, forward)
    for i in range(1, tp_count):
        gather_copy(i, g, lax.rem(t + i, tp_count)).wait_recv()

    after = lax.rem(s + 1, sp_count)
    after_line = after // lanes
    after_slot = lax.rem(after_line, team)
    after_base = after_line - after_slot

    def halo_copy(which, slot):
        return remote(
            ffn.at[pl.ds(pl.multiple_of(g * slot_rows + rows, 16), halo)],
            ffn.at[pl.ds(pl.multiple_of(slot * slot_rows, 16), halo)],
            halo_send.at[which],
            halo_recv.at[slot],
            (after_base + which) * lanes + lax.rem(after, lanes),
            t,
        )

    @pl.when(s < sp_count - 1)
    def _():
        for which in range(team):
            halo_copy(which, after_slot).start()

    for slot in range(team):
        if slot == team - 1 and early > 2:
            near(3, forward)

        @pl.when(slot != g)
        def _():
            team_copy(slot, g).wait_recv()
            for i in range(1, tp_count):
                gather_copy(i, slot, t).start()

    @pl.loop(early + 1, lines)
    def _(distance):
        near(distance, forward)

    @pl.loop(0, lines)
    def _(line):
        def act(skip):
            for c in range(2):
                wx(c, line, 1 - x, skip).wait_recv()

        by_width(z, act)

    down_load.wait()
    pairs = tp_count // 2
    c_own = lax.rem(t, 2)
    k_own = t // 2
    chunk = 512 if width % 512 == 0 else width

    def slot_of(n):
        return lax.rem(g + 1 + n, team)

    def part_rows(k):
        return pl.ds(pl.multiple_of(k * part, 16), part)

    def pair_copy(n):
        return remote(
            pair_out.at[n, 1 - c_own],
            pair_in.at[n],
            pair_send.at[n],
            pair_recv.at[n],
            s,
            t + 1 - 2 * c_own,
        )

    def y_copy(n, k, source):
        return remote(
            y_out.at[n, k],
            y_in.at[n, source],
            y_send.at[n, k],
            y_recv.at[n, source],
            s,
            2 * k + c_own,
        )

    def z_copy(n, source):
        return remote(
            z_out.at[n], z_in.at[source], z_send.at[n], z_recv.at[source], member(slot_of(n)), t
        )

    def compute(n):
        slot = slot_of(n)

        @pl.when(slot != g)
        def _():
            for i in range(1, tp_count):
                gather_copy(i, slot, lax.rem(t + i, tp_count)).wait_recv()

        block = member(slot)
        halo_rows = pl.ds(pl.multiple_of(slot * slot_rows, 16), halo)

        @pl.when(block == 0)
        def _():
            ffn[halo_rows, :] = jnp.zeros((halo, width), bf16)

        @pl.when(block > 0)
        def _():
            halo_copy(0, slot).wait_recv()

        rows_at = pl.ds(pl.multiple_of(slot * slot_rows, 16), slot_rows)
        for c in range(2):
            acc[c] = jnp.dot(ffn[rows_at, :], w[c], preferred_element_type=f32)
        for i in range(piece // 128):
            at = slice(i * 128, (i + 1) * 128)
            tap_at = pl.ds(pl.multiple_of(columns(z) + i * 128, 128), 128)
            made = []
            for c, tap in enumerate((gate_taps, up_taps)):
                total = None
                for k in range(taps):
                    first = halo - taps + 1 + k
                    row = acc[c, first : first + rows, at].astype(bf16).astype(f32)
                    term = tap[pl.ds(k, 1), tap_at] * row
                    total = term if total is None else total + term
                made.append(total)
            value = made[0] / (1 + jnp.exp(-made[0])) * made[1]
            if (i + 1) * 128 <= piece - fresh:
                value = jnp.where(g < team - 1, value, 0.0)
            hidden[:, at] = value.astype(bf16)
        for i in range(width // chunk):
            at = slice(i * chunk, (i + 1) * chunk)
            product = jnp.dot(hidden[...], down[:, at], preferred_element_type=f32).astype(bf16)
            for r in range(tp_count):
                first = (r // 2) * part
                pair_out[n, r % 2, first : first + part, at] = product[r * part : (r + 1) * part]
        pair_copy(n).start()

    def pair_sum(n, k):
        mine = pair_out[n, c_own, part_rows(k), :].astype(f32)
        return mine + pair_in[n, part_rows(k), :].astype(f32)

    def across(n):
        pair_copy(n).wait_recv()
        for i in range(1, pairs):
            k = lax.rem(k_own + i, pairs)
            y_out[n, k] = pair_sum(n, k).astype(bf16)
            y_copy(n, k, k_own).start()

    def along(n):
        total = pair_sum(n, k_own)
        for i in range(1, pairs):
            k = lax.rem(k_own + i, pairs)
            y_copy(n, k, k).wait_recv()
            total = total + y_in[n, k].astype(f32)
        if n < team - 1:
            z_out[n] = total.astype(bf16)
            z_copy(n, g).start()
        else:
            stream[...] += total

    for n in range(team + 2):
        if n < team:
            compute(n)
        if 0 < n <= team:
            across(n - 1)
        if n > 1:
            along(n - 2)
    for n in range(team - 1):
        source = slot_of(n)
        z_copy(n, source).wait_recv()
        stream[...] += z_in[source].astype(f32)
    out[...] = stream[...].astype(bf16)

    @pl.loop(z + 1, lines)
    def _(to):
        kvz(z, to, to).wait_send()

    @pl.loop(0, z + 1)
    def _(line):
        kvx(line, x).wait_send()

    @pl.loop(1, lines)
    def _(i):
        to = lax.rem(z + i, lines)

        def act(skip):
            for c in range(2):
                wz(c, z, to, to, skip).wait_send()

        by_width(to, act)

    @pl.loop(0, lines)
    def _(line):
        def act(skip):
            for c in range(2):
                wx(c, line, x, skip).wait_send()

        by_width(z, act)

    for i in range(1, team):
        team_copy(g, lax.rem(g + i, team)).wait_send()
    for i in range(1, tp_count):
        part_copy(i).wait_send()
        for slot in range(team):
            gather_copy(i, slot, t).wait_send()
    for n in range(team):
        pair_copy(n).wait_send()
        for i in range(1, pairs):
            y_copy(n, lax.rem(k_own + i, pairs), k_own).wait_send()
        if n < team - 1:
            z_copy(n, g).wait_send()

    @pl.when(s < sp_count - 1)
    def _():
        for which in range(team):
            halo_copy(which, after_slot).wait_send()


def shards(sp_count, tp_count, *args):
    (q_a, _, _, _, vals, lambdas, head_gain, out_weight, residual, mix_gain, gate, _, _, _, down) = args
    rows = q_a.shape[0]
    width = residual.shape[1]
    w_rows, ff = gate.shape
    part = rows // tp_count
    lines = sp_count // lanes
    team = next(n for n in (4, 2, 1) if lines % n == 0)
    pairs = tp_count // 2
    piece = -(-ff // (team * 128)) * 128
    args = list(args)
    args[6] = head_gain.reshape(1, -1)
    args[9] = mix_gain.reshape(1, -1)
    vmem = pl.BlockSpec(memory_space=pltpu.VMEM)
    hbm = pl.BlockSpec(memory_space=pl.ANY)
    smem = pl.BlockSpec(memory_space=pltpu.SMEM)
    dma = pltpu.SemaphoreType.DMA
    in_specs = [vmem, hbm, vmem, hbm, hbm, smem, vmem, hbm, hbm, vmem, hbm, hbm, vmem, vmem, hbm]
    return pl.pallas_call(
        functools.partial(layer, sp_count, tp_count, team),
        out_shape=jax.ShapeDtypeStruct((part, width), bf16),
        in_specs=in_specs,
        out_specs=vmem,
        scratch_shapes=[
            pltpu.VMEM((sp_count * rows, 2 * q_a.shape[1] + vals.shape[1]), bf16),
            pltpu.VMEM((2, w_rows, ff), bf16),
            pltpu.VMEM((2, sp_count * w_rows, piece), bf16),
            pltpu.VMEM((piece, width), bf16),
            pltpu.VMEM(out_weight.shape, bf16),
            pltpu.VMEM((part, width), bf16),
            pltpu.VMEM((rows, vals.shape[1]), bf16),
            pltpu.VMEM((tp_count, part, width), bf16),
            pltpu.VMEM((tp_count, part, width), bf16),
            pltpu.VMEM((part, width), f32),
            pltpu.VMEM((team * (halo + rows), width), bf16),
            pltpu.VMEM((2, halo + rows, piece), f32),
            pltpu.VMEM((rows, piece), bf16),
            pltpu.VMEM((team, 2, pairs * part, width), bf16),
            pltpu.VMEM((team, pairs * part, width), bf16),
            pltpu.VMEM((team, pairs, part, width), bf16),
            pltpu.VMEM((team, pairs, part, width), bf16),
            pltpu.VMEM((team, part, width), bf16),
            pltpu.VMEM((team, part, width), bf16),
            dma((10,)),
            dma((lines,)),
            dma((lines,)),
            dma((lines,)),
            dma((lines,)),
            dma((2, lines)),
            dma((2, lines)),
            dma((2, lines)),
            dma((2, lines)),
            dma((tp_count,)),
            dma((tp_count,)),
            dma((team, tp_count)),
            dma((team, tp_count)),
            dma((team,)),
            dma((team,)),
            dma((team,)),
            dma((team,)),
            dma((team, pairs)),
            dma((team, pairs)),
            dma((team,)),
            dma((team,)),
            dma((team,)),
            dma((team,)),
        ],
        compiler_params=pltpu.CompilerParams(
            collective_id=0, has_side_effects=True, vmem_limit_bytes=60 * 1024 * 1024
        ),
    )(*args)


def solution(mesh):
    in_specs = (
        P("sp", "tp"),
        P("sp", "tp"),
        P("sp", "tp"),
        P("sp", "tp"),
        P("sp", "tp"),
        P("tp"),
        P(),
        P("tp", None),
        P("sp", None),
        P(),
        P("sp", "tp"),
        P("sp", "tp"),
        P(None, "tp"),
        P(None, "tp"),
        P("tp", None),
    )
    body = functools.partial(shards, mesh.shape["sp"], mesh.shape["tp"])
    return jax.shard_map(
        body, mesh=mesh, in_specs=in_specs, out_specs=P(("sp", "tp"), None), check_vma=False
    )
```

```python
import functools

import jax
import jax.numpy as jnp
from jax import lax
from jax.experimental import pallas as pl
from jax.experimental.pallas import tpu as pltpu
from jax.sharding import PartitionSpec as P

norm_eps = 1e-06
far_below = -1e30
halo = 16
lanes = 2
f32 = jnp.float32
bf16 = jnp.bfloat16


def rms_scale(field, gain):
    return field * lax.rsqrt(jnp.mean(field * field, axis=-1, keepdims=True) + norm_eps) * gain


def layer(
    sp_count,
    tp_count,
    team,
    q_a,
    k_a,
    q_b,
    k_b,
    vals,
    lambdas,
    head_gain,
    out_weight,
    residual,
    mix_gain,
    gate_weight,
    up_weight,
    gate_taps,
    up_taps,
    down_weight,
    out,
    kv,
    w_own,
    w,
    down,
    out_w,
    res,
    heads,
    part_out,
    part_in,
    stream,
    ffn,
    acc,
    hidden,
    pair_out,
    pair_in,
    y_out,
    y_in,
    z_out,
    z_in,
    local,
    kvz_send,
    kvz_recv,
    kvx_send,
    kvx_recv,
    relay_send,
    wz_send,
    wz_recv,
    wx_send,
    wx_recv,
    rs_send,
    rs_recv,
    gy_send,
    gy_recv,
    gc_send,
    gc_recv,
    halo_send,
    halo_recv,
    pair_send,
    pair_recv,
    y_send,
    y_recv,
    z_send,
    z_recv,
    team_send,
    team_recv,
    up_send,
):
    s = lax.axis_index("sp")
    t = lax.axis_index("tp")
    x = lax.rem(s, lanes)
    z = s // lanes
    lines = sp_count // lanes
    mate = z * lanes + (1 - x)
    rows = q_a.shape[0]
    key_width = q_a.shape[1]
    value_width = vals.shape[1]
    head_count = lambdas.shape[0]
    head_dim = key_width // head_count
    value_dim = value_width // head_count
    part = rows // tp_count
    width = out.shape[1]
    w_rows = gate_weight.shape[0]
    ff = gate_weight.shape[1]
    taps = gate_taps.shape[0]
    piece = w.shape[2]
    fresh = ff - (team - 1) * piece
    g = lax.rem(z, team)
    base = z - g
    pairs = tp_count // 2
    c_own = lax.rem(t, 2)
    k_own = t // 2
    slot_rows = halo + rows

    def member(slot):
        return (base + slot) * lanes + x

    def columns(line):
        return pl.multiple_of(jnp.minimum(lax.rem(line, team) * piece, ff - piece), 128)

    def by_width(line, act):
        if fresh == piece:
            act(0)
        else:
            last = lax.rem(line, team) == team - 1

            @pl.when(last)
            def _():
                act(piece - fresh)

            @pl.when(jnp.logical_not(last))
            def _():
                act(0)

    def remote(src, dst, send, recv, sp, tp):
        return pltpu.make_async_remote_copy(
            src_ref=src,
            dst_ref=dst,
            send_sem=send,
            recv_sem=recv,
            device_id=(sp, tp),
            device_id_type=pl.DeviceIdType.MESH,
        )

    def kv_block(block):
        return kv.at[pl.ds(pl.multiple_of(block * rows, 16), rows)]

    def w_block(c, block, skip=0):
        at = pl.ds(pl.multiple_of(block * w_rows, 16), w_rows)
        return w.at[c, at, pl.ds(skip, piece - skip)]

    own = pl.ds(pl.multiple_of(s * rows, 16), rows)
    kv_loads = (
        pltpu.make_async_copy(k_a, kv.at[own, pl.ds(0, key_width)], local.at[0]),
        pltpu.make_async_copy(k_b, kv.at[own, pl.ds(key_width, key_width)], local.at[1]),
        pltpu.make_async_copy(vals, kv.at[own, pl.ds(2 * key_width, value_width)], local.at[2]),
    )
    w_loads = (
        pltpu.make_async_copy(gate_weight, w_own.at[0], local.at[3]),
        pltpu.make_async_copy(up_weight, w_own.at[1], local.at[4]),
        pltpu.make_async_copy(gate_weight.at[:, pl.ds(columns(z), piece)], w_block(0, s), local.at[8]),
        pltpu.make_async_copy(up_weight.at[:, pl.ds(columns(z), piece)], w_block(1, s), local.at[9]),
    )
    out_load = pltpu.make_async_copy(out_weight, out_w, local.at[5])
    res_load = pltpu.make_async_copy(
        residual.at[pl.ds(pl.multiple_of(t * part, 16), part)], res, local.at[6]
    )
    down_load = pltpu.make_async_copy(down_weight.at[pl.ds(columns(z), piece)], down, local.at[7])
    for load in kv_loads + w_loads + (out_load, res_load, down_load):
        load.start()

    barrier = pltpu.get_barrier_semaphore()

    @pl.loop(1, sp_count)
    def _(i):
        pl.semaphore_signal(
            barrier,
            inc=1,
            device_id=(lax.rem(s + i, sp_count), t),
            device_id_type=pl.DeviceIdType.MESH,
        )

    @pl.loop(1, tp_count)
    def _(i):
        pl.semaphore_signal(
            barrier,
            inc=1,
            device_id=(s, lax.rem(t + i, tp_count)),
            device_id_type=pl.DeviceIdType.MESH,
        )

    @pl.loop(1, team)
    def _(j):
        @pl.loop(1, tp_count)
        def _(i):
            pl.semaphore_signal(
                barrier,
                inc=1,
                device_id=(member(lax.rem(g + j, team)), lax.rem(t + i, tp_count)),
                device_id_type=pl.DeviceIdType.MESH,
            )

    pl.semaphore_wait(barrier, sp_count - 1 + team * (tp_count - 1))

    def kvz(line, to, index):
        block = kv_block(line * lanes + x)
        return remote(block, block, kvz_send.at[index], kvz_recv.at[line], to * lanes + x, t)

    def kv_relay(line):
        block = kv_block(line * lanes + x)
        return remote(
            block, block, relay_send.at[line], kvz_recv.at[line], (z + 1) * lanes + x, t
        )

    def relays(line):
        direct = (line == z - 1) & (lax.rem(line, 2) == 0)
        return (z + 1 < lines) & jnp.logical_not(direct)

    def kvx(line, lane):
        block = kv_block(line * lanes + lane)
        return remote(block, block, kvx_send.at[line], kvx_recv.at[line], mate, t)

    def wz(c, line, to, index, skip):
        block = w_block(c, line * lanes + x, skip)
        at = pl.ds(pl.multiple_of(columns(to) + skip, 128), piece - skip)
        return remote(
            w_own.at[c, :, at], block, wz_send.at[c, index], wz_recv.at[c, line], to * lanes + x, t
        )

    def wx(c, line, lane, skip):
        block = w_block(c, line * lanes + lane, skip)
        return remote(block, block, wx_send.at[c, line], wx_recv.at[c, line], mate, t)

    for load in kv_loads:
        load.wait()

    @pl.when((lax.rem(z, 2) == 0) & (z + 2 < lines))
    def _():
        kvz(z, z + 2, z + 2).start()

    @pl.when(z + 1 < lines)
    def _():
        kvz(z, z + 1, z + 1).start()

    kvx(z, x).start()
    for load in w_loads:
        load.wait()

    def near(distance, act):
        for line, there in ((z + distance, z + distance < lines), (z - distance, z >= distance)):

            @pl.when(there)
            def _():
                act(line)

    def send_weights(to):
        def act(skip):
            for c in range(2):
                wz(c, z, to, to, skip).start()

        by_width(to, act)

    def deferred(to):
        return (to - z >= 2) & (lax.rem(to, team) == team - 1)

    def send_first(to):
        @pl.when(jnp.logical_not(deferred(to)))
        def _():
            send_weights(to)

    def send_later(to):
        @pl.when(deferred(to))
        def _():
            send_weights(to)

    @pl.loop(1, lines)
    def _(distance):
        near(distance, send_first)

    scale = head_dim**-0.5
    column = lax.broadcasted_iota(jnp.int32, (rows, key_width), 1) // head_dim
    queries = [
        jnp.where(column == h, q[...], jnp.zeros((), bf16))
        for q in (q_a, q_b)
        for h in range(head_count)
    ]
    span = lanes * rows
    query_pos = s * rows + lax.broadcasted_iota(jnp.int32, (rows, span), 0)
    key_step = lax.broadcasted_iota(jnp.int32, (rows, span), 1)

    def attend(i, state):
        line = z - i

        @pl.when(i < z)
        def _():
            kvz(line - 1, mate // lanes, line - 1).wait_recv()
            kvx(line - 1, x).start()

            @pl.when(relays(line - 1))
            def _():
                kv_relay(line - 1).start()


        @pl.when(i == jnp.maximum(z - 1, 0))
        def _():
            def act(skip):
                for c in range(2):
                    wx(c, z, x, skip).start()

            by_width(z, act)

        kvx(line, 1 - x).wait_recv()
        keys_at = pl.ds(pl.multiple_of(line * span, 16), span)
        visible = line * span + key_step <= query_pos
        following = []
        for m in range(2):
            keys = kv[keys_at, pl.ds(m * key_width, key_width)]
            for h in range(head_count):
                peak, total, sums = state[m * head_count + h]
                value = kv[keys_at, pl.ds(2 * key_width + h * value_dim, value_dim)]
                scores = (
                    lax.dot_general(
                        queries[m * head_count + h],
                        keys,
                        (((1,), (1,)), ((), ())),
                        preferred_element_type=f32,
                    )
                    * scale
                )
                scores = jnp.where(visible, scores, far_below)
                new_peak = jnp.maximum(peak, jnp.max(scores, axis=-1, keepdims=True))
                fade = jnp.exp(peak - new_peak)
                expo = jnp.exp(scores - new_peak)
                total = total * fade + jnp.sum(expo, axis=-1, keepdims=True)
                sums = sums * fade + jnp.dot(expo.astype(bf16), value, preferred_element_type=f32)
                following.append((new_peak, total, sums))
        return tuple(following)

    start = tuple(
        (
            jnp.full((rows, 1), far_below, f32),
            jnp.zeros((rows, 1), f32),
            jnp.zeros((rows, value_dim), f32),
        )
        for _ in range(2 * head_count)
    )
    state = lax.fori_loop(0, z + 1, attend, start)
    for h in range(head_count):
        _, total_a, sums_a = state[h]
        _, total_b, sums_b = state[head_count + h]
        diff = sums_a / total_a - lambdas[h] * (sums_b / total_b)
        heads[:, h * value_dim : (h + 1) * value_dim] = rms_scale(diff, head_gain[...]).astype(bf16)

    def forward(line):
        def act(skip):
            for c in range(2):
                wz(c, line, mate // lanes, line, skip).wait_recv()
                wx(c, line, x, skip).start()

        by_width(z, act)

    early = min(3, lines - 1)

    out_load.wait()
    res_load.wait()
    stream[...] = res[...].astype(f32)

    def part_copy(i):
        to = lax.rem(t + i, tp_count)
        return remote(part_out.at[to], part_in.at[t], rs_send.at[to], rs_recv.at[t], s, to)

    for i in range(1, tp_count + 1):
        to = lax.rem(t + i, tp_count)
        product = jnp.dot(
            heads[pl.ds(pl.multiple_of(to * part, 16), part), :],
            out_w[...],
            preferred_element_type=f32,
        )
        if i < tp_count:
            part_out[to] = product.astype(bf16)
            part_copy(i).start()
        else:
            stream[...] += product
    for i in range(1, tp_count):
        source = lax.rem(t + i, tp_count)
        remote(
            part_out.at[source], part_in.at[source], rs_send.at[source], rs_recv.at[source], s, source
        ).wait_recv()
        stream[...] += part_in[source].astype(f32)

    def ffn_rows(slot, rank):
        return pl.ds(pl.multiple_of(slot * slot_rows + halo + rank * part, 16), part)

    ffn[ffn_rows(g, t), :] = rms_scale(stream[...], mix_gain[...]).astype(bf16)

    def team_copy(slot, to):
        rows_here = ffn.at[ffn_rows(slot, t)]
        return remote(rows_here, rows_here, team_send.at[to], team_recv.at[slot], member(to), t)

    def relayed_up(slot, at_slot):
        direct = (slot == at_slot - 1) & (lax.rem(slot, 2) == 0)
        return (slot < at_slot) & (at_slot + 1 < team) & jnp.logical_not(direct)

    def sent_direct(to):
        return (to < g) | (to == g + 1) | ((to == g + 2) & (lax.rem(g, 2) == 0))

    def team_relay(slot):
        rows_here = ffn.at[ffn_rows(slot, t)]
        return remote(
            rows_here, rows_here, up_send.at[slot], team_recv.at[slot], member(g + 1), t
        )

    def y_gather(slot, k, source):
        rows_here = ffn.at[ffn_rows(slot, 2 * source + c_own)]
        return remote(
            rows_here, rows_here, gy_send.at[slot, k], gy_recv.at[slot, source], s, 2 * k + c_own
        )

    def core_gather(slot, k, c):
        rows_here = ffn.at[ffn_rows(slot, 2 * k + c)]
        return remote(
            rows_here, rows_here, gc_send.at[slot, k], gc_recv.at[slot, k], s, t + 1 - 2 * c_own
        )

    def hold(slot):
        for i in range(1, pairs):
            y_gather(slot, lax.rem(k_own + i, pairs), k_own).start()
        core_gather(slot, k_own, c_own).start()

    def halo_copy(slot, to_slot, to):
        return remote(
            ffn.at[pl.ds(pl.multiple_of(slot * slot_rows + rows, 16), halo)],
            ffn.at[pl.ds(pl.multiple_of(to_slot * slot_rows, 16), halo)],
            halo_send.at[slot],
            halo_recv.at[to_slot],
            to,
            t,
        )

    def halos(slot, act):
        @pl.when(x < lanes - 1)
        def _():
            act(halo_copy(slot, slot, mate))

        @pl.when((x == lanes - 1) & (slot < team - 1))
        def _():
            act(halo_copy(slot, slot + 1, mate))

        @pl.when((x == lanes - 1) & (slot == team - 1) & (z + team < lines))
        def _():
            act(halo_copy(slot, 0, (z + team) * lanes))

    def pass_on(slot):
        for i in range(1, pairs):
            k = lax.rem(k_own + i, pairs)
            y_gather(slot, k, k).wait_recv()
            core_gather(slot, k, c_own).start()

    def ready(slot):
        for k in range(pairs):
            core_gather(slot, k, 1 - c_own).wait_recv()
        halos(slot, lambda copy: copy.start())

    @pl.loop(0, team)
    def _(i):
        to = jnp.where(i < g, i, team - 1 - i + g)

        @pl.when(sent_direct(to) & (to != g))
        def _():
            team_copy(g, to).start()

    hold(g)

    @pl.loop(1, lines)
    def _(distance):
        near(distance, send_later)

    if early > 0:
        near(1, forward)
    pass_on(g)
    ready(g)

    def other(slot, act):
        @pl.when(slot != g)
        def _():
            act(slot)

    def take(slot):
        team_copy(slot, g).wait_recv()

        @pl.when(relayed_up(slot, g))
        def _():
            team_relay(slot).start()

        hold(slot)

    def settle(slot):
        pass_on(slot)
        ready(slot)

    for slot in range(team + 1):
        if slot == 2 and early > 1:
            near(2, forward)
        if slot == 3 and early > 2:
            near(3, forward)
        if slot < team:
            other(slot, take)
        if slot > 0:
            other(slot - 1, settle)

    @pl.loop(early + 1, lines)
    def _(distance):
        near(distance, forward)

    @pl.loop(0, lines)
    def _(line):
        def act(skip):
            for c in range(2):
                wx(c, line, 1 - x, skip).wait_recv()

        by_width(z, act)

    down_load.wait()
    chunk = 512 if width % 512 == 0 else width

    def slot_of(n):
        if team > 2 and n < 2:
            n = jnp.where(g == team - 2, 1 - n, n)
        return lax.rem(g + 1 + n, team)

    def part_rows(k):
        return pl.ds(pl.multiple_of(k * part, 16), part)

    def pair_copy(n):
        return remote(
            pair_out.at[n, 1 - c_own],
            pair_in.at[n],
            pair_send.at[n],
            pair_recv.at[n],
            s,
            t + 1 - 2 * c_own,
        )

    def y_copy(n, k, source):
        return remote(
            y_out.at[n, k],
            y_in.at[n, source],
            y_send.at[n, k],
            y_recv.at[n, source],
            s,
            2 * k + c_own,
        )

    def z_copy(n, source):
        return remote(
            z_out.at[n], z_in.at[source], z_send.at[n], z_recv.at[source], member(slot_of(n)), t
        )

    def compute(n):
        slot = slot_of(n)

        block = member(slot)
        halo_rows = pl.ds(pl.multiple_of(slot * slot_rows, 16), halo)

        @pl.when(block == 0)
        def _():
            ffn[halo_rows, :] = jnp.zeros((halo, width), bf16)

        @pl.when(block > 0)
        def _():
            halo_copy(slot, slot, mate).wait_recv()

        rows_at = pl.ds(pl.multiple_of(slot * slot_rows, 16), slot_rows)
        for c in range(2):
            acc[c] = jnp.dot(ffn[rows_at, :], w[c], preferred_element_type=f32)
        for i in range(piece // 128):
            at = slice(i * 128, (i + 1) * 128)
            tap_at = pl.ds(pl.multiple_of(columns(z) + i * 128, 128), 128)
            made = []
            for c, tap in enumerate((gate_taps, up_taps)):
                total = None
                for k in range(taps):
                    first = halo - taps + 1 + k
                    row = acc[c, first : first + rows, at].astype(bf16).astype(f32)
                    term = tap[pl.ds(k, 1), tap_at] * row
                    total = term if total is None else total + term
                made.append(total)
            value = made[0] / (1 + jnp.exp(-made[0])) * made[1]
            if (i + 1) * 128 <= piece - fresh:
                value = jnp.where(g < team - 1, value, 0.0)
            hidden[:, at] = value.astype(bf16)
        for i in range(width // chunk):
            at = slice(i * chunk, (i + 1) * chunk)
            product = jnp.dot(hidden[...], down[:, at], preferred_element_type=f32).astype(bf16)
            for r in range(tp_count):
                first = (r // 2) * part
                pair_out[n, r % 2, first : first + part, at] = product[r * part : (r + 1) * part]
        pair_copy(n).start()

    def pair_sum(n, k):
        mine = pair_out[n, c_own, part_rows(k), :].astype(f32)
        return mine + pair_in[n, part_rows(k), :].astype(f32)

    def across(n):
        pair_copy(n).wait_recv()
        for i in range(1, pairs):
            k = lax.rem(k_own + i, pairs)
            y_out[n, k] = pair_sum(n, k).astype(bf16)
            y_copy(n, k, k_own).start()

    def along(n):
        total = pair_sum(n, k_own)
        for i in range(1, pairs):
            k = lax.rem(k_own + i, pairs)
            y_copy(n, k, k).wait_recv()
            total = total + y_in[n, k].astype(f32)
        if n < team - 1:
            z_out[n] = total.astype(bf16)
            z_copy(n, g).start()
        else:
            stream[...] += total

    for n in range(team + 2):
        if n < team:
            compute(n)
        if 0 < n <= team:
            across(n - 1)
        if n > 1:
            along(n - 2)
    for n in range(team - 1):
        source = slot_of(n)
        z_copy(n, source).wait_recv()
        stream[...] += z_in[source].astype(f32)
    out[...] = stream[...].astype(bf16)

    @pl.when((lax.rem(z, 2) == 0) & (z + 2 < lines))
    def _():
        kvz(z, z + 2, z + 2).wait_send()

    @pl.when(z + 1 < lines)
    def _():
        kvz(z, z + 1, z + 1).wait_send()

    @pl.loop(0, z)
    def _(line):
        @pl.when(relays(line))
        def _():
            kv_relay(line).wait_send()

    @pl.loop(0, z + 1)
    def _(line):
        kvx(line, x).wait_send()

    @pl.loop(1, lines)
    def _(i):
        to = lax.rem(z + i, lines)

        def act(skip):
            for c in range(2):
                wz(c, z, to, to, skip).wait_send()

        by_width(to, act)

    @pl.loop(0, lines)
    def _(line):
        def act(skip):
            for c in range(2):
                wx(c, line, x, skip).wait_send()

        by_width(z, act)

    for i in range(1, tp_count):
        part_copy(i).wait_send()
    for slot in range(team):

        @pl.when(sent_direct(slot) & (slot != g))
        def _():
            team_copy(g, slot).wait_send()

        @pl.when(relayed_up(slot, g))
        def _():
            team_relay(slot).wait_send()

        for i in range(1, pairs):
            y_gather(slot, lax.rem(k_own + i, pairs), k_own).wait_send()
        for k in range(pairs):
            core_gather(slot, k, c_own).wait_send()
        halos(slot, lambda copy: copy.wait_send())
    for n in range(team):
        pair_copy(n).wait_send()
        for i in range(1, pairs):
            y_copy(n, lax.rem(k_own + i, pairs), k_own).wait_send()
        if n < team - 1:
            z_copy(n, g).wait_send()


def shards(sp_count, tp_count, *args):
    (q_a, _, _, _, vals, lambdas, head_gain, out_weight, residual, mix_gain, gate, _, _, _, down) = args
    rows = q_a.shape[0]
    width = residual.shape[1]
    w_rows, ff = gate.shape
    part = rows // tp_count
    lines = sp_count // lanes
    team = next(n for n in (4, 2, 1) if lines % n == 0)
    pairs = tp_count // 2
    piece = -(-ff // (team * 128)) * 128
    args = list(args)
    args[6] = head_gain.reshape(1, -1)
    args[9] = mix_gain.reshape(1, -1)
    vmem = pl.BlockSpec(memory_space=pltpu.VMEM)
    hbm = pl.BlockSpec(memory_space=pl.ANY)
    smem = pl.BlockSpec(memory_space=pltpu.SMEM)
    dma = pltpu.SemaphoreType.DMA
    in_specs = [vmem, hbm, vmem, hbm, hbm, smem, vmem, hbm, hbm, vmem, hbm, hbm, vmem, vmem, hbm]
    return pl.pallas_call(
        functools.partial(layer, sp_count, tp_count, team),
        out_shape=jax.ShapeDtypeStruct((part, width), bf16),
        in_specs=in_specs,
        out_specs=vmem,
        scratch_shapes=[
            pltpu.VMEM((sp_count * rows, 2 * q_a.shape[1] + vals.shape[1]), bf16),
            pltpu.VMEM((2, w_rows, ff), bf16),
            pltpu.VMEM((2, sp_count * w_rows, piece), bf16),
            pltpu.VMEM((piece, width), bf16),
            pltpu.VMEM(out_weight.shape, bf16),
            pltpu.VMEM((part, width), bf16),
            pltpu.VMEM((rows, vals.shape[1]), bf16),
            pltpu.VMEM((tp_count, part, width), bf16),
            pltpu.VMEM((tp_count, part, width), bf16),
            pltpu.VMEM((part, width), f32),
            pltpu.VMEM((team * (halo + rows), width), bf16),
            pltpu.VMEM((2, halo + rows, piece), f32),
            pltpu.VMEM((rows, piece), bf16),
            pltpu.VMEM((team, 2, pairs * part, width), bf16),
            pltpu.VMEM((team, pairs * part, width), bf16),
            pltpu.VMEM((team, pairs, part, width), bf16),
            pltpu.VMEM((team, pairs, part, width), bf16),
            pltpu.VMEM((team, part, width), bf16),
            pltpu.VMEM((team, part, width), bf16),
            dma((10,)),
            dma((lines,)),
            dma((lines,)),
            dma((lines,)),
            dma((lines,)),
            dma((lines,)),
            dma((2, lines)),
            dma((2, lines)),
            dma((2, lines)),
            dma((2, lines)),
            dma((tp_count,)),
            dma((tp_count,)),
            dma((team, pairs)),
            dma((team, pairs)),
            dma((team, pairs)),
            dma((team, pairs)),
            dma((team,)),
            dma((team,)),
            dma((team,)),
            dma((team,)),
            dma((team, pairs)),
            dma((team, pairs)),
            dma((team,)),
            dma((team,)),
            dma((team,)),
            dma((team,)),
            dma((team,)),
        ],
        compiler_params=pltpu.CompilerParams(
            collective_id=0, has_side_effects=True, vmem_limit_bytes=60 * 1024 * 1024
        ),
    )(*args)


def solution(mesh):
    in_specs = (
        P("sp", "tp"),
        P("sp", "tp"),
        P("sp", "tp"),
        P("sp", "tp"),
        P("sp", "tp"),
        P("tp"),
        P(),
        P("tp", None),
        P("sp", None),
        P(),
        P("sp", "tp"),
        P("sp", "tp"),
        P(None, "tp"),
        P(None, "tp"),
        P("tp", None),
    )
    body = functools.partial(shards, mesh.shape["sp"], mesh.shape["tp"])
    return jax.shard_map(
        body, mesh=mesh, in_specs=in_specs, out_specs=P(("sp", "tp"), None), check_vma=False
    )
```

```python
import functools

import jax
import jax.numpy as jnp
from jax import lax
from jax.experimental import pallas as pl
from jax.experimental.pallas import tpu as pltpu
from jax.sharding import PartitionSpec as P

norm_eps = 1e-06
far_below = -1e30
halo = 16
lanes = 2
f32 = jnp.float32
bf16 = jnp.bfloat16


def rms_scale(field, gain):
    return field * lax.rsqrt(jnp.mean(field * field, axis=-1, keepdims=True) + norm_eps) * gain


def layer(
    sp_count,
    tp_count,
    team,
    q_a,
    k_a,
    q_b,
    k_b,
    vals,
    lambdas,
    head_gain,
    out_weight,
    residual,
    mix_gain,
    gate_weight,
    up_weight,
    gate_taps,
    up_taps,
    down_weight,
    out,
    kv,
    w_own,
    w,
    down,
    out_w,
    res,
    heads,
    part_out,
    part_in,
    stream,
    ffn,
    acc,
    hidden,
    pair_out,
    pair_in,
    y_out,
    y_in,
    z_out,
    z_in,
    local,
    kvz_send,
    kvz_recv,
    kvx_send,
    kvx_recv,
    relay_send,
    wz_send,
    wz_recv,
    wx_send,
    wx_recv,
    rs_send,
    rs_recv,
    gy_send,
    gy_recv,
    gc_send,
    gc_recv,
    halo_send,
    halo_recv,
    pair_send,
    pair_recv,
    y_send,
    y_recv,
    z_send,
    z_recv,
    team_send,
    team_recv,
    up_send,
):
    s = lax.axis_index("sp")
    t = lax.axis_index("tp")
    x = lax.rem(s, lanes)
    z = s // lanes
    lines = sp_count // lanes
    mate = z * lanes + (1 - x)
    rows = q_a.shape[0]
    key_width = q_a.shape[1]
    value_width = vals.shape[1]
    head_count = lambdas.shape[0]
    head_dim = key_width // head_count
    value_dim = value_width // head_count
    part = rows // tp_count
    width = out.shape[1]
    w_rows = gate_weight.shape[0]
    ff = gate_weight.shape[1]
    taps = gate_taps.shape[0]
    piece = w.shape[2]
    fresh = ff - (team - 1) * piece
    g = lax.rem(z, team)
    base = z - g
    pairs = tp_count // 2
    c_own = lax.rem(t, 2)
    k_own = t // 2
    slot_rows = halo + rows

    def member(slot):
        return (base + slot) * lanes + x

    def columns(line):
        return pl.multiple_of(jnp.minimum(lax.rem(line, team) * piece, ff - piece), 128)

    def by_width(line, act):
        if fresh == piece:
            act(0)
        else:
            last = lax.rem(line, team) == team - 1

            @pl.when(last)
            def _():
                act(piece - fresh)

            @pl.when(jnp.logical_not(last))
            def _():
                act(0)

    def remote(src, dst, send, recv, sp, tp):
        return pltpu.make_async_remote_copy(
            src_ref=src,
            dst_ref=dst,
            send_sem=send,
            recv_sem=recv,
            device_id=(sp, tp),
            device_id_type=pl.DeviceIdType.MESH,
        )

    def kv_block(block):
        return kv.at[pl.ds(pl.multiple_of(block * rows, 16), rows)]

    def w_block(c, block, skip=0):
        at = pl.ds(pl.multiple_of(block * w_rows, 16), w_rows)
        return w.at[c, at, pl.ds(skip, piece - skip)]

    own = pl.ds(pl.multiple_of(s * rows, 16), rows)
    kv_loads = (
        pltpu.make_async_copy(k_a, kv.at[own, pl.ds(0, key_width)], local.at[0]),
        pltpu.make_async_copy(k_b, kv.at[own, pl.ds(key_width, key_width)], local.at[1]),
        pltpu.make_async_copy(vals, kv.at[own, pl.ds(2 * key_width, value_width)], local.at[2]),
    )
    w_loads = (
        pltpu.make_async_copy(gate_weight, w_own.at[0], local.at[3]),
        pltpu.make_async_copy(up_weight, w_own.at[1], local.at[4]),
        pltpu.make_async_copy(gate_weight.at[:, pl.ds(columns(z), piece)], w_block(0, s), local.at[8]),
        pltpu.make_async_copy(up_weight.at[:, pl.ds(columns(z), piece)], w_block(1, s), local.at[9]),
    )
    out_load = pltpu.make_async_copy(out_weight, out_w, local.at[5])
    res_load = pltpu.make_async_copy(
        residual.at[pl.ds(pl.multiple_of(t * part, 16), part)], res, local.at[6]
    )
    down_load = pltpu.make_async_copy(down_weight.at[pl.ds(columns(z), piece)], down, local.at[7])
    for load in kv_loads + w_loads + (out_load, res_load, down_load):
        load.start()

    barrier = pltpu.get_barrier_semaphore()

    @pl.loop(1, sp_count)
    def _(i):
        pl.semaphore_signal(
            barrier,
            inc=1,
            device_id=(lax.rem(s + i, sp_count), t),
            device_id_type=pl.DeviceIdType.MESH,
        )

    @pl.loop(1, tp_count)
    def _(i):
        pl.semaphore_signal(
            barrier,
            inc=1,
            device_id=(s, lax.rem(t + i, tp_count)),
            device_id_type=pl.DeviceIdType.MESH,
        )

    @pl.loop(1, team)
    def _(j):
        @pl.loop(1, tp_count)
        def _(i):
            pl.semaphore_signal(
                barrier,
                inc=1,
                device_id=(member(lax.rem(g + j, team)), lax.rem(t + i, tp_count)),
                device_id_type=pl.DeviceIdType.MESH,
            )

    pl.semaphore_wait(barrier, sp_count - 1 + team * (tp_count - 1))

    def kvz(line, to, index):
        block = kv_block(line * lanes + x)
        return remote(block, block, kvz_send.at[index], kvz_recv.at[line], to * lanes + x, t)

    def kv_relay(line):
        block = kv_block(line * lanes + x)
        return remote(
            block, block, relay_send.at[line], kvz_recv.at[line], (z + 1) * lanes + x, t
        )

    def relays(line):
        direct = (line == z - 1) & (lax.rem(line, 2) == 0)
        return (z + 1 < lines) & jnp.logical_not(direct)

    def kvx(line, lane):
        block = kv_block(line * lanes + lane)
        return remote(block, block, kvx_send.at[line], kvx_recv.at[line], mate, t)

    def wz(c, line, to, index, skip):
        block = w_block(c, line * lanes + x, skip)
        at = pl.ds(pl.multiple_of(columns(to) + skip, 128), piece - skip)
        return remote(
            w_own.at[c, :, at], block, wz_send.at[c, index], wz_recv.at[c, line], to * lanes + x, t
        )

    def wx(c, line, lane, skip):
        block = w_block(c, line * lanes + lane, skip)
        return remote(block, block, wx_send.at[c, line], wx_recv.at[c, line], mate, t)

    for load in kv_loads:
        load.wait()

    @pl.when((lax.rem(z, 2) == 0) & (z + 2 < lines))
    def _():
        kvz(z, z + 2, z + 2).start()

    @pl.when(z + 1 < lines)
    def _():
        kvz(z, z + 1, z + 1).start()

    kvx(z, x).start()
    for load in w_loads:
        load.wait()

    def near(distance, act):
        for line, there in ((z + distance, z + distance < lines), (z - distance, z >= distance)):

            @pl.when(there)
            def _():
                act(line)

    def send_weights(to):
        def act(skip):
            for c in range(2):
                wz(c, z, to, to, skip).start()

        by_width(to, act)

    def deferred(to):
        step = to - z
        slot = lax.rem(to, team)
        up = ((slot == team // 2) & (step <= 2)) | ((slot == team - 1) & (step == 1))
        down = (step != -2) | (slot != 0)
        return jnp.logical_not(jnp.where(step > 0, up, down))

    def send_first(to):
        @pl.when(jnp.logical_not(deferred(to)))
        def _():
            send_weights(to)

    def send_later(to):
        @pl.when(deferred(to))
        def _():
            send_weights(to)

    @pl.loop(1, lines)
    def _(distance):
        near(distance, send_first)

    scale = head_dim**-0.5
    column = lax.broadcasted_iota(jnp.int32, (rows, key_width), 1) // head_dim
    queries = [
        jnp.where(column == h, q[...], jnp.zeros((), bf16))
        for q in (q_a, q_b)
        for h in range(head_count)
    ]
    span = lanes * rows
    query_pos = s * rows + lax.broadcasted_iota(jnp.int32, (rows, span), 0)
    key_step = lax.broadcasted_iota(jnp.int32, (rows, span), 1)

    def attend(i, state):
        line = z - i

        @pl.when(i < z)
        def _():
            kvz(line - 1, mate // lanes, line - 1).wait_recv()
            kvx(line - 1, x).start()

            @pl.when(relays(line - 1))
            def _():
                kv_relay(line - 1).start()


        @pl.when(i == jnp.maximum(z - 1, 0))
        def _():
            def act(skip):
                for c in range(2):
                    wx(c, z, x, skip).start()

            by_width(z, act)

        kvx(line, 1 - x).wait_recv()
        keys_at = pl.ds(pl.multiple_of(line * span, 16), span)
        visible = line * span + key_step <= query_pos
        following = []
        for m in range(2):
            keys = kv[keys_at, pl.ds(m * key_width, key_width)]
            for h in range(head_count):
                peak, total, sums = state[m * head_count + h]
                value = kv[keys_at, pl.ds(2 * key_width + h * value_dim, value_dim)]
                scores = (
                    lax.dot_general(
                        queries[m * head_count + h],
                        keys,
                        (((1,), (1,)), ((), ())),
                        preferred_element_type=f32,
                    )
                    * scale
                )
                scores = jnp.where(visible, scores, far_below)
                new_peak = jnp.maximum(peak, jnp.max(scores, axis=-1, keepdims=True))
                fade = jnp.exp(peak - new_peak)
                expo = jnp.exp(scores - new_peak)
                total = total * fade + jnp.sum(expo, axis=-1, keepdims=True)
                sums = sums * fade + jnp.dot(expo.astype(bf16), value, preferred_element_type=f32)
                following.append((new_peak, total, sums))
        return tuple(following)

    start = tuple(
        (
            jnp.full((rows, 1), far_below, f32),
            jnp.zeros((rows, 1), f32),
            jnp.zeros((rows, value_dim), f32),
        )
        for _ in range(2 * head_count)
    )
    state = lax.fori_loop(0, z + 1, attend, start)
    for h in range(head_count):
        _, total_a, sums_a = state[h]
        _, total_b, sums_b = state[head_count + h]
        diff = sums_a / total_a - lambdas[h] * (sums_b / total_b)
        heads[:, h * value_dim : (h + 1) * value_dim] = rms_scale(diff, head_gain[...]).astype(bf16)

    def forward(line):
        def act(skip):
            for c in range(2):
                wz(c, line, mate // lanes, line, skip).wait_recv()
                wx(c, line, x, skip).start()

        by_width(z, act)

    out_load.wait()
    res_load.wait()
    stream[...] = res[...].astype(f32)

    def part_copy(i):
        to = lax.rem(t + i, tp_count)
        return remote(part_out.at[to], part_in.at[t], rs_send.at[to], rs_recv.at[t], s, to)

    for i in range(1, tp_count + 1):
        to = lax.rem(t + i, tp_count)
        product = jnp.dot(
            heads[pl.ds(pl.multiple_of(to * part, 16), part), :],
            out_w[...],
            preferred_element_type=f32,
        )
        if i < tp_count:
            part_out[to] = product.astype(bf16)
            part_copy(i).start()
        else:
            stream[...] += product
    for i in range(1, tp_count):
        source = lax.rem(t + i, tp_count)
        remote(
            part_out.at[source], part_in.at[source], rs_send.at[source], rs_recv.at[source], s, source
        ).wait_recv()
        stream[...] += part_in[source].astype(f32)

    def ffn_rows(slot, rank):
        return pl.ds(pl.multiple_of(slot * slot_rows + halo + rank * part, 16), part)

    ffn[ffn_rows(g, t), :] = rms_scale(stream[...], mix_gain[...]).astype(bf16)

    def team_copy(slot, to):
        rows_here = ffn.at[ffn_rows(slot, t)]
        return remote(rows_here, rows_here, team_send.at[to], team_recv.at[slot], member(to), t)

    def direct(source, to):
        if team < 4:
            return True
        if source < to:
            return to - source == 1 or (to - source == 2 and source % 2 == 0)
        return (source, to) != (2, 0)

    def relay_to(source, at):
        if at > source and at + 1 < team and not direct(source, at + 1):
            return at + 1
        if at < source and at > 0 and not direct(source, at - 1):
            return at - 1
        return None

    def team_relay(slot, to):
        rows_here = ffn.at[ffn_rows(slot, t)]
        return remote(
            rows_here, rows_here, up_send.at[slot], team_recv.at[slot], member(to), t
        )

    def y_gather(slot, k, source):
        rows_here = ffn.at[ffn_rows(slot, 2 * source + c_own)]
        return remote(
            rows_here, rows_here, gy_send.at[slot, k], gy_recv.at[slot, source], s, 2 * k + c_own
        )

    def core_gather(slot, k, c):
        rows_here = ffn.at[ffn_rows(slot, 2 * k + c)]
        return remote(
            rows_here, rows_here, gc_send.at[slot, k], gc_recv.at[slot, k], s, t + 1 - 2 * c_own
        )

    def hold(slot):
        for i in range(1, pairs):
            y_gather(slot, lax.rem(k_own + i, pairs), k_own).start()
        core_gather(slot, k_own, c_own).start()

    def halo_copy(slot, to_slot, to):
        return remote(
            ffn.at[pl.ds(pl.multiple_of(slot * slot_rows + rows, 16), halo)],
            ffn.at[pl.ds(pl.multiple_of(to_slot * slot_rows, 16), halo)],
            halo_send.at[slot],
            halo_recv.at[to_slot],
            to,
            t,
        )

    def halos(slot, act):
        @pl.when(x < lanes - 1)
        def _():
            act(halo_copy(slot, slot, mate))

        @pl.when((x == lanes - 1) & (slot < team - 1))
        def _():
            act(halo_copy(slot, slot + 1, mate))

        @pl.when((x == lanes - 1) & (slot == team - 1) & (z + team < lines))
        def _():
            act(halo_copy(slot, 0, (z + team) * lanes))

    def pass_on(slot):
        for i in range(1, pairs):
            k = lax.rem(k_own + i, pairs)
            y_gather(slot, k, k).wait_recv()
            core_gather(slot, k, c_own).start()

    def ready(slot):
        for k in range(pairs):
            core_gather(slot, k, 1 - c_own).wait_recv()
        halos(slot, lambda copy: copy.start())

    targets = {(4, 0): (2, 1), (4, 1): (2, 0), (4, 2): (1, 3), (4, 3): (0, 1, 2)}
    orders = {
        (4, 0): "w1 o w3 x1 s1 x3 w2 x2 s3 s2",
        (4, 1): "w2 w3 x0 x2 s0 o s2 w0 x3 s3",
        (4, 2): "w3 w0 x0 w1 x1 o s0 s1 x3 s3",
        (4, 3): "w2 x2 o w0 w1 x0 s2 x1 s0 s1",
    }

    def take(slot, at):
        team_copy(slot, at).wait_recv()
        to = relay_to(slot, at)
        if to is not None:
            team_relay(slot, to).start()
        hold(slot)

    def settle(slot):
        pass_on(slot)
        ready(slot)

    def plan(at):
        others = [j for j in range(team) if j != at]
        for to in targets.get((team, at), others):
            team_copy(at, to).start()
        hold(at)

        @pl.loop(1, lines)
        def _(i):
            near(lines - i, send_later)

        default = " ".join(["o"] + [kind + str(j) for kind in "wxs" for j in others])
        for step in orders.get((team, at), default).split():
            if step == "o":
                settle(at)
            elif step[0] == "w":
                forward(base + int(step[1]))
            elif step[0] == "x":
                take(int(step[1]), at)
            else:
                settle(int(step[1]))

    def at_own(act):
        for at in range(team):

            @pl.when(g == at)
            def _():
                act(at)

    at_own(plan)

    if lines > team:

        @pl.loop(0, lines - team)
        def _(i):
            forward(jnp.where(i < base, i, i + team))

    @pl.loop(0, lines)
    def _(line):
        def act(skip):
            for c in range(2):
                wx(c, line, 1 - x, skip).wait_recv()

        by_width(z, act)

    down_load.wait()
    chunk = 512 if width % 512 == 0 else width

    turns = {4: ((2, 3, 1, 0), (2, 3, 0, 1), (0, 1, 3, 2), (0, 1, 2, 3))}

    def slot_of(n):
        if team not in turns:
            return lax.rem(g + 1 + n, team)
        slot = turns[team][0][n]
        for at in range(1, team):
            slot = jnp.where(g == at, turns[team][at][n], slot)
        return slot

    def part_rows(k):
        return pl.ds(pl.multiple_of(k * part, 16), part)

    def pair_copy(n):
        return remote(
            pair_out.at[n, 1 - c_own],
            pair_in.at[n],
            pair_send.at[n],
            pair_recv.at[n],
            s,
            t + 1 - 2 * c_own,
        )

    def y_copy(n, k, source):
        return remote(
            y_out.at[n, k],
            y_in.at[n, source],
            y_send.at[n, k],
            y_recv.at[n, source],
            s,
            2 * k + c_own,
        )

    def z_copy(n, source):
        return remote(
            z_out.at[n], z_in.at[source], z_send.at[n], z_recv.at[source], member(slot_of(n)), t
        )

    def compute(n):
        slot = slot_of(n)

        block = member(slot)
        halo_rows = pl.ds(pl.multiple_of(slot * slot_rows, 16), halo)

        @pl.when(block == 0)
        def _():
            ffn[halo_rows, :] = jnp.zeros((halo, width), bf16)

        @pl.when(block > 0)
        def _():
            halo_copy(slot, slot, mate).wait_recv()

        rows_at = pl.ds(pl.multiple_of(slot * slot_rows, 16), slot_rows)
        for c in range(2):
            acc[c] = jnp.dot(ffn[rows_at, :], w[c], preferred_element_type=f32)
        for i in range(piece // 128):
            at = slice(i * 128, (i + 1) * 128)
            tap_at = pl.ds(pl.multiple_of(columns(z) + i * 128, 128), 128)
            made = []
            for c, tap in enumerate((gate_taps, up_taps)):
                total = None
                for k in range(taps):
                    first = halo - taps + 1 + k
                    row = acc[c, first : first + rows, at].astype(bf16).astype(f32)
                    term = tap[pl.ds(k, 1), tap_at] * row
                    total = term if total is None else total + term
                made.append(total)
            value = made[0] / (1 + jnp.exp(-made[0])) * made[1]
            if (i + 1) * 128 <= piece - fresh:
                value = jnp.where(g < team - 1, value, 0.0)
            hidden[:, at] = value.astype(bf16)
        for i in range(width // chunk):
            at = slice(i * chunk, (i + 1) * chunk)
            product = jnp.dot(hidden[...], down[:, at], preferred_element_type=f32).astype(bf16)
            for r in range(tp_count):
                first = (r // 2) * part
                pair_out[n, r % 2, first : first + part, at] = product[r * part : (r + 1) * part]
        pair_copy(n).start()

    def pair_sum(n, k):
        mine = pair_out[n, c_own, part_rows(k), :].astype(f32)
        return mine + pair_in[n, part_rows(k), :].astype(f32)

    def across(n):
        pair_copy(n).wait_recv()
        for i in range(1, pairs):
            k = lax.rem(k_own + i, pairs)
            y_out[n, k] = pair_sum(n, k).astype(bf16)
            y_copy(n, k, k_own).start()

    def along(n):
        total = pair_sum(n, k_own)
        for i in range(1, pairs):
            k = lax.rem(k_own + i, pairs)
            y_copy(n, k, k).wait_recv()
            total = total + y_in[n, k].astype(f32)
        if n < team - 1:
            z_out[n] = total.astype(bf16)
            z_copy(n, g).start()
        else:
            stream[...] += total

    for n in range(team + 1):
        if n < team:
            compute(n)
        if n > 0:
            across(n - 1)
    for n in range(team):
        along(n)
    for n in range(team - 1):
        source = slot_of(n)
        z_copy(n, source).wait_recv()
        stream[...] += z_in[source].astype(f32)
    out[...] = stream[...].astype(bf16)

    @pl.when((lax.rem(z, 2) == 0) & (z + 2 < lines))
    def _():
        kvz(z, z + 2, z + 2).wait_send()

    @pl.when(z + 1 < lines)
    def _():
        kvz(z, z + 1, z + 1).wait_send()

    @pl.loop(0, z)
    def _(line):
        @pl.when(relays(line))
        def _():
            kv_relay(line).wait_send()

    @pl.loop(0, z + 1)
    def _(line):
        kvx(line, x).wait_send()

    @pl.loop(1, lines)
    def _(i):
        to = lax.rem(z + i, lines)

        def act(skip):
            for c in range(2):
                wz(c, z, to, to, skip).wait_send()

        by_width(to, act)

    @pl.loop(0, lines)
    def _(line):
        def act(skip):
            for c in range(2):
                wx(c, line, x, skip).wait_send()

        by_width(z, act)

    for i in range(1, tp_count):
        part_copy(i).wait_send()

    def sent(at):
        for slot in range(team):
            if slot == at:
                continue
            if (team, at) not in targets or slot in targets[team, at]:
                team_copy(at, slot).wait_send()
            to = relay_to(slot, at)
            if to is not None:
                team_relay(slot, to).wait_send()

    at_own(sent)
    for slot in range(team):
        for i in range(1, pairs):
            y_gather(slot, lax.rem(k_own + i, pairs), k_own).wait_send()
        for k in range(pairs):
            core_gather(slot, k, c_own).wait_send()
        halos(slot, lambda copy: copy.wait_send())
    for n in range(team):
        pair_copy(n).wait_send()
        for i in range(1, pairs):
            y_copy(n, lax.rem(k_own + i, pairs), k_own).wait_send()
        if n < team - 1:
            z_copy(n, g).wait_send()


def shards(sp_count, tp_count, *args):
    (q_a, _, _, _, vals, lambdas, head_gain, out_weight, residual, mix_gain, gate, _, _, _, down) = args
    rows = q_a.shape[0]
    width = residual.shape[1]
    w_rows, ff = gate.shape
    part = rows // tp_count
    lines = sp_count // lanes
    team = next(n for n in (4, 2, 1) if lines % n == 0)
    pairs = tp_count // 2
    piece = -(-ff // (team * 128)) * 128
    args = list(args)
    args[6] = head_gain.reshape(1, -1)
    args[9] = mix_gain.reshape(1, -1)
    vmem = pl.BlockSpec(memory_space=pltpu.VMEM)
    hbm = pl.BlockSpec(memory_space=pl.ANY)
    smem = pl.BlockSpec(memory_space=pltpu.SMEM)
    dma = pltpu.SemaphoreType.DMA
    in_specs = [vmem, hbm, vmem, hbm, hbm, smem, vmem, hbm, hbm, vmem, hbm, hbm, vmem, vmem, hbm]
    return pl.pallas_call(
        functools.partial(layer, sp_count, tp_count, team),
        out_shape=jax.ShapeDtypeStruct((part, width), bf16),
        in_specs=in_specs,
        out_specs=vmem,
        scratch_shapes=[
            pltpu.VMEM((sp_count * rows, 2 * q_a.shape[1] + vals.shape[1]), bf16),
            pltpu.VMEM((2, w_rows, ff), bf16),
            pltpu.VMEM((2, sp_count * w_rows, piece), bf16),
            pltpu.VMEM((piece, width), bf16),
            pltpu.VMEM(out_weight.shape, bf16),
            pltpu.VMEM((part, width), bf16),
            pltpu.VMEM((rows, vals.shape[1]), bf16),
            pltpu.VMEM((tp_count, part, width), bf16),
            pltpu.VMEM((tp_count, part, width), bf16),
            pltpu.VMEM((part, width), f32),
            pltpu.VMEM((team * (halo + rows), width), bf16),
            pltpu.VMEM((2, halo + rows, piece), f32),
            pltpu.VMEM((rows, piece), bf16),
            pltpu.VMEM((team, 2, pairs * part, width), bf16),
            pltpu.VMEM((team, pairs * part, width), bf16),
            pltpu.VMEM((team, pairs, part, width), bf16),
            pltpu.VMEM((team, pairs, part, width), bf16),
            pltpu.VMEM((team, part, width), bf16),
            pltpu.VMEM((team, part, width), bf16),
            dma((10,)),
            dma((lines,)),
            dma((lines,)),
            dma((lines,)),
            dma((lines,)),
            dma((lines,)),
            dma((2, lines)),
            dma((2, lines)),
            dma((2, lines)),
            dma((2, lines)),
            dma((tp_count,)),
            dma((tp_count,)),
            dma((team, pairs)),
            dma((team, pairs)),
            dma((team, pairs)),
            dma((team, pairs)),
            dma((team,)),
            dma((team,)),
            dma((team,)),
            dma((team,)),
            dma((team, pairs)),
            dma((team, pairs)),
            dma((team,)),
            dma((team,)),
            dma((team,)),
            dma((team,)),
            dma((team,)),
        ],
        compiler_params=pltpu.CompilerParams(
            collective_id=0, has_side_effects=True, vmem_limit_bytes=60 * 1024 * 1024
        ),
    )(*args)


def solution(mesh):
    in_specs = (
        P("sp", "tp"),
        P("sp", "tp"),
        P("sp", "tp"),
        P("sp", "tp"),
        P("sp", "tp"),
        P("tp"),
        P(),
        P("tp", None),
        P("sp", None),
        P(),
        P("sp", "tp"),
        P("sp", "tp"),
        P(None, "tp"),
        P(None, "tp"),
        P("tp", None),
    )
    body = functools.partial(shards, mesh.shape["sp"], mesh.shape["tp"])
    return jax.shard_map(
        body, mesh=mesh, in_specs=in_specs, out_specs=P(("sp", "tp"), None), check_vma=False
    )
```

```python
import functools

import jax
import jax.numpy as jnp
from jax import lax
from jax.experimental import pallas as pl
from jax.experimental.pallas import tpu as pltpu
from jax.sharding import PartitionSpec as P

norm_eps = 1e-06
far_below = -1e30
halo = 16
lanes = 2
f32 = jnp.float32
bf16 = jnp.bfloat16


def rms_scale(field, gain):
    return field * lax.rsqrt(jnp.mean(field * field, axis=-1, keepdims=True) + norm_eps) * gain


def layer(
    sp_count,
    tp_count,
    team,
    q_a,
    k_a,
    q_b,
    k_b,
    vals,
    lambdas,
    head_gain,
    out_weight,
    residual,
    mix_gain,
    gate_weight,
    up_weight,
    gate_taps,
    up_taps,
    down_weight,
    out,
    kv,
    w_own,
    w,
    down,
    out_w,
    res,
    heads,
    part_out,
    part_in,
    stream,
    ffn,
    acc,
    hidden,
    pair_out,
    pair_in,
    y_out,
    y_in,
    z_out,
    z_in,
    local,
    kvz_send,
    kvz_recv,
    kvx_send,
    kvx_recv,
    relay_send,
    wz_send,
    wz_recv,
    wx_send,
    wx_recv,
    rs_send,
    rs_recv,
    gy_send,
    gy_recv,
    gc_send,
    gc_recv,
    halo_send,
    halo_recv,
    pair_send,
    pair_recv,
    y_send,
    y_recv,
    z_send,
    z_recv,
    team_send,
    team_recv,
    up_send,
):
    s = lax.axis_index("sp")
    t = lax.axis_index("tp")
    x = lax.rem(s, lanes)
    z = s // lanes
    lines = sp_count // lanes
    mate = z * lanes + (1 - x)
    rows = q_a.shape[0]
    key_width = q_a.shape[1]
    value_width = vals.shape[1]
    head_count = lambdas.shape[0]
    head_dim = key_width // head_count
    value_dim = value_width // head_count
    part = rows // tp_count
    width = out.shape[1]
    w_rows = gate_weight.shape[0]
    ff = gate_weight.shape[1]
    taps = gate_taps.shape[0]
    piece = w.shape[2]
    fresh = ff - (team - 1) * piece
    g = lax.rem(z, team)
    base = z - g
    pairs = tp_count // 2
    c_own = lax.rem(t, 2)
    k_own = t // 2
    slot_rows = halo + rows

    def member(slot):
        return (base + slot) * lanes + x

    def columns(line):
        return pl.multiple_of(jnp.minimum(lax.rem(line, team) * piece, ff - piece), 128)

    def by_width(line, act):
        if fresh == piece:
            act(0)
        else:
            last = lax.rem(line, team) == team - 1

            @pl.when(last)
            def _():
                act(piece - fresh)

            @pl.when(jnp.logical_not(last))
            def _():
                act(0)

    def remote(src, dst, send, recv, sp, tp):
        return pltpu.make_async_remote_copy(
            src_ref=src,
            dst_ref=dst,
            send_sem=send,
            recv_sem=recv,
            device_id=(sp, tp),
            device_id_type=pl.DeviceIdType.MESH,
        )

    def kv_block(block):
        return kv.at[pl.ds(pl.multiple_of(block * rows, 16), rows)]

    def w_block(c, block, skip=0):
        at = pl.ds(pl.multiple_of(block * w_rows, 16), w_rows)
        return w.at[c, at, pl.ds(skip, piece - skip)]

    own = pl.ds(pl.multiple_of(s * rows, 16), rows)
    kv_loads = (
        pltpu.make_async_copy(k_a, kv.at[own, pl.ds(0, key_width)], local.at[0]),
        pltpu.make_async_copy(k_b, kv.at[own, pl.ds(key_width, key_width)], local.at[1]),
        pltpu.make_async_copy(vals, kv.at[own, pl.ds(2 * key_width, value_width)], local.at[2]),
    )
    w_loads = (
        pltpu.make_async_copy(gate_weight, w_own.at[0], local.at[3]),
        pltpu.make_async_copy(up_weight, w_own.at[1], local.at[4]),
        pltpu.make_async_copy(gate_weight.at[:, pl.ds(columns(z), piece)], w_block(0, s), local.at[8]),
        pltpu.make_async_copy(up_weight.at[:, pl.ds(columns(z), piece)], w_block(1, s), local.at[9]),
    )
    out_load = pltpu.make_async_copy(out_weight, out_w, local.at[5])
    res_load = pltpu.make_async_copy(
        residual.at[pl.ds(pl.multiple_of(t * part, 16), part)], res, local.at[6]
    )
    down_load = pltpu.make_async_copy(down_weight.at[pl.ds(columns(z), piece)], down, local.at[7])
    for load in kv_loads + w_loads + (out_load, res_load, down_load):
        load.start()

    barrier = pltpu.get_barrier_semaphore()

    @pl.loop(1, sp_count)
    def _(i):
        pl.semaphore_signal(
            barrier,
            inc=1,
            device_id=(lax.rem(s + i, sp_count), t),
            device_id_type=pl.DeviceIdType.MESH,
        )

    @pl.loop(1, tp_count)
    def _(i):
        pl.semaphore_signal(
            barrier,
            inc=1,
            device_id=(s, lax.rem(t + i, tp_count)),
            device_id_type=pl.DeviceIdType.MESH,
        )

    @pl.loop(1, team)
    def _(j):
        @pl.loop(1, tp_count)
        def _(i):
            pl.semaphore_signal(
                barrier,
                inc=1,
                device_id=(member(lax.rem(g + j, team)), lax.rem(t + i, tp_count)),
                device_id_type=pl.DeviceIdType.MESH,
            )

    pl.semaphore_wait(barrier, sp_count - 1 + team * (tp_count - 1))

    def kvz(line, to, index):
        block = kv_block(line * lanes + x)
        return remote(block, block, kvz_send.at[index], kvz_recv.at[line], to * lanes + x, t)

    def kv_relay(line):
        block = kv_block(line * lanes + x)
        return remote(
            block, block, relay_send.at[line], kvz_recv.at[line], (z + 1) * lanes + x, t
        )

    def relays(line):
        direct = (line == z - 1) & (lax.rem(line, 2) == 0)
        return (z + 1 < lines) & jnp.logical_not(direct)

    def kvx(line, lane):
        block = kv_block(line * lanes + lane)
        return remote(block, block, kvx_send.at[line], kvx_recv.at[line], mate, t)

    def wz(c, line, to, index, skip):
        block = w_block(c, line * lanes + x, skip)
        at = pl.ds(pl.multiple_of(columns(to) + skip, 128), piece - skip)
        return remote(
            w_own.at[c, :, at], block, wz_send.at[c, index], wz_recv.at[c, line], to * lanes + x, t
        )

    def wx(c, line, lane, skip):
        block = w_block(c, line * lanes + lane, skip)
        return remote(block, block, wx_send.at[c, line], wx_recv.at[c, line], mate, t)

    for load in kv_loads:
        load.wait()

    @pl.when((lax.rem(z, 2) == 0) & (z + 2 < lines))
    def _():
        kvz(z, z + 2, z + 2).start()

    @pl.when(z + 1 < lines)
    def _():
        kvz(z, z + 1, z + 1).start()

    kvx(z, x).start()
    for load in w_loads:
        load.wait()

    def near(distance, act):
        for line, there in ((z + distance, z + distance < lines), (z - distance, z >= distance)):

            @pl.when(there)
            def _():
                act(line)

    def deferred(to, c):
        step = to - z
        slot = lax.rem(to, team)
        up = ((slot == team // 2) & (step <= 2)) | ((slot == team - 1) & (step == 1))
        down = (step != -2) | (slot != 0) | (c == 0)
        return jnp.logical_not(jnp.where(step > 0, up, down))

    def send_weights(to, later):
        def act(skip):
            for c in range(2):

                @pl.when(deferred(to, c) == later)
                def _():
                    wz(c, z, to, to, skip).start()

        by_width(to, act)

    def send_first(to):
        send_weights(to, False)

    def send_later(to):
        send_weights(to, True)

    @pl.loop(1, lines)
    def _(distance):
        near(distance, send_first)

    scale = head_dim**-0.5
    column = lax.broadcasted_iota(jnp.int32, (rows, key_width), 1) // head_dim
    queries = [
        jnp.where(column == h, q[...], jnp.zeros((), bf16))
        for q in (q_a, q_b)
        for h in range(head_count)
    ]
    span = lanes * rows
    query_pos = s * rows + lax.broadcasted_iota(jnp.int32, (rows, span), 0)
    key_step = lax.broadcasted_iota(jnp.int32, (rows, span), 1)

    hurry = (z >= 2) & (z + 1 < lines)

    def take_keys(line):
        kvz(line, mate // lanes, line).wait_recv()

        @pl.when(relays(line))
        def _():
            kv_relay(line).start()

        kvx(line, x).start()

    @pl.when(hurry)
    def _():
        take_keys(z - 1)
        take_keys(z - 2)

    def attend(i, state):
        line = z - i

        @pl.when((i < z) & ((i > 1) | jnp.logical_not(hurry)))
        def _():
            take_keys(line - 1)


        @pl.when(i == jnp.maximum(z - 1, 0))
        def _():
            def act(skip):
                for c in range(2):
                    wx(c, z, x, skip).start()

            by_width(z, act)

        kvx(line, 1 - x).wait_recv()
        keys_at = pl.ds(pl.multiple_of(line * span, 16), span)
        visible = line * span + key_step <= query_pos
        following = []
        for m in range(2):
            keys = kv[keys_at, pl.ds(m * key_width, key_width)]
            for h in range(head_count):
                peak, total, sums = state[m * head_count + h]
                value = kv[keys_at, pl.ds(2 * key_width + h * value_dim, value_dim)]
                scores = (
                    lax.dot_general(
                        queries[m * head_count + h],
                        keys,
                        (((1,), (1,)), ((), ())),
                        preferred_element_type=f32,
                    )
                    * scale
                )
                scores = jnp.where(visible, scores, far_below)
                new_peak = jnp.maximum(peak, jnp.max(scores, axis=-1, keepdims=True))
                fade = jnp.exp(peak - new_peak)
                expo = jnp.exp(scores - new_peak)
                total = total * fade + jnp.sum(expo, axis=-1, keepdims=True)
                sums = sums * fade + jnp.dot(expo.astype(bf16), value, preferred_element_type=f32)
                following.append((new_peak, total, sums))
        return tuple(following)

    start = tuple(
        (
            jnp.full((rows, 1), far_below, f32),
            jnp.zeros((rows, 1), f32),
            jnp.zeros((rows, value_dim), f32),
        )
        for _ in range(2 * head_count)
    )
    state = lax.fori_loop(0, z + 1, attend, start)
    for h in range(head_count):
        _, total_a, sums_a = state[h]
        _, total_b, sums_b = state[head_count + h]
        diff = sums_a / total_a - lambdas[h] * (sums_b / total_b)
        heads[:, h * value_dim : (h + 1) * value_dim] = rms_scale(diff, head_gain[...]).astype(bf16)

    def forward(line, parts=(0, 1)):
        def act(skip):
            for c in parts:
                wz(c, line, mate // lanes, line, skip).wait_recv()
                wx(c, line, x, skip).start()

        by_width(z, act)

    out_load.wait()
    res_load.wait()
    stream[...] = res[...].astype(f32)

    def part_copy(i):
        to = lax.rem(t + i, tp_count)
        return remote(part_out.at[to], part_in.at[t], rs_send.at[to], rs_recv.at[t], s, to)

    for i in range(1, tp_count + 1):
        to = lax.rem(t + i, tp_count)
        product = jnp.dot(
            heads[pl.ds(pl.multiple_of(to * part, 16), part), :],
            out_w[...],
            preferred_element_type=f32,
        )
        if i < tp_count:
            part_out[to] = product.astype(bf16)
            part_copy(i).start()
        else:
            stream[...] += product
    for i in range(1, tp_count):
        source = lax.rem(t + i, tp_count)
        remote(
            part_out.at[source], part_in.at[source], rs_send.at[source], rs_recv.at[source], s, source
        ).wait_recv()
        stream[...] += part_in[source].astype(f32)

    def ffn_rows(slot, rank):
        return pl.ds(pl.multiple_of(slot * slot_rows + halo + rank * part, 16), part)

    ffn[ffn_rows(g, t), :] = rms_scale(stream[...], mix_gain[...]).astype(bf16)

    def team_copy(slot, to):
        rows_here = ffn.at[ffn_rows(slot, t)]
        return remote(rows_here, rows_here, team_send.at[to], team_recv.at[slot], member(to), t)

    def direct(source, to):
        if team < 4:
            return True
        if source < to:
            return to - source == 1 or (to - source == 2 and source % 2 == 0)
        return (source, to) != (2, 0)

    def relay_to(source, at):
        if at > source and at + 1 < team and not direct(source, at + 1):
            return at + 1
        if at < source and at > 0 and not direct(source, at - 1):
            return at - 1
        return None

    def team_relay(slot, to):
        rows_here = ffn.at[ffn_rows(slot, t)]
        return remote(
            rows_here, rows_here, up_send.at[slot], team_recv.at[slot], member(to), t
        )

    def y_gather(slot, k, source):
        rows_here = ffn.at[ffn_rows(slot, 2 * source + c_own)]
        return remote(
            rows_here, rows_here, gy_send.at[slot, k], gy_recv.at[slot, source], s, 2 * k + c_own
        )

    def core_gather(slot, k, c):
        rows_here = ffn.at[ffn_rows(slot, 2 * k + c)]
        return remote(
            rows_here, rows_here, gc_send.at[slot, k], gc_recv.at[slot, k], s, t + 1 - 2 * c_own
        )

    def hold(slot):
        for i in range(1, pairs):
            y_gather(slot, lax.rem(k_own + i, pairs), k_own).start()
        core_gather(slot, k_own, c_own).start()

    def halo_copy(slot, to_slot, to):
        return remote(
            ffn.at[pl.ds(pl.multiple_of(slot * slot_rows + rows, 16), halo)],
            ffn.at[pl.ds(pl.multiple_of(to_slot * slot_rows, 16), halo)],
            halo_send.at[slot],
            halo_recv.at[to_slot],
            to,
            t,
        )

    def halos(slot, act):
        @pl.when(x < lanes - 1)
        def _():
            act(halo_copy(slot, slot, mate))

        @pl.when((x == lanes - 1) & (slot < team - 1))
        def _():
            act(halo_copy(slot, slot + 1, mate))

        @pl.when((x == lanes - 1) & (slot == team - 1) & (z + team < lines))
        def _():
            act(halo_copy(slot, 0, (z + team) * lanes))

    def pass_on(slot):
        for i in range(1, pairs):
            k = lax.rem(k_own + i, pairs)
            y_gather(slot, k, k).wait_recv()
            core_gather(slot, k, c_own).start()

    def ready(slot):
        for k in range(pairs):
            core_gather(slot, k, 1 - c_own).wait_recv()
        halos(slot, lambda copy: copy.start())

    targets = {(4, 0): (2, 1), (4, 1): (2, 0), (4, 2): (1, 3), (4, 3): (0, 1, 2)}
    orders = {
        (4, 0): ("w1", "o", "w3", "x1", "a2", "s1", "x3", "b2", "x2", "s3", "s2"),
        (4, 1): ("w2", "w3", "x0", "x2", "s0", "o", "s2", "w0", "x3", "s3"),
        (4, 2): ("w3", "w0", "x0", "w1", "x1", "o", "s0", "s1", "x3", "s3"),
        (4, 3): ("w2", "x2", "o", "w0", "w1", "x0", "s2", "x1", "s0", "s1"),
    }

    def take(slot, at):
        team_copy(slot, at).wait_recv()
        to = relay_to(slot, at)
        if to is not None:
            team_relay(slot, to).start()
        hold(slot)

    def settle(slot):
        pass_on(slot)
        ready(slot)

    def plan(at):
        others = [j for j in range(team) if j != at]
        for to in targets.get((team, at), others):
            team_copy(at, to).start()
        hold(at)

        @pl.loop(1, lines)
        def _(i):
            near(lines - i, send_later)

        default = ["o"] + [kind + str(j) for kind in "wxs" for j in others]
        for step in orders.get((team, at), default):
            if step == "o":
                settle(at)
            elif step[0] in "wab":
                forward(base + int(step[1]), {"w": (0, 1), "a": (0,), "b": (1,)}[step[0]])
            elif step[0] == "x":
                take(int(step[1]), at)
            else:
                settle(int(step[1]))

    def at_own(act):
        for at in range(team):

            @pl.when(g == at)
            def _():
                act(at)

    at_own(plan)

    if lines > team:

        @pl.loop(0, lines - team)
        def _(i):
            forward(jnp.where(i < base, i, i + team))

    @pl.loop(0, lines)
    def _(line):
        def act(skip):
            for c in range(2):
                wx(c, line, 1 - x, skip).wait_recv()

        by_width(z, act)

    down_load.wait()
    halves, half = pair_out.shape[1], pair_out.shape[4]
    chunk = 512 if half % 512 == 0 else half

    turns = {4: ((2, 3, 1, 0), (2, 3, 0, 1), (0, 1, 3, 2), (0, 1, 2, 3))}

    def slot_of(n):
        if team not in turns:
            return lax.rem(g + 1 + n, team)
        slot = turns[team][0][n]
        for at in range(1, team):
            slot = jnp.where(g == at, turns[team][at][n], slot)
        return slot

    def part_rows(k):
        return pl.ds(pl.multiple_of(k * part, 16), part)

    def pair_copy(n, h):
        return remote(
            pair_out.at[n, h, 1 - c_own],
            pair_in.at[n, h],
            pair_send.at[n, h],
            pair_recv.at[n, h],
            s,
            t + 1 - 2 * c_own,
        )

    def y_copy(n, h, k, source):
        return remote(
            y_out.at[n, h, k],
            y_in.at[n, h, source],
            y_send.at[n, h, k],
            y_recv.at[n, h, source],
            s,
            2 * k + c_own,
        )

    def z_copy(n, h, kind, to):
        return remote(
            z_out.at[n, h], z_in.at[kind, h], z_send.at[n, h], z_recv.at[kind, h], member(to), t
        )

    def front(n):
        slot = slot_of(n)

        block = member(slot)
        halo_rows = pl.ds(pl.multiple_of(slot * slot_rows, 16), halo)

        @pl.when(block == 0)
        def _():
            ffn[halo_rows, :] = jnp.zeros((halo, width), bf16)

        @pl.when(block > 0)
        def _():
            halo_copy(slot, slot, mate).wait_recv()

        rows_at = pl.ds(pl.multiple_of(slot * slot_rows, 16), slot_rows)
        for c in range(2):
            acc[c] = jnp.dot(ffn[rows_at, :], w[c], preferred_element_type=f32)
        for i in range(piece // 128):
            at = slice(i * 128, (i + 1) * 128)
            tap_at = pl.ds(pl.multiple_of(columns(z) + i * 128, 128), 128)
            made = []
            for c, tap in enumerate((gate_taps, up_taps)):
                total = None
                for k in range(taps):
                    first = halo - taps + 1 + k
                    row = acc[c, first : first + rows, at].astype(bf16).astype(f32)
                    term = tap[pl.ds(k, 1), tap_at] * row
                    total = term if total is None else total + term
                made.append(total)
            value = made[0] / (1 + jnp.exp(-made[0])) * made[1]
            if (i + 1) * 128 <= piece - fresh:
                value = jnp.where(g < team - 1, value, 0.0)
            hidden[:, at] = value.astype(bf16)

    def back(n):
        for h in range(halves):
            for i in range(half // chunk):
                at = slice(i * chunk, (i + 1) * chunk)
                down_at = slice(h * half + i * chunk, h * half + (i + 1) * chunk)
                product = jnp.dot(
                    hidden[...], down[:, down_at], preferred_element_type=f32
                ).astype(bf16)
                for r in range(tp_count):
                    first = (r // 2) * part
                    pair_out[n, h, r % 2, first : first + part, at] = product[
                        r * part : (r + 1) * part
                    ]
            pair_copy(n, h).start()

    def pair_sum(n, h, k):
        mine = pair_out[n, h, c_own, part_rows(k), :].astype(f32)
        return mine + pair_in[n, h, part_rows(k), :].astype(f32)

    def across(n):
        for h in range(halves):
            pair_copy(n, h).wait_recv()
            for i in range(1, pairs):
                k = lax.rem(k_own + i, pairs)
                y_out[n, h, k] = pair_sum(n, h, k).astype(bf16)
                y_copy(n, h, k, k_own).start()

    far = 2 if team == 4 else 0
    near_slot = g + 1 - 2 * lax.rem(g, 2)
    inner = (g == 1) | (g == 2)

    def along(n, h):
        at = slice(h * half, (h + 1) * half)
        total = pair_sum(n, h, k_own)
        for i in range(1, pairs):
            k = lax.rem(k_own + i, pairs)
            y_copy(n, h, k, k).wait_recv()
            total = total + y_in[n, h, k].astype(f32)
        if n < far:

            @pl.when(inner)
            def _():
                z_copy(n, h, 2 + n, near_slot).wait_recv()
                z_out[n, h] = (total + z_in[2 + n, h].astype(f32)).astype(bf16)
                z_copy(n, h, 1, slot_of(n)).start()

            @pl.when(jnp.logical_not(inner))
            def _():
                z_out[n, h] = total.astype(bf16)
                z_copy(n, h, 2 + n, near_slot).start()

        elif n < team - 1:
            z_out[n, h] = total.astype(bf16)
            z_copy(n, h, 0, near_slot).start()
        else:
            stream[:, at] += total

    for n in range(team + 1):
        if n < team:
            front(n)
        if n > 0:
            across(n - 1)
        if n < team:
            back(n)
    for n in range(team):
        for h in range(halves):
            along(n, h)
    for h in range(halves):
        at = slice(h * half, (h + 1) * half)
        total = stream[:, at]
        for kind in range(min(2, team - 1) if far else team - 1):
            z_copy(0, h, kind, near_slot).wait_recv()
            total = total + z_in[kind, h].astype(f32)
        out[:, at] = total.astype(bf16)

    @pl.when((lax.rem(z, 2) == 0) & (z + 2 < lines))
    def _():
        kvz(z, z + 2, z + 2).wait_send()

    @pl.when(z + 1 < lines)
    def _():
        kvz(z, z + 1, z + 1).wait_send()

    @pl.loop(0, z)
    def _(line):
        @pl.when(relays(line))
        def _():
            kv_relay(line).wait_send()

    @pl.loop(0, z + 1)
    def _(line):
        kvx(line, x).wait_send()

    @pl.loop(1, lines)
    def _(i):
        to = lax.rem(z + i, lines)

        def act(skip):
            for c in range(2):
                wz(c, z, to, to, skip).wait_send()

        by_width(to, act)

    @pl.loop(0, lines)
    def _(line):
        def act(skip):
            for c in range(2):
                wx(c, line, x, skip).wait_send()

        by_width(z, act)

    for i in range(1, tp_count):
        part_copy(i).wait_send()

    def sent(at):
        for slot in range(team):
            if slot == at:
                continue
            if (team, at) not in targets or slot in targets[team, at]:
                team_copy(at, slot).wait_send()
            to = relay_to(slot, at)
            if to is not None:
                team_relay(slot, to).wait_send()

    at_own(sent)
    for slot in range(team):
        for i in range(1, pairs):
            y_gather(slot, lax.rem(k_own + i, pairs), k_own).wait_send()
        for k in range(pairs):
            core_gather(slot, k, c_own).wait_send()
        halos(slot, lambda copy: copy.wait_send())
    for n in range(team):
        for h in range(halves):
            pair_copy(n, h).wait_send()
            for i in range(1, pairs):
                y_copy(n, h, lax.rem(k_own + i, pairs), k_own).wait_send()
            if n < team - 1:
                z_copy(n, h, 0, near_slot).wait_send()


def shards(sp_count, tp_count, *args):
    (q_a, _, _, _, vals, lambdas, head_gain, out_weight, residual, mix_gain, gate, _, _, _, down) = args
    rows = q_a.shape[0]
    width = residual.shape[1]
    w_rows, ff = gate.shape
    part = rows // tp_count
    lines = sp_count // lanes
    team = next(n for n in (4, 2, 1) if lines % n == 0)
    pairs = tp_count // 2
    piece = -(-ff // (team * 128)) * 128
    halves = 2 if width % 256 == 0 else 1
    half = width // halves
    args = list(args)
    args[6] = head_gain.reshape(1, -1)
    args[9] = mix_gain.reshape(1, -1)
    vmem = pl.BlockSpec(memory_space=pltpu.VMEM)
    hbm = pl.BlockSpec(memory_space=pl.ANY)
    smem = pl.BlockSpec(memory_space=pltpu.SMEM)
    dma = pltpu.SemaphoreType.DMA
    in_specs = [vmem, hbm, vmem, hbm, hbm, smem, vmem, hbm, hbm, vmem, hbm, hbm, vmem, vmem, hbm]
    return pl.pallas_call(
        functools.partial(layer, sp_count, tp_count, team),
        out_shape=jax.ShapeDtypeStruct((part, width), bf16),
        in_specs=in_specs,
        out_specs=vmem,
        scratch_shapes=[
            pltpu.VMEM((sp_count * rows, 2 * q_a.shape[1] + vals.shape[1]), bf16),
            pltpu.VMEM((2, w_rows, ff), bf16),
            pltpu.VMEM((2, sp_count * w_rows, piece), bf16),
            pltpu.VMEM((piece, width), bf16),
            pltpu.VMEM(out_weight.shape, bf16),
            pltpu.VMEM((part, width), bf16),
            pltpu.VMEM((rows, vals.shape[1]), bf16),
            pltpu.VMEM((tp_count, part, width), bf16),
            pltpu.VMEM((tp_count, part, width), bf16),
            pltpu.VMEM((part, width), f32),
            pltpu.VMEM((team * (halo + rows), width), bf16),
            pltpu.VMEM((2, halo + rows, piece), f32),
            pltpu.VMEM((rows, piece), bf16),
            pltpu.VMEM((team, halves, 2, pairs * part, half), bf16),
            pltpu.VMEM((team, halves, pairs * part, half), bf16),
            pltpu.VMEM((team, halves, pairs, part, half), bf16),
            pltpu.VMEM((team, halves, pairs, part, half), bf16),
            pltpu.VMEM((team, halves, part, half), bf16),
            pltpu.VMEM((4, halves, part, half), bf16),
            dma((10,)),
            dma((lines,)),
            dma((lines,)),
            dma((lines,)),
            dma((lines,)),
            dma((lines,)),
            dma((2, lines)),
            dma((2, lines)),
            dma((2, lines)),
            dma((2, lines)),
            dma((tp_count,)),
            dma((tp_count,)),
            dma((team, pairs)),
            dma((team, pairs)),
            dma((team, pairs)),
            dma((team, pairs)),
            dma((team,)),
            dma((team,)),
            dma((team, halves)),
            dma((team, halves)),
            dma((team, halves, pairs)),
            dma((team, halves, pairs)),
            dma((team, halves)),
            dma((4, halves)),
            dma((team,)),
            dma((team,)),
            dma((team,)),
        ],
        compiler_params=pltpu.CompilerParams(
            collective_id=0, has_side_effects=True, vmem_limit_bytes=60 * 1024 * 1024
        ),
    )(*args)


def solution(mesh):
    in_specs = (
        P("sp", "tp"),
        P("sp", "tp"),
        P("sp", "tp"),
        P("sp", "tp"),
        P("sp", "tp"),
        P("tp"),
        P(),
        P("tp", None),
        P("sp", None),
        P(),
        P("sp", "tp"),
        P("sp", "tp"),
        P(None, "tp"),
        P(None, "tp"),
        P("tp", None),
    )
    body = functools.partial(shards, mesh.shape["sp"], mesh.shape["tp"])
    return jax.shard_map(
        body, mesh=mesh, in_specs=in_specs, out_specs=P(("sp", "tp"), None), check_vma=False
    )
```

```python
import functools

import jax
import jax.numpy as jnp
from jax import lax
from jax.experimental import pallas as pl
from jax.experimental.pallas import tpu as pltpu
from jax.sharding import PartitionSpec as P

norm_eps = 1e-06
far_below = -1e30
halo = 16
lanes = 2
f32 = jnp.float32
bf16 = jnp.bfloat16


def rms_scale(field, gain):
    return field * lax.rsqrt(jnp.mean(field * field, axis=-1, keepdims=True) + norm_eps) * gain


def layer(
    sp_count,
    tp_count,
    team,
    q_a_in,
    k_a,
    q_b_in,
    k_b,
    vals,
    lambdas,
    head_gain_in,
    out_weight,
    residual,
    mix_gain_in,
    gate_weight,
    up_weight,
    gate_taps_in,
    up_taps_in,
    down_weight,
    result,
    kv,
    w_own,
    w,
    down,
    out_w,
    res,
    heads,
    part_out,
    part_in,
    stream,
    ffn,
    acc,
    hidden,
    pair_out,
    pair_in,
    y_out,
    y_in,
    z_out,
    z_in,
    q_a,
    q_b,
    head_gain,
    mix_gain,
    gate_taps,
    up_taps,
    out,
    local,
    kvz_send,
    kvz_recv,
    kvx_send,
    kvx_recv,
    relay_send,
    wz_send,
    wz_recv,
    wx_send,
    wx_recv,
    rs_send,
    rs_recv,
    gy_send,
    gy_recv,
    gc_send,
    gc_recv,
    halo_send,
    halo_recv,
    pair_send,
    pair_recv,
    y_send,
    y_recv,
    z_send,
    z_recv,
    team_send,
    team_recv,
    up_send,
):
    s = lax.axis_index("sp")
    t = lax.axis_index("tp")
    x = lax.rem(s, lanes)
    z = s // lanes
    lines = sp_count // lanes
    mate = z * lanes + (1 - x)
    rows = q_a.shape[0]
    key_width = q_a.shape[1]
    value_width = vals.shape[1]
    head_count = lambdas.shape[0]
    head_dim = key_width // head_count
    value_dim = value_width // head_count
    part = rows // tp_count
    width = out.shape[1]
    w_rows = gate_weight.shape[0]
    w_parts = wz_recv.shape[2]
    w_piece = w_rows // w_parts
    ff = gate_weight.shape[1]
    taps = gate_taps.shape[0]
    piece = w.shape[2]
    fresh = ff - (team - 1) * piece
    g = lax.rem(z, team)
    base = z - g
    pairs = tp_count // 2
    c_own = lax.rem(t, 2)
    k_own = t // 2
    slot_rows = halo + rows
    kv_parts = kvz_recv.shape[1]
    kv_piece = rows // kv_parts
    row_parts = team_recv.shape[1]
    row_piece = part // row_parts

    def member(slot):
        return (base + slot) * lanes + x

    def columns(line):
        return pl.multiple_of(jnp.minimum(lax.rem(line, team) * piece, ff - piece), 128)

    def by_width(line, act):
        if fresh == piece:
            act(0)
        else:
            last = lax.rem(line, team) == team - 1

            @pl.when(last)
            def _():
                act(piece - fresh)

            @pl.when(jnp.logical_not(last))
            def _():
                act(0)

    def remote(src, dst, send, recv, sp, tp):
        return pltpu.make_async_remote_copy(
            src_ref=src,
            dst_ref=dst,
            send_sem=send,
            recv_sem=recv,
            device_id=(sp, tp),
            device_id_type=pl.DeviceIdType.MESH,
        )

    def sent_all(block, sem):
        remote(block, block, sem, sem, s, t).wait_send()

    def came_all(block, sem):
        remote(block, block, sem, sem, s, t).wait_recv()

    def kv_rows(block):
        return kv.at[pl.ds(pl.multiple_of(block * rows, 16), rows)]

    def kv_block(block, p):
        return kv.at[pl.ds(pl.multiple_of(block * rows + p * kv_piece, 16), kv_piece)]

    def w_block(c, block):
        return w.at[c, pl.ds(pl.multiple_of(block * w_rows, 16), w_rows)]

    def w_part(c, block, skip, p):
        at = pl.ds(pl.multiple_of(block * w_rows + p * w_piece, 16), w_piece)
        return w.at[c, at, pl.ds(skip, piece - skip)]

    barrier = pltpu.get_barrier_semaphore()

    @pl.loop(1, sp_count)
    def _(i):
        pl.semaphore_signal(
            barrier,
            inc=1,
            device_id=(lax.rem(s + i, sp_count), t),
            device_id_type=pl.DeviceIdType.MESH,
        )

    @pl.loop(1, tp_count)
    def _(i):
        pl.semaphore_signal(
            barrier,
            inc=1,
            device_id=(s, lax.rem(t + i, tp_count)),
            device_id_type=pl.DeviceIdType.MESH,
        )

    @pl.loop(1, team)
    def _(j):
        @pl.loop(1, tp_count)
        def _(i):
            pl.semaphore_signal(
                barrier,
                inc=1,
                device_id=(member(lax.rem(g + j, team)), lax.rem(t + i, tp_count)),
                device_id_type=pl.DeviceIdType.MESH,
            )

    own = pl.ds(pl.multiple_of(s * rows, 16), rows)
    kv_loads = (
        pltpu.make_async_copy(k_a, kv.at[own, pl.ds(0, key_width)], local.at[0]),
        pltpu.make_async_copy(k_b, kv.at[own, pl.ds(key_width, key_width)], local.at[1]),
        pltpu.make_async_copy(vals, kv.at[own, pl.ds(2 * key_width, value_width)], local.at[2]),
    )
    w_loads = (
        pltpu.make_async_copy(gate_weight, w_own.at[0], local.at[3]),
        pltpu.make_async_copy(up_weight, w_own.at[1], local.at[4]),
        pltpu.make_async_copy(gate_weight.at[:, pl.ds(columns(z), piece)], w_block(0, s), local.at[8]),
        pltpu.make_async_copy(up_weight.at[:, pl.ds(columns(z), piece)], w_block(1, s), local.at[9]),
    )
    out_load = pltpu.make_async_copy(out_weight, out_w, local.at[5])
    res_load = pltpu.make_async_copy(
        residual.at[pl.ds(pl.multiple_of(t * part, 16), part)], res, local.at[6]
    )
    down_load = pltpu.make_async_copy(down_weight.at[pl.ds(columns(z), piece)], down, local.at[7])
    small_loads = (
        pltpu.make_async_copy(q_a_in, q_a, local.at[10]),
        pltpu.make_async_copy(q_b_in, q_b, local.at[11]),
        pltpu.make_async_copy(head_gain_in, head_gain, local.at[12]),
        pltpu.make_async_copy(mix_gain_in, mix_gain, local.at[13]),
        pltpu.make_async_copy(gate_taps_in, gate_taps, local.at[14]),
        pltpu.make_async_copy(up_taps_in, up_taps, local.at[15]),
    )
    for load in kv_loads + w_loads + small_loads + (out_load, res_load, down_load):
        load.start()

    pl.semaphore_wait(barrier, sp_count - 1 + team * (tp_count - 1))

    def kvz(line, to, p):
        block = kv_block(line * lanes + x, p)
        return remote(
            block, block, kvz_send.at[to], kvz_recv.at[line, p], to * lanes + x, t
        )

    def kv_relay(line, p):
        block = kv_block(line * lanes + x, p)
        return remote(
            block, block, relay_send.at[line], kvz_recv.at[line, p], (z + 1) * lanes + x, t
        )

    def relays(line):
        direct = (line == z - 1) & (lax.rem(line, 2) == 0)
        return (z + 1 < lines) & jnp.logical_not(direct)

    def kvx(line, lane, p):
        block = kv_block(line * lanes + lane, p)
        return remote(block, block, kvx_send.at[line], kvx_recv.at[line], mate, t)

    def wz(c, line, to, skip, p):
        at = pl.ds(pl.multiple_of(columns(to) + skip, 128), piece - skip)
        return remote(
            w_own.at[c, pl.ds(p * w_piece, w_piece), at],
            w_part(c, line * lanes + x, skip, p),
            wz_send.at[to],
            wz_recv.at[c, line, p],
            to * lanes + x,
            t,
        )

    def wx(c, line, lane, skip, p):
        block = w_part(c, line * lanes + lane, skip, p)
        return remote(block, block, wx_send.at[0], wx_recv.at[0], mate, t)

    for load in kv_loads:
        load.wait()

    @pl.when((lax.rem(z, 2) == 0) & (z + 2 < lines))
    def _():
        for p in range(kv_parts):
            kvz(z, z + 2, p).start()

    @pl.when(z + 1 < lines)
    def _():
        for p in range(kv_parts):
            kvz(z, z + 1, p).start()

    for p in range(kv_parts):
        kvx(z, x, p).start()
    for load in w_loads:
        load.wait()

    def near(distance, act):
        for line, there in ((z + distance, z + distance < lines), (z - distance, z >= distance)):

            @pl.when(there)
            def _():
                act(line)

    def deferred(to, c):
        step = to - z
        slot = lax.rem(to, team)
        up = (slot == team // 2) & ((step == 2) | ((step == 1) & (c == 0)))
        up = up | ((slot == team - 1) & (step == 1))
        down = (step != -2) | (slot != 0) | (c == 0)
        return jnp.logical_not(jnp.where(step > 0, up, down))

    def send_weights(to, later):
        def act(skip):
            for c in range(2):

                @pl.when(deferred(to, c) == later)
                def _():
                    for p in range(w_parts):
                        wz(c, z, to, skip, p).start()

        by_width(to, act)

    def send_first(to):
        send_weights(to, False)

    def send_later(to):
        send_weights(to, True)

    @pl.loop(1, lines)
    def _(distance):
        near(distance, send_first)

    for load in small_loads:
        load.wait()
    scale = head_dim**-0.5
    column = lax.broadcasted_iota(jnp.int32, (rows, key_width), 1) // head_dim
    queries = [
        jnp.where(column == h, q[...], jnp.zeros((), bf16))
        for q in (q_a, q_b)
        for h in range(head_count)
    ]
    span = lanes * rows
    query_pos = s * rows + lax.broadcasted_iota(jnp.int32, (rows, span), 0)
    key_step = lax.broadcasted_iota(jnp.int32, (rows, span), 1)

    hurry = (z >= 2) & (z + 1 < lines)

    def take_keys(line):
        for p in range(kv_parts):
            kvz(line, mate // lanes, p).wait_recv()

            @pl.when(relays(line))
            def _():
                kv_relay(line, p).start()

            kvx(line, x, p).start()

    @pl.when(hurry)
    def _():
        take_keys(z - 1)
        take_keys(z - 2)

    def attend(i, state):
        line = z - i

        @pl.when((i < z) & ((i > 1) | jnp.logical_not(hurry)))
        def _():
            take_keys(line - 1)


        @pl.when(i == jnp.maximum(z - 1, 0))
        def _():
            def act(skip):
                for c in range(2):
                    for p in range(w_parts):
                        wx(c, z, x, skip, p).start()

            by_width(z, act)

        came_all(kv_rows(line * lanes + 1 - x), kvx_recv.at[line])
        keys_at = pl.ds(pl.multiple_of(line * span, 16), span)
        visible = line * span + key_step <= query_pos
        following = []
        for m in range(2):
            keys = kv[keys_at, pl.ds(m * key_width, key_width)]
            for h in range(head_count):
                peak, total, sums = state[m * head_count + h]
                value = kv[keys_at, pl.ds(2 * key_width + h * value_dim, value_dim)]
                scores = (
                    lax.dot_general(
                        queries[m * head_count + h],
                        keys,
                        (((1,), (1,)), ((), ())),
                        preferred_element_type=f32,
                    )
                    * scale
                )
                scores = jnp.where(visible, scores, far_below)
                new_peak = jnp.maximum(peak, jnp.max(scores, axis=-1, keepdims=True))
                fade = jnp.exp(peak - new_peak)
                expo = jnp.exp(scores - new_peak)
                total = total * fade + jnp.sum(expo, axis=-1, keepdims=True)
                sums = sums * fade + jnp.dot(expo.astype(bf16), value, preferred_element_type=f32)
                following.append((new_peak, total, sums))
        return tuple(following)

    start = tuple(
        (
            jnp.full((rows, 1), far_below, f32),
            jnp.zeros((rows, 1), f32),
            jnp.zeros((rows, value_dim), f32),
        )
        for _ in range(2 * head_count)
    )
    state = lax.fori_loop(0, z + 1, attend, start)
    for h in range(head_count):
        _, total_a, sums_a = state[h]
        _, total_b, sums_b = state[head_count + h]
        diff = sums_a / total_a - lambdas[h] * (sums_b / total_b)
        heads[:, h * value_dim : (h + 1) * value_dim] = rms_scale(diff, head_gain[...]).astype(bf16)

    def forward(line, parts=(0, 1)):
        def act(skip):
            for c in parts:
                for p in range(w_parts):
                    wz(c, line, mate // lanes, skip, p).wait_recv()
                    wx(c, line, x, skip, p).start()

        by_width(z, act)

    out_load.wait()
    res_load.wait()
    stream[...] = res[...].astype(f32)

    def part_copy(to):
        return remote(part_out.at[to], part_in.at[t], rs_send.at[0], rs_recv.at[t], s, to)

    def spread():
        ranks = [2 * lax.rem(k_own + i, pairs) + c for i in range(1, pairs) for c in range(2)]
        return ranks + [t + 1 - 2 * c_own]

    def project_part(to):
        at = pl.ds(pl.multiple_of(to * part, 16), part)
        return jnp.dot(heads[at, :], out_w[...], preferred_element_type=f32)

    for to in spread():
        part_out[to] = project_part(to).astype(bf16)
        part_copy(to).start()
    stream[...] += project_part(t)
    for source in reversed(spread()):
        remote(
            part_out.at[source], part_in.at[source], rs_send.at[0], rs_recv.at[source], s, source
        ).wait_recv()
        stream[...] += part_in[source].astype(f32)

    def ffn_rows(slot, rank):
        return pl.ds(pl.multiple_of(slot * slot_rows + halo + rank * part, 16), part)

    ffn[ffn_rows(g, t), :] = rms_scale(stream[...], mix_gain[...]).astype(bf16)

    def row_block(slot, rank, p):
        first = slot * slot_rows + halo + rank * part + p * row_piece
        return ffn.at[pl.ds(pl.multiple_of(first, 16), row_piece)]

    def team_copy(slot, to, p):
        block = row_block(slot, t, p)
        return remote(block, block, team_send.at[to], team_recv.at[slot, p], member(to), t)

    def direct(source, to):
        if team < 4:
            return True
        if source < to:
            return to - source == 1 or (to - source == 2 and source % 2 == 0)
        return (source, to) != (2, 0)

    def relay_to(source, at):
        if at > source and at + 1 < team and not direct(source, at + 1):
            return at + 1
        if at < source and at > 0 and not direct(source, at - 1):
            return at - 1
        return None

    def team_relay(slot, to, p):
        block = row_block(slot, t, p)
        return remote(block, block, up_send.at[slot], team_recv.at[slot, p], member(to), t)

    def y_gather(slot, k, source, p):
        block = row_block(slot, 2 * source + c_own, p)
        return remote(
            block, block, gy_send.at[0], gy_recv.at[slot, source], s, 2 * k + c_own
        )

    def core_gather(slot, k, c):
        rows_here = ffn.at[ffn_rows(slot, 2 * k + c)]
        return remote(
            rows_here, rows_here, gc_send.at[0], gc_recv.at[slot], s, t + 1 - 2 * c_own
        )

    def some_rows(count):
        return ffn.at[pl.ds(0, count * part)]

    def hold(slot, p):
        for i in range(1, pairs):
            y_gather(slot, lax.rem(k_own + i, pairs), k_own, p).start()

    def halo_copy(slot, to_slot, to):
        return remote(
            ffn.at[pl.ds(pl.multiple_of(slot * slot_rows + rows, 16), halo)],
            ffn.at[pl.ds(pl.multiple_of(to_slot * slot_rows, 16), halo)],
            halo_send.at[slot],
            halo_recv.at[to_slot],
            to,
            t,
        )

    def halos(slot, act):
        @pl.when(x < lanes - 1)
        def _():
            act(halo_copy(slot, slot, mate))

        @pl.when((x == lanes - 1) & (slot < team - 1))
        def _():
            act(halo_copy(slot, slot + 1, mate))

        @pl.when((x == lanes - 1) & (slot == team - 1) & (z + team < lines))
        def _():
            act(halo_copy(slot, 0, (z + team) * lanes))

    def pass_on(slot):
        for i in range(1, pairs):
            k = lax.rem(k_own + i, pairs)
            came_all(ffn.at[ffn_rows(slot, 2 * k + c_own)], gy_recv.at[slot, k])
            core_gather(slot, k, c_own).start()

    def ready(slot):
        came_all(some_rows(pairs), gc_recv.at[slot])
        halos(slot, lambda copy: copy.start())

    targets = {(4, 0): (2, 1), (4, 1): (2, 0), (4, 2): (1, 3), (4, 3): (0, 1, 2)}
    orders = {
        (4, 0): ("w1", "o", "w3", "x1", "a2", "s1", "x3", "b2", "x2", "s3", "s2"),
        (4, 1): ("w2", "w3", "x0", "w0", "x2", "s0", "o", "x3", "s2", "s3"),
        (4, 2): ("w3", "w0", "x0", "a1", "x1", "b1", "o", "s0", "s1", "x3", "s3"),
        (4, 3): ("w2", "o", "x2", "w0", "w1", "x0", "x1", "s2", "s0", "s1"),
    }

    def take(slot, at):
        to = relay_to(slot, at)
        for p in range(row_parts):
            team_copy(slot, at, p).wait_recv()
            if to is not None:
                team_relay(slot, to, p).start()
            hold(slot, p)
        core_gather(slot, k_own, c_own).start()

    def settle(slot):
        pass_on(slot)
        ready(slot)

    def plan(at):
        others = [j for j in range(team) if j != at]
        for to in targets.get((team, at), others):
            for p in range(row_parts):
                team_copy(at, to, p).start()
        for p in range(row_parts):
            hold(at, p)
        core_gather(at, k_own, c_own).start()

        @pl.loop(1, lines)
        def _(distance):
            near(distance, send_later)

        default = ["o"] + [kind + str(j) for kind in "wxs" for j in others]
        for step in orders.get((team, at), default):
            if step == "o":
                settle(at)
            elif step[0] in "wab":
                forward(base + int(step[1]), {"w": (0, 1), "a": (0,), "b": (1,)}[step[0]])
            elif step[0] == "x":
                take(int(step[1]), at)
            else:
                settle(int(step[1]))

    def at_own(act):
        for at in range(team):

            @pl.when(g == at)
            def _():
                act(at)

    at_own(plan)

    if lines > team:

        @pl.loop(0, lines - team)
        def _(i):
            forward(jnp.where(i < base, i, i + team))

    def w_lines(skip):
        return w.at[:, pl.ds(0, lines * w_rows), pl.ds(skip, piece - skip)]

    by_width(z, lambda skip: came_all(w_lines(skip), wx_recv.at[0]))

    down_load.wait()
    halves, half = pair_out.shape[1], pair_out.shape[4]
    chunk = 512 if half % 512 == 0 else half

    turns = {4: ((2, 3, 1, 0), (2, 3, 0, 1), (0, 1, 3, 2), (0, 1, 2, 3))}

    def slot_of(n):
        if team not in turns:
            return lax.rem(g + 1 + n, team)
        slot = turns[team][0][n]
        for at in range(1, team):
            slot = jnp.where(g == at, turns[team][at][n], slot)
        return slot

    def part_rows(k):
        return pl.ds(pl.multiple_of(k * part, 16), part)

    def pair_copy(n, h):
        return remote(
            pair_out.at[n, h, 1 - c_own],
            pair_in.at[n, h],
            pair_send.at[0],
            pair_recv.at[n, h],
            s,
            t + 1 - 2 * c_own,
        )

    def y_copy(n, h, k, source):
        return remote(
            y_out.at[n, h, k],
            y_in.at[n, h, source],
            y_send.at[0],
            y_recv.at[n, h, lax.rem(source - k + pairs - 1 + pairs, pairs)],
            s,
            2 * k + c_own,
        )

    def z_copy(n, h, kind, to):
        return remote(
            z_out.at[n, h], z_in.at[kind, h], z_send.at[0], z_recv.at[kind, h], member(to), t
        )

    def front(n):
        slot = slot_of(n)

        block = member(slot)
        halo_rows = pl.ds(pl.multiple_of(slot * slot_rows, 16), halo)

        @pl.when(block == 0)
        def _():
            ffn[halo_rows, :] = jnp.zeros((halo, width), bf16)

        @pl.when(block > 0)
        def _():
            halo_copy(slot, slot, mate).wait_recv()

        rows_at = pl.ds(pl.multiple_of(slot * slot_rows, 16), slot_rows)
        for c in range(2):
            acc[c] = jnp.dot(ffn[rows_at, :], w[c], preferred_element_type=f32)
        for i in range(piece // 128):
            at = slice(i * 128, (i + 1) * 128)
            tap_at = pl.ds(pl.multiple_of(columns(z) + i * 128, 128), 128)
            made = []
            for c, tap in enumerate((gate_taps, up_taps)):
                total = None
                for k in range(taps):
                    first = halo - taps + 1 + k
                    row = acc[c, first : first + rows, at].astype(bf16).astype(f32)
                    term = tap[pl.ds(k, 1), tap_at] * row
                    total = term if total is None else total + term
                made.append(total)
            value = made[0] / (1 + jnp.exp(-made[0])) * made[1]
            if (i + 1) * 128 <= piece - fresh:
                value = jnp.where(g < team - 1, value, 0.0)
            hidden[:, at] = value.astype(bf16)

    def back(n):
        for h in range(halves):
            for i in range(half // chunk):
                at = slice(i * chunk, (i + 1) * chunk)
                down_at = slice(h * half + i * chunk, h * half + (i + 1) * chunk)
                product = jnp.dot(
                    hidden[...], down[:, down_at], preferred_element_type=f32
                ).astype(bf16)
                for r in range(tp_count):
                    first = (r // 2) * part
                    pair_out[n, h, r % 2, first : first + part, at] = product[
                        r * part : (r + 1) * part
                    ]
            pair_copy(n, h).start()

    def pair_sum(n, h, k):
        mine = pair_out[n, h, c_own, part_rows(k), :].astype(f32)
        return mine + pair_in[n, h, part_rows(k), :].astype(f32)

    def across(n):
        for h in range(halves):
            pair_copy(n, h).wait_recv()
            for i in range(1, pairs):
                k = lax.rem(k_own + i, pairs)
                y_out[n, h, k] = pair_sum(n, h, k).astype(bf16)
                y_copy(n, h, k, k_own).start()

    far = 2 if team == 4 else 0
    near_slot = g + 1 - 2 * lax.rem(g, 2)
    inner = (g == 1) | (g == 2)

    def along(n, h, merging):
        at = slice(h * half, (h + 1) * half)
        total = pair_sum(n, h, k_own)
        for i in range(1, pairs):
            k = lax.rem(k_own + i, pairs)
            y_copy(n, h, k_own, k).wait_recv()
            total = total + y_in[n, h, k].astype(f32)
        if n < far and merging:
            z_copy(n, h, 2 + n, near_slot).wait_recv()
            z_out[n, h] = (total + z_in[2 + n, h].astype(f32)).astype(bf16)
            z_copy(n, h, 1, slot_of(n)).start()
        elif n < far:
            z_out[n, h] = total.astype(bf16)
            z_copy(n, h, 2 + n, near_slot).start()
        elif n < team - 1:
            z_out[n, h] = total.astype(bf16)
            z_copy(n, h, 0, near_slot).start()
        else:
            stream[:, at] += total

    for n in range(team + 1):
        if n < team:
            front(n)
        if n > 0:
            across(n - 1)
        if far and n == team - 1:

            @pl.when(jnp.logical_not(inner))
            def _():
                for h in range(halves):
                    along(0, h, False)

        if n < team:
            back(n)
    @pl.when((lax.rem(z, 2) == 0) & (z + 2 < lines))
    def _():
        sent_all(kv_rows(s), kvz_send.at[z + 2])

    @pl.when(z + 1 < lines)
    def _():
        sent_all(kv_rows(s), kvz_send.at[z + 1])

    @pl.loop(0, z)
    def _(line):
        @pl.when(relays(line))
        def _():
            sent_all(kv_rows(s), relay_send.at[line])

    @pl.loop(0, z + 1)
    def _(line):
        sent_all(kv_rows(s), kvx_send.at[line])

    @pl.loop(1, lines)
    def _(i):
        to = lax.rem(z + i, lines)

        def act(skip):
            at = pl.ds(pl.multiple_of(columns(to) + skip, 128), piece - skip)
            sent_all(w_own.at[:, :, at], wz_send.at[to])

        by_width(to, act)

    by_width(z, lambda skip: sent_all(w_lines(skip), wx_send.at[0]))

    sent_all(part_out.at[pl.ds(0, tp_count - 1)], rs_send.at[0])

    def sent(at):
        for slot in range(team):
            if slot == at:
                continue
            if (team, at) not in targets or slot in targets[team, at]:
                sent_all(some_rows(1), team_send.at[slot])
            to = relay_to(slot, at)
            if to is not None:
                sent_all(some_rows(1), up_send.at[slot])

    at_own(sent)
    for slot in range(team):
        halos(slot, lambda copy: copy.wait_send())
    sent_all(some_rows(team * (pairs - 1)), gy_send.at[0])
    sent_all(some_rows(team * pairs), gc_send.at[0])
    def leave(h):
        at = pl.ds(h * half, half)
        return pltpu.make_async_copy(out.at[:, at], result.at[:, at], local.at[16 + h])

    def finish(merging):
        rest = [(n, h) for n in range(1 if far else 0, team) for h in range(halves)]
        if merging:
            pairwise = [(n, h) for h in range(halves) for n in (1, 2)]
            rest = [(0, h) for h in range(halves)] + pairwise + rest[2 * halves :]
        for n, h in rest:
            along(n, h, merging)

    if far:

        @pl.when(inner)
        def _():
            finish(True)

        @pl.when(jnp.logical_not(inner))
        def _():
            finish(False)

    else:
        finish(False)
    sent_all(pair_in, pair_send.at[0])
    if pairs > 1:
        sent_all(y_in.at[:, :, pl.ds(0, pairs - 1)], y_send.at[0])
    if team > 1:
        sent_all(z_out.at[pl.ds(0, team - 1)], z_send.at[0])
    for h in range(halves):
        at = slice(h * half, (h + 1) * half)
        total = stream[:, at]
        for kind in range(min(2, team - 1) if far else team - 1):
            z_copy(0, h, kind, near_slot).wait_recv()
            total = total + z_in[kind, h].astype(f32)
        out[:, at] = total.astype(bf16)
        leave(h).start()
    for h in range(halves):
        leave(h).wait()


def shards(sp_count, tp_count, *args):
    (q_a, _, _, _, vals, lambdas, head_gain, out_weight, residual, mix_gain, gate, _, _, _, down) = args
    rows = q_a.shape[0]
    width = residual.shape[1]
    w_rows, ff = gate.shape
    part = rows // tp_count
    lines = sp_count // lanes
    team = next(n for n in (4, 2, 1) if lines % n == 0)
    pairs = tp_count // 2
    piece = -(-ff // (team * 128)) * 128
    halves = 4 if width % 512 == 0 else 1
    kv_parts = 2 if rows % 32 == 0 else 1
    w_parts = 2 if w_rows % 32 == 0 else 1
    row_parts = part // 16 if part % 16 == 0 else 1
    half = width // halves
    args = list(args)
    args[6] = head_gain.reshape(1, -1)
    args[9] = mix_gain.reshape(1, -1)
    hbm = pl.BlockSpec(memory_space=pl.ANY)
    smem = pl.BlockSpec(memory_space=pltpu.SMEM)
    dma = pltpu.SemaphoreType.DMA
    in_specs = [hbm] * 5 + [smem] + [hbm] * 9
    return pl.pallas_call(
        functools.partial(layer, sp_count, tp_count, team),
        out_shape=jax.ShapeDtypeStruct((part, width), bf16),
        in_specs=in_specs,
        out_specs=hbm,
        scratch_shapes=[
            pltpu.VMEM((sp_count * rows, 2 * q_a.shape[1] + vals.shape[1]), bf16),
            pltpu.VMEM((2, w_rows, ff), bf16),
            pltpu.VMEM((2, sp_count * w_rows, piece), bf16),
            pltpu.VMEM((piece, width), bf16),
            pltpu.VMEM(out_weight.shape, bf16),
            pltpu.VMEM((part, width), bf16),
            pltpu.VMEM((rows, vals.shape[1]), bf16),
            pltpu.VMEM((tp_count, part, width), bf16),
            pltpu.VMEM((tp_count, part, width), bf16),
            pltpu.VMEM((part, width), f32),
            pltpu.VMEM((team * (halo + rows), width), bf16),
            pltpu.VMEM((2, halo + rows, piece), f32),
            pltpu.VMEM((rows, piece), bf16),
            pltpu.VMEM((team, halves, 2, pairs * part, half), bf16),
            pltpu.VMEM((team, halves, pairs * part, half), bf16),
            pltpu.VMEM((team, halves, pairs, part, half), bf16),
            pltpu.VMEM((team, halves, pairs, part, half), bf16),
            pltpu.VMEM((team, halves, part, half), bf16),
            pltpu.VMEM((4, halves, part, half), bf16),
            pltpu.VMEM(q_a.shape, bf16),
            pltpu.VMEM(q_a.shape, bf16),
            pltpu.VMEM(args[6].shape, f32),
            pltpu.VMEM(args[9].shape, f32),
            pltpu.VMEM(args[12].shape, f32),
            pltpu.VMEM(args[12].shape, f32),
            pltpu.VMEM((part, width), bf16),
            dma((16 + halves,)),
            dma((lines,)),
            dma((lines, kv_parts)),
            dma((lines,)),
            dma((lines,)),
            dma((lines,)),
            dma((lines,)),
            dma((2, lines, w_parts)),
            dma((1,)),
            dma((1,)),
            dma((1,)),
            dma((tp_count,)),
            dma((1,)),
            dma((team, pairs)),
            dma((1,)),
            dma((team,)),
            dma((team,)),
            dma((team,)),
            dma((1,)),
            dma((team, halves)),
            dma((1,)),
            dma((team, halves, max(pairs - 1, 1))),
            dma((1,)),
            dma((4, halves)),
            dma((team,)),
            dma((team, row_parts)),
            dma((team,)),
        ],
        compiler_params=pltpu.CompilerParams(
            collective_id=0, has_side_effects=True, vmem_limit_bytes=60 * 1024 * 1024
        ),
    )(*args)


def solution(mesh):
    in_specs = (
        P("sp", "tp"),
        P("sp", "tp"),
        P("sp", "tp"),
        P("sp", "tp"),
        P("sp", "tp"),
        P("tp"),
        P(),
        P("tp", None),
        P("sp", None),
        P(),
        P("sp", "tp"),
        P("sp", "tp"),
        P(None, "tp"),
        P(None, "tp"),
        P("tp", None),
    )
    body = functools.partial(shards, mesh.shape["sp"], mesh.shape["tp"])
    return jax.shard_map(
        body, mesh=mesh, in_specs=in_specs, out_specs=P(("sp", "tp"), None), check_vma=False
    )
```

```python
import functools

import jax
import jax.numpy as jnp
from jax import lax
from jax.experimental import pallas as pl
from jax.experimental.pallas import tpu as pltpu
from jax.sharding import PartitionSpec as P

norm_eps = 1e-06
far_below = -1e30
halo = 16
lanes = 2
f32 = jnp.float32
bf16 = jnp.bfloat16


def rms_scale(field, gain):
    return field * lax.rsqrt(jnp.mean(field * field, axis=-1, keepdims=True) + norm_eps) * gain


def layer(
    sp_count,
    tp_count,
    team,
    q_a_in,
    k_a,
    q_b_in,
    k_b,
    vals,
    lambdas,
    head_gain_in,
    out_weight,
    residual,
    mix_gain_in,
    gate_weight,
    up_weight,
    gate_taps_in,
    up_taps_in,
    down_weight,
    result,
    kv,
    w_own,
    w,
    down,
    out_w,
    res,
    heads,
    part_out,
    part_in,
    stream,
    ffn,
    acc,
    hidden,
    pair_out,
    pair_in,
    y_out,
    y_in,
    z_out,
    z_in,
    q_a,
    q_b,
    head_gain,
    mix_gain,
    gate_taps,
    up_taps,
    out,
    local,
    kvz_send,
    kvz_recv,
    kvx_send,
    kvx_recv,
    relay_send,
    wz_send,
    wz_recv,
    wx_send,
    wx_recv,
    rs_send,
    rs_recv,
    gy_send,
    gy_recv,
    gc_send,
    gc_recv,
    halo_send,
    halo_recv,
    pair_send,
    pair_recv,
    y_send,
    y_recv,
    z_send,
    z_recv,
    team_send,
    team_recv,
    up_send,
):
    s = lax.axis_index("sp")
    t = lax.axis_index("tp")
    x = lax.rem(s, lanes)
    z = s // lanes
    lines = sp_count // lanes
    mate = z * lanes + (1 - x)
    rows = q_a.shape[0]
    key_width = q_a.shape[1]
    value_width = vals.shape[1]
    head_count = lambdas.shape[0]
    head_dim = key_width // head_count
    value_dim = value_width // head_count
    part = rows // tp_count
    width = out.shape[1]
    w_rows = gate_weight.shape[0]
    w_parts = wz_recv.shape[2]
    w_piece = w_rows // w_parts
    ff = gate_weight.shape[1]
    taps = gate_taps.shape[0]
    piece = w.shape[2]
    fresh = ff - (team - 1) * piece
    g = lax.rem(z, team)
    base = z - g
    pairs = tp_count // 2
    c_own = lax.rem(t, 2)
    k_own = t // 2
    slot_rows = halo + rows
    kv_parts = kvz_recv.shape[1]
    kv_piece = rows // kv_parts
    row_parts = team_recv.shape[1]
    row_piece = part // row_parts

    def member(slot):
        return (base + slot) * lanes + x

    def columns(line):
        return pl.multiple_of(jnp.minimum(lax.rem(line, team) * piece, ff - piece), 128)

    def by_width(line, act):
        if fresh == piece:
            act(0)
        else:
            last = lax.rem(line, team) == team - 1

            @pl.when(last)
            def _():
                act(piece - fresh)

            @pl.when(jnp.logical_not(last))
            def _():
                act(0)

    def remote(src, dst, send, recv, sp, tp):
        return pltpu.make_async_remote_copy(
            src_ref=src,
            dst_ref=dst,
            send_sem=send,
            recv_sem=recv,
            device_id=(sp, tp),
            device_id_type=pl.DeviceIdType.MESH,
        )

    def sent_all(block, sem):
        remote(block, block, sem, sem, s, t).wait_send()

    def came_all(block, sem):
        remote(block, block, sem, sem, s, t).wait_recv()

    def kv_rows(block):
        return kv.at[pl.ds(pl.multiple_of(block * rows, 16), rows)]

    def kv_block(block, p):
        return kv.at[pl.ds(pl.multiple_of(block * rows + p * kv_piece, 16), kv_piece)]

    def w_block(c, block):
        return w.at[c, pl.ds(pl.multiple_of(block * w_rows, 16), w_rows)]

    def w_part(c, block, skip, p):
        at = pl.ds(pl.multiple_of(block * w_rows + p * w_piece, 16), w_piece)
        return w.at[c, at, pl.ds(skip, piece - skip)]

    barrier = pltpu.get_barrier_semaphore()

    @pl.loop(1, sp_count)
    def _(i):
        pl.semaphore_signal(
            barrier,
            inc=1,
            device_id=(lax.rem(s + i, sp_count), t),
            device_id_type=pl.DeviceIdType.MESH,
        )

    @pl.loop(1, tp_count)
    def _(i):
        pl.semaphore_signal(
            barrier,
            inc=1,
            device_id=(s, lax.rem(t + i, tp_count)),
            device_id_type=pl.DeviceIdType.MESH,
        )

    @pl.loop(1, team)
    def _(j):
        @pl.loop(1, tp_count)
        def _(i):
            pl.semaphore_signal(
                barrier,
                inc=1,
                device_id=(member(lax.rem(g + j, team)), lax.rem(t + i, tp_count)),
                device_id_type=pl.DeviceIdType.MESH,
            )

    own = pl.ds(pl.multiple_of(s * rows, 16), rows)
    kv_loads = (
        pltpu.make_async_copy(k_a, kv.at[own, pl.ds(0, key_width)], local.at[0]),
        pltpu.make_async_copy(k_b, kv.at[own, pl.ds(key_width, key_width)], local.at[1]),
        pltpu.make_async_copy(vals, kv.at[own, pl.ds(2 * key_width, value_width)], local.at[2]),
    )
    w_loads = (
        pltpu.make_async_copy(gate_weight, w_own.at[0], local.at[3]),
        pltpu.make_async_copy(up_weight, w_own.at[1], local.at[4]),
        pltpu.make_async_copy(gate_weight.at[:, pl.ds(columns(z), piece)], w_block(0, s), local.at[8]),
        pltpu.make_async_copy(up_weight.at[:, pl.ds(columns(z), piece)], w_block(1, s), local.at[9]),
    )
    out_load = pltpu.make_async_copy(out_weight, out_w, local.at[5])
    res_load = pltpu.make_async_copy(
        residual.at[pl.ds(pl.multiple_of(t * part, 16), part)], res, local.at[6]
    )
    down_load = pltpu.make_async_copy(down_weight.at[pl.ds(columns(z), piece)], down, local.at[7])
    small_loads = (
        pltpu.make_async_copy(q_a_in, q_a, local.at[10]),
        pltpu.make_async_copy(q_b_in, q_b, local.at[11]),
        pltpu.make_async_copy(head_gain_in, head_gain, local.at[12]),
        pltpu.make_async_copy(mix_gain_in, mix_gain, local.at[13]),
        pltpu.make_async_copy(gate_taps_in, gate_taps, local.at[14]),
        pltpu.make_async_copy(up_taps_in, up_taps, local.at[15]),
    )
    for load in kv_loads + w_loads + small_loads + (out_load, res_load, down_load):
        load.start()

    pl.semaphore_wait(barrier, sp_count - 1 + team * (tp_count - 1))

    def kvz(line, to, p):
        block = kv_block(line * lanes + x, p)
        return remote(
            block, block, kvz_send.at[to], kvz_recv.at[line, p], to * lanes + x, t
        )

    def kv_relay(line, p):
        block = kv_block(line * lanes + x, p)
        return remote(
            block, block, relay_send.at[line], kvz_recv.at[line, p], (z + 1) * lanes + x, t
        )

    def relays(line):
        direct = (line == z - 1) & (lax.rem(line, 2) == 0)
        return (z + 1 < lines) & jnp.logical_not(direct)

    def kvx(line, lane, p):
        block = kv_block(line * lanes + lane, p)
        return remote(block, block, kvx_send.at[line], kvx_recv.at[line], mate, t)

    def wz(c, line, to, skip, p):
        at = pl.ds(pl.multiple_of(columns(to) + skip, 128), piece - skip)
        return remote(
            w_own.at[c, pl.ds(p * w_piece, w_piece), at],
            w_part(c, line * lanes + x, skip, p),
            wz_send.at[to],
            wz_recv.at[c, line, p],
            to * lanes + x,
            t,
        )

    def wx(c, line, lane, skip, p):
        block = w_part(c, line * lanes + lane, skip, p)
        return remote(block, block, wx_send.at[0], wx_recv.at[0], mate, t)

    for load in kv_loads:
        load.wait()

    @pl.when((lax.rem(z, 2) == 0) & (z + 2 < lines))
    def _():
        for p in range(kv_parts):
            kvz(z, z + 2, p).start()

    @pl.when(z + 1 < lines)
    def _():
        for p in range(kv_parts):
            kvz(z, z + 1, p).start()

    for p in range(kv_parts):
        kvx(z, x, p).start()
    for load in w_loads:
        load.wait()

    def near(distance, act):
        for line, there in ((z + distance, z + distance < lines), (z - distance, z >= distance)):

            @pl.when(there)
            def _():
                act(line)

    def deferred(to, c):
        step = to - z
        slot = lax.rem(to, team)
        up = (slot == team // 2) & ((step == 2) | ((step == 1) & (c == 0)))
        up = up | (slot == team - 1)
        down = (step != -1) | (slot != team // 2 - 1) | (c == 0)
        return jnp.logical_not(jnp.where(step > 0, up, down))

    def send_weights(to, later):
        def act(skip):
            for c in range(2):

                @pl.when(deferred(to, c) == later)
                def _():
                    for p in range(w_parts):
                        wz(c, z, to, skip, p).start()

        by_width(to, act)

    def send_first(to):
        send_weights(to, False)

    def send_later(to):
        send_weights(to, True)

    for distance in (3, 1, 2):

        @pl.when(z >= distance)
        def _():
            send_first(z - distance)

    @pl.loop(1, lines)
    def _(distance):
        @pl.when(z + distance < lines)
        def _():
            send_first(z + distance)

        @pl.when((distance > 3) & (z >= distance))
        def _():
            send_first(z - distance)


    for load in small_loads:
        load.wait()
    scale = head_dim**-0.5
    column = lax.broadcasted_iota(jnp.int32, (rows, key_width), 1) // head_dim
    queries = [
        jnp.where(column == h, q[...], jnp.zeros((), bf16))
        for q in (q_a, q_b)
        for h in range(head_count)
    ]
    span = lanes * rows
    query_pos = s * rows + lax.broadcasted_iota(jnp.int32, (rows, span), 0)
    key_step = lax.broadcasted_iota(jnp.int32, (rows, span), 1)

    hurry = (z >= 2) & (z + 1 < lines)

    def take_keys(line):
        for p in range(kv_parts):
            kvz(line, mate // lanes, p).wait_recv()

            @pl.when(relays(line))
            def _():
                kv_relay(line, p).start()

            kvx(line, x, p).start()

    @pl.when(hurry)
    def _():
        take_keys(z - 1)
        take_keys(z - 2)

    def attend(i, state):
        line = z - i

        @pl.when((i < z) & ((i > 1) | jnp.logical_not(hurry)))
        def _():
            take_keys(line - 1)


        @pl.when(i == jnp.maximum(z - 1, 0))
        def _():
            def act(skip):
                for c in range(2):
                    for p in range(w_parts):
                        wx(c, z, x, skip, p).start()

            by_width(z, act)

        came_all(kv_rows(line * lanes + 1 - x), kvx_recv.at[line])
        keys_at = pl.ds(pl.multiple_of(line * span, 16), span)
        visible = line * span + key_step <= query_pos
        following = []
        for m in range(2):
            keys = kv[keys_at, pl.ds(m * key_width, key_width)]
            for h in range(head_count):
                peak, total, sums = state[m * head_count + h]
                value = kv[keys_at, pl.ds(2 * key_width + h * value_dim, value_dim)]
                scores = (
                    lax.dot_general(
                        queries[m * head_count + h],
                        keys,
                        (((1,), (1,)), ((), ())),
                        preferred_element_type=f32,
                    )
                    * scale
                )
                scores = jnp.where(visible, scores, far_below)
                new_peak = jnp.maximum(peak, jnp.max(scores, axis=-1, keepdims=True))
                fade = jnp.exp(peak - new_peak)
                expo = jnp.exp(scores - new_peak)
                total = total * fade + jnp.sum(expo, axis=-1, keepdims=True)
                sums = sums * fade + jnp.dot(expo.astype(bf16), value, preferred_element_type=f32)
                following.append((new_peak, total, sums))
        return tuple(following)

    start = tuple(
        (
            jnp.full((rows, 1), far_below, f32),
            jnp.zeros((rows, 1), f32),
            jnp.zeros((rows, value_dim), f32),
        )
        for _ in range(2 * head_count)
    )
    state = lax.fori_loop(0, z + 1, attend, start)
    for h in range(head_count):
        _, total_a, sums_a = state[h]
        _, total_b, sums_b = state[head_count + h]
        diff = sums_a / total_a - lambdas[h] * (sums_b / total_b)
        heads[:, h * value_dim : (h + 1) * value_dim] = rms_scale(diff, head_gain[...]).astype(bf16)

    def forward(line, parts=(0, 1)):
        def act(skip):
            for c in parts:
                for p in range(w_parts):
                    wz(c, line, mate // lanes, skip, p).wait_recv()
                    wx(c, line, x, skip, p).start()

        by_width(z, act)

    if team == 4:

        @pl.when(g == 2)
        def _():
            forward(z + 1)

        @pl.when(g == 3)
        def _():
            forward(z - 1)

    out_load.wait()
    res_load.wait()
    stream[...] = res[...].astype(f32)

    def part_copy(to):
        return remote(part_out.at[to], part_in.at[t], rs_send.at[0], rs_recv.at[t], s, to)

    def spread():
        ranks = [2 * lax.rem(k_own + i, pairs) + c for i in range(1, pairs) for c in range(2)]
        return ranks + [t + 1 - 2 * c_own]

    def project_part(to):
        at = pl.ds(pl.multiple_of(to * part, 16), part)
        return jnp.dot(heads[at, :], out_w[...], preferred_element_type=f32)

    for to in spread():
        part_out[to] = project_part(to).astype(bf16)
        part_copy(to).start()
    stream[...] += project_part(t)
    for source in reversed(spread()):
        remote(
            part_out.at[source], part_in.at[source], rs_send.at[0], rs_recv.at[source], s, source
        ).wait_recv()
        stream[...] += part_in[source].astype(f32)

    def ffn_rows(slot, rank):
        return pl.ds(pl.multiple_of(slot * slot_rows + halo + rank * part, 16), part)

    ffn[ffn_rows(g, t), :] = rms_scale(stream[...], mix_gain[...]).astype(bf16)

    def row_block(slot, rank, p):
        first = slot * slot_rows + halo + rank * part + p * row_piece
        return ffn.at[pl.ds(pl.multiple_of(first, 16), row_piece)]

    def team_copy(slot, to, p):
        block = row_block(slot, t, p)
        return remote(block, block, team_send.at[to], team_recv.at[slot, p], member(to), t)

    def direct(source, to):
        if team < 4:
            return True
        if source < to:
            return to - source == 1 or (to - source == 2 and source % 2 == 0)
        return (source, to) != (2, 0)

    def relay_to(source, at):
        if at > source and at + 1 < team and not direct(source, at + 1):
            return at + 1
        if at < source and at > 0 and not direct(source, at - 1):
            return at - 1
        return None

    def team_relay(slot, to, p):
        block = row_block(slot, t, p)
        return remote(block, block, up_send.at[slot], team_recv.at[slot, p], member(to), t)

    def y_gather(slot, k, source, p):
        block = row_block(slot, 2 * source + c_own, p)
        return remote(
            block, block, gy_send.at[0], gy_recv.at[slot, source], s, 2 * k + c_own
        )

    def core_gather(slot, k, c):
        rows_here = ffn.at[ffn_rows(slot, 2 * k + c)]
        return remote(
            rows_here, rows_here, gc_send.at[0], gc_recv.at[slot], s, t + 1 - 2 * c_own
        )

    def some_rows(count):
        return ffn.at[pl.ds(0, count * part)]

    def hold(slot, p):
        for i in range(1, pairs):
            y_gather(slot, lax.rem(k_own + i, pairs), k_own, p).start()

    def halo_copy(slot, to_slot, to):
        return remote(
            ffn.at[pl.ds(pl.multiple_of(slot * slot_rows + rows, 16), halo)],
            ffn.at[pl.ds(pl.multiple_of(to_slot * slot_rows, 16), halo)],
            halo_send.at[slot],
            halo_recv.at[to_slot],
            to,
            t,
        )

    def halos(slot, act):
        @pl.when(x < lanes - 1)
        def _():
            act(halo_copy(slot, slot, mate))

        @pl.when((x == lanes - 1) & (slot < team - 1))
        def _():
            act(halo_copy(slot, slot + 1, mate))

        @pl.when((x == lanes - 1) & (slot == team - 1) & (z + team < lines))
        def _():
            act(halo_copy(slot, 0, (z + team) * lanes))

    def pass_on(slot):
        for i in range(1, pairs):
            k = lax.rem(k_own + i, pairs)
            came_all(ffn.at[ffn_rows(slot, 2 * k + c_own)], gy_recv.at[slot, k])
            core_gather(slot, k, c_own).start()

    def ready(slot):
        came_all(some_rows(pairs), gc_recv.at[slot])
        halos(slot, lambda copy: copy.start())

    targets = {(4, 0): (2, 1), (4, 1): (2, 0), (4, 2): (1, 3), (4, 3): (0, 1, 2)}
    orders = {
        (4, 0): ("w1", "w3", "o", "w2", "x1", "x2", "s1", "x3", "s2", "s3"),
        (4, 1): ("w3", "x0", "a2", "x2", "w0", "s0", "o", "x3", "b2", "s2", "s3"),
        (4, 2): ("w0", "x0", "a1", "x1", "o", "s0", "s1", "b1", "x3", "s3"),
        (4, 3): ("w0", "o", "x2", "w1", "x0", "x1", "s2", "s0", "s1"),
    }

    def take(slot, at):
        to = relay_to(slot, at)
        for p in range(row_parts):
            team_copy(slot, at, p).wait_recv()
            if to is not None:
                team_relay(slot, to, p).start()
            hold(slot, p)
        core_gather(slot, k_own, c_own).start()

    def settle(slot):
        pass_on(slot)
        ready(slot)

    def plan(at):
        others = [j for j in range(team) if j != at]
        for to in targets.get((team, at), others):
            for p in range(row_parts):
                team_copy(at, to, p).start()
        for p in range(row_parts):
            hold(at, p)
        core_gather(at, k_own, c_own).start()

        @pl.loop(1, lines)
        def _(distance):
            near(distance, send_later)

        default = ["o"] + [kind + str(j) for kind in "wxs" for j in others]
        for step in orders.get((team, at), default):
            if step == "o":
                settle(at)
            elif step[0] in "wab":
                forward(base + int(step[1]), {"w": (0, 1), "a": (0,), "b": (1,)}[step[0]])
            elif step[0] == "x":
                take(int(step[1]), at)
            else:
                settle(int(step[1]))

    def at_own(act):
        for at in range(team):

            @pl.when(g == at)
            def _():
                act(at)

    at_own(plan)

    if lines > team:

        @pl.loop(0, lines - team)
        def _(i):
            forward(jnp.where(i < base, i, i + team))

    def w_lines(skip):
        return w.at[:, pl.ds(0, lines * w_rows), pl.ds(skip, piece - skip)]

    by_width(z, lambda skip: came_all(w_lines(skip), wx_recv.at[0]))

    down_load.wait()
    halves, half = pair_out.shape[1], pair_out.shape[4]
    chunk = 512 if half % 512 == 0 else half

    turns = {4: ((2, 3, 1, 0), (2, 3, 0, 1), (0, 1, 3, 2), (0, 1, 2, 3))}

    def slot_of(n):
        if team not in turns:
            return lax.rem(g + 1 + n, team)
        slot = turns[team][0][n]
        for at in range(1, team):
            slot = jnp.where(g == at, turns[team][at][n], slot)
        return slot

    def part_rows(k):
        return pl.ds(pl.multiple_of(k * part, 16), part)

    def pair_copy(n, h):
        return remote(
            pair_out.at[n, h, 1 - c_own],
            pair_in.at[n, h],
            pair_send.at[0],
            pair_recv.at[n, h],
            s,
            t + 1 - 2 * c_own,
        )

    def y_copy(n, h, k, source):
        return remote(
            y_out.at[n, h, k],
            y_in.at[n, h, source],
            y_send.at[0],
            y_recv.at[n, h, lax.rem(source - k + pairs - 1 + pairs, pairs)],
            s,
            2 * k + c_own,
        )

    def z_copy(n, h, kind, to):
        return remote(
            z_out.at[n, h], z_in.at[kind, h], z_send.at[0], z_recv.at[kind, h], member(to), t
        )

    def front(n):
        slot = slot_of(n)

        block = member(slot)
        halo_rows = pl.ds(pl.multiple_of(slot * slot_rows, 16), halo)

        @pl.when(block == 0)
        def _():
            ffn[halo_rows, :] = jnp.zeros((halo, width), bf16)

        @pl.when(block > 0)
        def _():
            halo_copy(slot, slot, mate).wait_recv()

        rows_at = pl.ds(pl.multiple_of(slot * slot_rows, 16), slot_rows)
        for c in range(2):
            acc[c] = jnp.dot(ffn[rows_at, :], w[c], preferred_element_type=f32)
        for i in range(piece // 128):
            at = slice(i * 128, (i + 1) * 128)
            tap_at = pl.ds(pl.multiple_of(columns(z) + i * 128, 128), 128)
            made = []
            for c, tap in enumerate((gate_taps, up_taps)):
                total = None
                for k in range(taps):
                    first = halo - taps + 1 + k
                    row = acc[c, first : first + rows, at].astype(bf16).astype(f32)
                    term = tap[pl.ds(k, 1), tap_at] * row
                    total = term if total is None else total + term
                made.append(total)
            value = made[0] / (1 + jnp.exp(-made[0])) * made[1]
            if (i + 1) * 128 <= piece - fresh:
                value = jnp.where(g < team - 1, value, 0.0)
            hidden[:, at] = value.astype(bf16)

    def back(n):
        for h in range(halves):
            for i in range(half // chunk):
                at = slice(i * chunk, (i + 1) * chunk)
                down_at = slice(h * half + i * chunk, h * half + (i + 1) * chunk)
                product = jnp.dot(
                    hidden[...], down[:, down_at], preferred_element_type=f32
                ).astype(bf16)
                for r in range(tp_count):
                    first = (r // 2) * part
                    pair_out[n, h, r % 2, first : first + part, at] = product[
                        r * part : (r + 1) * part
                    ]
            pair_copy(n, h).start()

    def pair_sum(n, h, k):
        mine = pair_out[n, h, c_own, part_rows(k), :].astype(f32)
        return mine + pair_in[n, h, part_rows(k), :].astype(f32)

    def across(n):
        for h in range(halves):
            pair_copy(n, h).wait_recv()
            for i in range(1, pairs):
                k = lax.rem(k_own + i, pairs)
                y_out[n, h, k] = pair_sum(n, h, k).astype(bf16)
                y_copy(n, h, k, k_own).start()

    far = 2 if team == 4 else 0
    near_slot = g + 1 - 2 * lax.rem(g, 2)
    inner = (g == 1) | (g == 2)

    def along(n, h, merging):
        at = slice(h * half, (h + 1) * half)
        total = pair_sum(n, h, k_own)
        for i in range(1, pairs):
            k = lax.rem(k_own + i, pairs)
            y_copy(n, h, k_own, k).wait_recv()
            total = total + y_in[n, h, k].astype(f32)
        if n < far and merging:
            z_copy(n, h, 2 + n, near_slot).wait_recv()
            z_out[n, h] = (total + z_in[2 + n, h].astype(f32)).astype(bf16)
            z_copy(n, h, 1, slot_of(n)).start()
        elif n < far:
            z_out[n, h] = total.astype(bf16)
            z_copy(n, h, 2 + n, near_slot).start()
        elif n < team - 1:
            z_out[n, h] = total.astype(bf16)
            z_copy(n, h, 0, near_slot).start()
        else:
            stream[:, at] += total

    for n in range(team + 1):
        if n < team:
            front(n)
        if n > 0:
            across(n - 1)
        if far and n == team - 1:

            @pl.when(jnp.logical_not(inner))
            def _():
                for h in range(halves):
                    along(0, h, False)

        if n < team:
            back(n)
    @pl.when((lax.rem(z, 2) == 0) & (z + 2 < lines))
    def _():
        sent_all(kv_rows(s), kvz_send.at[z + 2])

    @pl.when(z + 1 < lines)
    def _():
        sent_all(kv_rows(s), kvz_send.at[z + 1])

    @pl.loop(0, z)
    def _(line):
        @pl.when(relays(line))
        def _():
            sent_all(kv_rows(s), relay_send.at[line])

    @pl.loop(0, z + 1)
    def _(line):
        sent_all(kv_rows(s), kvx_send.at[line])

    @pl.loop(1, lines)
    def _(i):
        to = lax.rem(z + i, lines)

        def act(skip):
            at = pl.ds(pl.multiple_of(columns(to) + skip, 128), piece - skip)
            sent_all(w_own.at[:, :, at], wz_send.at[to])

        by_width(to, act)

    by_width(z, lambda skip: sent_all(w_lines(skip), wx_send.at[0]))

    sent_all(part_out.at[pl.ds(0, tp_count - 1)], rs_send.at[0])

    def sent(at):
        for slot in range(team):
            if slot == at:
                continue
            if (team, at) not in targets or slot in targets[team, at]:
                sent_all(some_rows(1), team_send.at[slot])
            to = relay_to(slot, at)
            if to is not None:
                sent_all(some_rows(1), up_send.at[slot])

    at_own(sent)
    for slot in range(team):
        halos(slot, lambda copy: copy.wait_send())
    sent_all(some_rows(team * (pairs - 1)), gy_send.at[0])
    sent_all(some_rows(team * pairs), gc_send.at[0])
    def leave(h):
        at = pl.ds(h * half, half)
        return pltpu.make_async_copy(out.at[:, at], result.at[:, at], local.at[16 + h])

    def finish(merging):
        rest = [(n, h) for n in range(1 if far else 0, team) for h in range(halves)]
        if merging:
            pairwise = [(n, h) for h in range(halves) for n in (1, 2)]
            rest = [(0, h) for h in range(halves)] + pairwise + rest[2 * halves :]
        for n, h in rest:
            along(n, h, merging)

    if far:

        @pl.when(inner)
        def _():
            finish(True)

        @pl.when(jnp.logical_not(inner))
        def _():
            finish(False)

    else:
        finish(False)
    sent_all(pair_in, pair_send.at[0])
    if pairs > 1:
        sent_all(y_in.at[:, :, pl.ds(0, pairs - 1)], y_send.at[0])
    if team > 1:
        sent_all(z_out.at[pl.ds(0, team - 1)], z_send.at[0])
    for h in range(halves):
        at = slice(h * half, (h + 1) * half)
        total = stream[:, at]
        for kind in range(min(2, team - 1) if far else team - 1):
            z_copy(0, h, kind, near_slot).wait_recv()
            total = total + z_in[kind, h].astype(f32)
        out[:, at] = total.astype(bf16)
        leave(h).start()
    for h in range(halves):
        leave(h).wait()


def shards(sp_count, tp_count, *args):
    (q_a, _, _, _, vals, lambdas, head_gain, out_weight, residual, mix_gain, gate, _, _, _, down) = args
    rows = q_a.shape[0]
    width = residual.shape[1]
    w_rows, ff = gate.shape
    part = rows // tp_count
    lines = sp_count // lanes
    team = next(n for n in (4, 2, 1) if lines % n == 0)
    pairs = tp_count // 2
    piece = -(-ff // (team * 128)) * 128
    halves = 4 if width % 512 == 0 else 1
    kv_parts = 2 if rows % 32 == 0 else 1
    w_parts = 2 if w_rows % 32 == 0 else 1
    row_parts = part // 16 if part % 16 == 0 else 1
    half = width // halves
    args = list(args)
    args[6] = head_gain.reshape(1, -1)
    args[9] = mix_gain.reshape(1, -1)
    hbm = pl.BlockSpec(memory_space=pl.ANY)
    smem = pl.BlockSpec(memory_space=pltpu.SMEM)
    dma = pltpu.SemaphoreType.DMA
    in_specs = [hbm] * 5 + [smem] + [hbm] * 9
    return pl.pallas_call(
        functools.partial(layer, sp_count, tp_count, team),
        out_shape=jax.ShapeDtypeStruct((part, width), bf16),
        in_specs=in_specs,
        out_specs=hbm,
        scratch_shapes=[
            pltpu.VMEM((sp_count * rows, 2 * q_a.shape[1] + vals.shape[1]), bf16),
            pltpu.VMEM((2, w_rows, ff), bf16),
            pltpu.VMEM((2, sp_count * w_rows, piece), bf16),
            pltpu.VMEM((piece, width), bf16),
            pltpu.VMEM(out_weight.shape, bf16),
            pltpu.VMEM((part, width), bf16),
            pltpu.VMEM((rows, vals.shape[1]), bf16),
            pltpu.VMEM((tp_count, part, width), bf16),
            pltpu.VMEM((tp_count, part, width), bf16),
            pltpu.VMEM((part, width), f32),
            pltpu.VMEM((team * (halo + rows), width), bf16),
            pltpu.VMEM((2, halo + rows, piece), f32),
            pltpu.VMEM((rows, piece), bf16),
            pltpu.VMEM((team, halves, 2, pairs * part, half), bf16),
            pltpu.VMEM((team, halves, pairs * part, half), bf16),
            pltpu.VMEM((team, halves, pairs, part, half), bf16),
            pltpu.VMEM((team, halves, pairs, part, half), bf16),
            pltpu.VMEM((team, halves, part, half), bf16),
            pltpu.VMEM((4, halves, part, half), bf16),
            pltpu.VMEM(q_a.shape, bf16),
            pltpu.VMEM(q_a.shape, bf16),
            pltpu.VMEM(args[6].shape, f32),
            pltpu.VMEM(args[9].shape, f32),
            pltpu.VMEM(args[12].shape, f32),
            pltpu.VMEM(args[12].shape, f32),
            pltpu.VMEM((part, width), bf16),
            dma((16 + halves,)),
            dma((lines,)),
            dma((lines, kv_parts)),
            dma((lines,)),
            dma((lines,)),
            dma((lines,)),
            dma((lines,)),
            dma((2, lines, w_parts)),
            dma((1,)),
            dma((1,)),
            dma((1,)),
            dma((tp_count,)),
            dma((1,)),
            dma((team, pairs)),
            dma((1,)),
            dma((team,)),
            dma((team,)),
            dma((team,)),
            dma((1,)),
            dma((team, halves)),
            dma((1,)),
            dma((team, halves, max(pairs - 1, 1))),
            dma((1,)),
            dma((4, halves)),
            dma((team,)),
            dma((team, row_parts)),
            dma((team,)),
        ],
        compiler_params=pltpu.CompilerParams(
            collective_id=0, has_side_effects=True, vmem_limit_bytes=60 * 1024 * 1024
        ),
    )(*args)


def solution(mesh):
    in_specs = (
        P("sp", "tp"),
        P("sp", "tp"),
        P("sp", "tp"),
        P("sp", "tp"),
        P("sp", "tp"),
        P("tp"),
        P(),
        P("tp", None),
        P("sp", None),
        P(),
        P("sp", "tp"),
        P("sp", "tp"),
        P(None, "tp"),
        P(None, "tp"),
        P("tp", None),
    )
    body = functools.partial(shards, mesh.shape["sp"], mesh.shape["tp"])
    return jax.shard_map(
        body, mesh=mesh, in_specs=in_specs, out_specs=P(("sp", "tp"), None), check_vma=False
    )
```

```python
import functools

import jax
import jax.numpy as jnp
from jax import lax
from jax.experimental import pallas as pl
from jax.experimental.pallas import tpu as pltpu
from jax.sharding import PartitionSpec as P

norm_eps = 1e-06
far_below = -1e30
halo = 16
lanes = 2
f32 = jnp.float32
bf16 = jnp.bfloat16


def rms_scale(field, gain):
    return field * lax.rsqrt(jnp.mean(field * field, axis=-1, keepdims=True) + norm_eps) * gain


def layer(
    sp_count,
    tp_count,
    team,
    q_a_in,
    k_a,
    q_b_in,
    k_b,
    vals,
    lambdas,
    head_gain_in,
    out_weight,
    residual,
    mix_gain_in,
    gate_weight,
    up_weight,
    gate_taps_in,
    up_taps_in,
    down_weight,
    result,
    kv,
    w_own,
    w,
    down,
    out_w,
    res,
    heads,
    part_out,
    part_in,
    stream,
    ffn,
    acc,
    hidden,
    pair_out,
    pair_in,
    y_out,
    y_in,
    z_out,
    z_in,
    q_a,
    q_b,
    head_gain,
    mix_gain,
    gate_taps,
    up_taps,
    out,
    local,
    kvz_send,
    kvz_recv,
    kvx_send,
    kvx_recv,
    relay_send,
    wz_send,
    wz_recv,
    wx_send,
    wx_recv,
    rs_send,
    rs_recv,
    gy_send,
    gy_recv,
    gc_send,
    gc_recv,
    halo_send,
    halo_recv,
    pair_send,
    pair_recv,
    y_send,
    y_recv,
    z_send,
    z_recv,
    team_send,
    team_recv,
    up_send,
):
    s = lax.axis_index("sp")
    t = lax.axis_index("tp")
    x = lax.rem(s, lanes)
    z = s // lanes
    lines = sp_count // lanes
    mate = z * lanes + (1 - x)
    rows = q_a.shape[0]
    key_width = q_a.shape[1]
    value_width = vals.shape[1]
    head_count = lambdas.shape[0]
    head_dim = key_width // head_count
    value_dim = value_width // head_count
    part = rows // tp_count
    width = out.shape[1]
    w_rows = gate_weight.shape[0]
    w_parts = wz_recv.shape[2]
    w_piece = w_rows // w_parts
    ff = gate_weight.shape[1]
    taps = gate_taps.shape[0]
    piece = w.shape[2]
    fresh = ff - (team - 1) * piece
    g = lax.rem(z, team)
    base = z - g
    pairs = tp_count // 2
    c_own = lax.rem(t, 2)
    k_own = t // 2
    slot_rows = halo + rows
    kv_parts = kvz_recv.shape[1]
    kv_piece = rows // kv_parts
    row_parts = team_recv.shape[1]
    row_piece = part // row_parts

    def member(slot):
        return (base + slot) * lanes + x

    def columns(line):
        return pl.multiple_of(jnp.minimum(lax.rem(line, team) * piece, ff - piece), 128)

    def by_width(line, act):
        if fresh == piece:
            act(0)
        else:
            last = lax.rem(line, team) == team - 1

            @pl.when(last)
            def _():
                act(piece - fresh)

            @pl.when(jnp.logical_not(last))
            def _():
                act(0)

    def remote(src, dst, send, recv, sp, tp):
        return pltpu.make_async_remote_copy(
            src_ref=src,
            dst_ref=dst,
            send_sem=send,
            recv_sem=recv,
            device_id=(sp, tp),
            device_id_type=pl.DeviceIdType.MESH,
        )

    def sent_all(block, sem):
        remote(block, block, sem, sem, s, t).wait_send()

    def came_all(block, sem):
        remote(block, block, sem, sem, s, t).wait_recv()

    def kv_rows(block):
        return kv.at[pl.ds(pl.multiple_of(block * rows, 16), rows)]

    def kv_block(block, p):
        return kv.at[pl.ds(pl.multiple_of(block * rows + p * kv_piece, 16), kv_piece)]

    def w_block(c, block):
        return w.at[c, pl.ds(pl.multiple_of(block * w_rows, 16), w_rows)]

    def w_part(c, block, skip, p):
        at = pl.ds(pl.multiple_of(block * w_rows + p * w_piece, 16), w_piece)
        return w.at[c, at, pl.ds(skip, piece - skip)]

    barrier = pltpu.get_barrier_semaphore()

    @pl.loop(1, sp_count)
    def _(i):
        pl.semaphore_signal(
            barrier,
            inc=1,
            device_id=(lax.rem(s + i, sp_count), t),
            device_id_type=pl.DeviceIdType.MESH,
        )

    @pl.loop(1, tp_count)
    def _(i):
        pl.semaphore_signal(
            barrier,
            inc=1,
            device_id=(s, lax.rem(t + i, tp_count)),
            device_id_type=pl.DeviceIdType.MESH,
        )

    @pl.loop(1, team)
    def _(j):
        @pl.loop(1, tp_count)
        def _(i):
            pl.semaphore_signal(
                barrier,
                inc=1,
                device_id=(member(lax.rem(g + j, team)), lax.rem(t + i, tp_count)),
                device_id_type=pl.DeviceIdType.MESH,
            )

    own = pl.ds(pl.multiple_of(s * rows, 16), rows)
    kv_loads = (
        pltpu.make_async_copy(k_a, kv.at[own, pl.ds(0, key_width)], local.at[0]),
        pltpu.make_async_copy(k_b, kv.at[own, pl.ds(key_width, key_width)], local.at[1]),
        pltpu.make_async_copy(vals, kv.at[own, pl.ds(2 * key_width, value_width)], local.at[2]),
    )
    w_loads = (
        pltpu.make_async_copy(gate_weight, w_own.at[0], local.at[3]),
        pltpu.make_async_copy(up_weight, w_own.at[1], local.at[4]),
        pltpu.make_async_copy(gate_weight.at[:, pl.ds(columns(z), piece)], w_block(0, s), local.at[8]),
        pltpu.make_async_copy(up_weight.at[:, pl.ds(columns(z), piece)], w_block(1, s), local.at[9]),
    )
    out_load = pltpu.make_async_copy(out_weight, out_w, local.at[5])
    res_load = pltpu.make_async_copy(
        residual.at[pl.ds(pl.multiple_of(t * part, 16), part)], res, local.at[6]
    )
    down_load = pltpu.make_async_copy(down_weight.at[pl.ds(columns(z), piece)], down, local.at[7])
    small_loads = (
        pltpu.make_async_copy(q_a_in, q_a, local.at[10]),
        pltpu.make_async_copy(q_b_in, q_b, local.at[11]),
        pltpu.make_async_copy(head_gain_in, head_gain, local.at[12]),
        pltpu.make_async_copy(mix_gain_in, mix_gain, local.at[13]),
        pltpu.make_async_copy(gate_taps_in, gate_taps, local.at[14]),
        pltpu.make_async_copy(up_taps_in, up_taps, local.at[15]),
    )
    for load in kv_loads + w_loads + small_loads + (out_load, res_load, down_load):
        load.start()

    pl.semaphore_wait(barrier, sp_count - 1 + team * (tp_count - 1))

    def kvz(line, to, p):
        block = kv_block(line * lanes + x, p)
        return remote(
            block, block, kvz_send.at[to], kvz_recv.at[line, p], to * lanes + x, t
        )

    def kv_relay(line, p):
        block = kv_block(line * lanes + x, p)
        return remote(
            block, block, relay_send.at[line], kvz_recv.at[line, p], (z + 1) * lanes + x, t
        )

    def relays(line):
        direct = (line == z - 1) & (lax.rem(line, 2) == 0)
        return (z + 1 < lines) & jnp.logical_not(direct)

    def kvx(line, lane, p):
        block = kv_block(line * lanes + lane, p)
        return remote(block, block, kvx_send.at[line], kvx_recv.at[line], mate, t)

    def wz(c, line, to, skip, p):
        at = pl.ds(pl.multiple_of(columns(to) + skip, 128), piece - skip)
        return remote(
            w_own.at[c, pl.ds(p * w_piece, w_piece), at],
            w_part(c, line * lanes + x, skip, p),
            wz_send.at[to],
            wz_recv.at[c, line, p],
            to * lanes + x,
            t,
        )

    def wx(c, line, lane, skip, p):
        block = w_part(c, line * lanes + lane, skip, p)
        return remote(block, block, wx_send.at[0], wx_recv.at[0], mate, t)

    for load in kv_loads:
        load.wait()

    @pl.when((lax.rem(z, 2) == 0) & (z + 2 < lines))
    def _():
        for p in range(kv_parts):
            kvz(z, z + 2, p).start()

    @pl.when(z + 1 < lines)
    def _():
        for p in range(kv_parts):
            kvz(z, z + 1, p).start()

    for p in range(kv_parts):
        kvx(z, x, p).start()
    for load in w_loads:
        load.wait()

    def near(distance, act):
        for line, there in ((z + distance, z + distance < lines), (z - distance, z >= distance)):

            @pl.when(there)
            def _():
                act(line)

    def deferred(to, c):
        step = to - z
        slot = lax.rem(to, team)
        up = (slot == team // 2) & ((step == 2) | ((step == 1) & (c == 0)))
        up = up | (slot == team - 1)
        down = (step != -1) | (slot != team // 2 - 1) | (c == 0)
        return jnp.logical_not(jnp.where(step > 0, up, down))

    def send_weights(to, later):
        def act(skip):
            for c in range(2):

                @pl.when(deferred(to, c) == later)
                def _():
                    for p in range(w_parts):
                        wz(c, z, to, skip, p).start()

        by_width(to, act)

    def send_first(to):
        send_weights(to, False)

    def send_later(to):
        send_weights(to, True)

    for distance in (3, 1, 2):

        @pl.when(z >= distance)
        def _():
            send_first(z - distance)

    @pl.loop(1, lines)
    def _(distance):
        @pl.when(z + distance < lines)
        def _():
            send_first(z + distance)

        @pl.when((distance > 3) & (z >= distance))
        def _():
            send_first(z - distance)


    for load in small_loads:
        load.wait()
    scale = head_dim**-0.5
    column = lax.broadcasted_iota(jnp.int32, (rows, key_width), 1) // head_dim
    queries = [
        jnp.where(column == h, q[...], jnp.zeros((), bf16))
        for q in (q_a, q_b)
        for h in range(head_count)
    ]
    span = lanes * rows
    query_pos = s * rows + lax.broadcasted_iota(jnp.int32, (rows, span), 0)
    key_step = lax.broadcasted_iota(jnp.int32, (rows, span), 1)

    hurry = (z >= 2) & (z + 1 < lines)

    def take_keys(line):
        for p in range(kv_parts):
            kvz(line, mate // lanes, p).wait_recv()

            @pl.when(relays(line))
            def _():
                kv_relay(line, p).start()

            kvx(line, x, p).start()

    @pl.when(hurry)
    def _():
        take_keys(z - 1)
        take_keys(z - 2)

    def attend(i, state):
        line = z - i

        @pl.when((i < z) & ((i > 1) | jnp.logical_not(hurry)))
        def _():
            take_keys(line - 1)


        @pl.when(i == jnp.maximum(z - 1, 0))
        def _():
            def act(skip):
                for c in range(2):
                    for p in range(w_parts):
                        wx(c, z, x, skip, p).start()

            by_width(z, act)

        came_all(kv_rows(line * lanes + 1 - x), kvx_recv.at[line])
        keys_at = pl.ds(pl.multiple_of(line * span, 16), span)
        visible = line * span + key_step <= query_pos
        following = []
        for m in range(2):
            keys = kv[keys_at, pl.ds(m * key_width, key_width)]
            for h in range(head_count):
                peak, total, sums = state[m * head_count + h]
                value = kv[keys_at, pl.ds(2 * key_width + h * value_dim, value_dim)]
                scores = (
                    lax.dot_general(
                        queries[m * head_count + h],
                        keys,
                        (((1,), (1,)), ((), ())),
                        preferred_element_type=f32,
                    )
                    * scale
                )
                scores = jnp.where(visible, scores, far_below)
                new_peak = jnp.maximum(peak, jnp.max(scores, axis=-1, keepdims=True))
                fade = jnp.exp(peak - new_peak)
                expo = jnp.exp(scores - new_peak)
                total = total * fade + jnp.sum(expo, axis=-1, keepdims=True)
                sums = sums * fade + jnp.dot(expo.astype(bf16), value, preferred_element_type=f32)
                following.append((new_peak, total, sums))
        return tuple(following)

    start = tuple(
        (
            jnp.full((rows, 1), far_below, f32),
            jnp.zeros((rows, 1), f32),
            jnp.zeros((rows, value_dim), f32),
        )
        for _ in range(2 * head_count)
    )
    state = lax.fori_loop(0, z + 1, attend, start)
    for h in range(head_count):
        _, total_a, sums_a = state[h]
        _, total_b, sums_b = state[head_count + h]
        diff = sums_a / total_a - lambdas[h] * (sums_b / total_b)
        heads[:, h * value_dim : (h + 1) * value_dim] = rms_scale(diff, head_gain[...]).astype(bf16)

    def forward(line, parts=(0, 1)):
        def act(skip):
            for c in parts:
                for p in range(w_parts):
                    wz(c, line, mate // lanes, skip, p).wait_recv()
                    wx(c, line, x, skip, p).start()

        by_width(z, act)

    if team == 4:

        @pl.when(g == 2)
        def _():
            forward(z + 1)

        @pl.when(g == 3)
        def _():
            forward(z - 1)

    out_load.wait()
    res_load.wait()
    stream[...] = res[...].astype(f32)

    def part_copy(to):
        return remote(part_out.at[to], part_in.at[t], rs_send.at[0], rs_recv.at[t], s, to)

    def spread():
        ranks = [2 * lax.rem(k_own + i, pairs) + c for i in range(1, pairs) for c in range(2)]
        return ranks + [t + 1 - 2 * c_own]

    def project_part(to):
        at = pl.ds(pl.multiple_of(to * part, 16), part)
        return jnp.dot(heads[at, :], out_w[...], preferred_element_type=f32)

    for to in spread():
        part_out[to] = project_part(to).astype(bf16)
        part_copy(to).start()
    stream[...] += project_part(t)
    for source in reversed(spread()):
        remote(
            part_out.at[source], part_in.at[source], rs_send.at[0], rs_recv.at[source], s, source
        ).wait_recv()
        stream[...] += part_in[source].astype(f32)

    def ffn_rows(slot, rank):
        return pl.ds(pl.multiple_of(slot * slot_rows + halo + rank * part, 16), part)

    ffn[ffn_rows(g, t), :] = rms_scale(stream[...], mix_gain[...]).astype(bf16)

    def row_block(slot, rank, p):
        first = slot * slot_rows + halo + rank * part + p * row_piece
        return ffn.at[pl.ds(pl.multiple_of(first, 16), row_piece)]

    def team_copy(slot, to, p):
        block = row_block(slot, t, p)
        return remote(block, block, team_send.at[to], team_recv.at[slot, p], member(to), t)

    def direct(source, to):
        if team < 4:
            return True
        if source < to:
            return to - source == 1 or (to - source == 2 and source % 2 == 0)
        return (source, to) != (2, 0)

    def relay_to(source, at):
        if at > source and at + 1 < team and not direct(source, at + 1):
            return at + 1
        if at < source and at > 0 and not direct(source, at - 1):
            return at - 1
        return None

    def team_relay(slot, to, p):
        block = row_block(slot, t, p)
        return remote(block, block, up_send.at[slot], team_recv.at[slot, p], member(to), t)

    def y_gather(slot, k, source, p):
        block = row_block(slot, 2 * source + c_own, p)
        return remote(
            block, block, gy_send.at[0], gy_recv.at[slot, source], s, 2 * k + c_own
        )

    def core_gather(slot, k, c):
        rows_here = ffn.at[ffn_rows(slot, 2 * k + c)]
        return remote(
            rows_here, rows_here, gc_send.at[0], gc_recv.at[slot], s, t + 1 - 2 * c_own
        )

    def some_rows(count):
        return ffn.at[pl.ds(0, count * part)]

    def hold(slot, p):
        for i in range(1, pairs):
            y_gather(slot, lax.rem(k_own + i, pairs), k_own, p).start()

    def halo_copy(slot, to_slot, to):
        return remote(
            ffn.at[pl.ds(pl.multiple_of(slot * slot_rows + rows, 16), halo)],
            ffn.at[pl.ds(pl.multiple_of(to_slot * slot_rows, 16), halo)],
            halo_send.at[slot],
            halo_recv.at[to_slot],
            to,
            t,
        )

    def halos(slot, act):
        @pl.when(x < lanes - 1)
        def _():
            act(halo_copy(slot, slot, mate))

        @pl.when((x == lanes - 1) & (slot < team - 1))
        def _():
            act(halo_copy(slot, slot + 1, mate))

        @pl.when((x == lanes - 1) & (slot == team - 1) & (z + team < lines))
        def _():
            act(halo_copy(slot, 0, (z + team) * lanes))

    def pass_on(slot):
        for i in range(1, pairs):
            k = lax.rem(k_own + i, pairs)
            came_all(ffn.at[ffn_rows(slot, 2 * k + c_own)], gy_recv.at[slot, k])
            core_gather(slot, k, c_own).start()

    def ready(slot):
        came_all(some_rows(pairs), gc_recv.at[slot])
        halos(slot, lambda copy: copy.start())

    targets = {(4, 0): (2, 1), (4, 1): (2, 0), (4, 2): (1, 3), (4, 3): (0, 1, 2)}
    orders = {
        (4, 0): ("w1", "w3", "o", "w2", "x1", "x2", "s1", "x3", "s2", "s3"),
        (4, 1): ("w3", "x0", "a2", "x2", "w0", "s0", "o", "x3", "b2", "s2", "s3"),
        (4, 2): ("w0", "x0", "a1", "x1", "o", "s0", "s1", "b1", "x3", "s3"),
        (4, 3): ("w0", "o", "x2", "w1", "x0", "x1", "s2", "s0", "s1"),
    }

    def take(slot, at):
        to = relay_to(slot, at)
        for p in range(row_parts):
            team_copy(slot, at, p).wait_recv()
            if to is not None:
                team_relay(slot, to, p).start()
            hold(slot, p)
        core_gather(slot, k_own, c_own).start()

    def settle(slot):
        pass_on(slot)
        ready(slot)

    def plan(at):
        others = [j for j in range(team) if j != at]
        for to in targets.get((team, at), others):
            for p in range(row_parts):
                team_copy(at, to, p).start()
        for p in range(row_parts):
            hold(at, p)
        core_gather(at, k_own, c_own).start()

        @pl.loop(1, lines)
        def _(distance):
            near(distance, send_later)

        default = ["o"] + [kind + str(j) for kind in "wxs" for j in others]
        for step in orders.get((team, at), default):
            if step == "o":
                settle(at)
            elif step[0] in "wab":
                forward(base + int(step[1]), {"w": (0, 1), "a": (0,), "b": (1,)}[step[0]])
            elif step[0] == "x":
                take(int(step[1]), at)
            else:
                settle(int(step[1]))

    def at_own(act):
        for at in range(team):

            @pl.when(g == at)
            def _():
                act(at)

    at_own(plan)

    if lines > team:

        @pl.loop(0, lines - team)
        def _(i):
            forward(jnp.where(i < base, i, i + team))

    def w_lines(skip):
        return w.at[:, pl.ds(0, lines * w_rows), pl.ds(skip, piece - skip)]

    by_width(z, lambda skip: came_all(w_lines(skip), wx_recv.at[0]))

    down_load.wait()
    halves, half = pair_out.shape[1], pair_out.shape[4]
    chunk = 512 if half % 512 == 0 else half

    turns = {4: ((2, 3, 1, 0), (0, 2, 3, 1), (3, 0, 1, 2), (0, 1, 2, 3))}

    def slot_of(n):
        if team not in turns:
            return lax.rem(g + 1 + n, team)
        slot = turns[team][0][n]
        for at in range(1, team):
            slot = jnp.where(g == at, turns[team][at][n], slot)
        return slot

    def part_rows(k):
        return pl.ds(pl.multiple_of(k * part, 16), part)

    def pair_copy(n, h):
        return remote(
            pair_out.at[n, h, 1 - c_own],
            pair_in.at[n, h],
            pair_send.at[0],
            pair_recv.at[n, h],
            s,
            t + 1 - 2 * c_own,
        )

    def y_copy(n, h, k, source):
        return remote(
            y_out.at[n, h, k],
            y_in.at[n, h, source],
            y_send.at[0],
            y_recv.at[n, h, lax.rem(source - k + pairs - 1 + pairs, pairs)],
            s,
            2 * k + c_own,
        )

    def z_copy(n, h, kind, to):
        return remote(
            z_out.at[n, h], z_in.at[kind, h], z_send.at[0], z_recv.at[kind, h], member(to), t
        )

    def front(n):
        slot = slot_of(n)

        block = member(slot)
        halo_rows = pl.ds(pl.multiple_of(slot * slot_rows, 16), halo)

        @pl.when(block == 0)
        def _():
            ffn[halo_rows, :] = jnp.zeros((halo, width), bf16)

        @pl.when(block > 0)
        def _():
            halo_copy(slot, slot, mate).wait_recv()

        rows_at = pl.ds(pl.multiple_of(slot * slot_rows, 16), slot_rows)
        for c in range(2):
            acc[c] = jnp.dot(ffn[rows_at, :], w[c], preferred_element_type=f32)
        for i in range(piece // 128):
            at = slice(i * 128, (i + 1) * 128)
            tap_at = pl.ds(pl.multiple_of(columns(z) + i * 128, 128), 128)
            made = []
            for c, tap in enumerate((gate_taps, up_taps)):
                total = None
                for k in range(taps):
                    first = halo - taps + 1 + k
                    row = acc[c, first : first + rows, at].astype(bf16).astype(f32)
                    term = tap[pl.ds(k, 1), tap_at] * row
                    total = term if total is None else total + term
                made.append(total)
            value = made[0] / (1 + jnp.exp(-made[0])) * made[1]
            if (i + 1) * 128 <= piece - fresh:
                value = jnp.where(g < team - 1, value, 0.0)
            hidden[:, at] = value.astype(bf16)

    def back(n):
        for h in range(halves):
            for i in range(half // chunk):
                at = slice(i * chunk, (i + 1) * chunk)
                down_at = slice(h * half + i * chunk, h * half + (i + 1) * chunk)
                product = jnp.dot(
                    hidden[...], down[:, down_at], preferred_element_type=f32
                ).astype(bf16)
                for r in range(tp_count):
                    first = (r // 2) * part
                    pair_out[n, h, r % 2, first : first + part, at] = product[
                        r * part : (r + 1) * part
                    ]
            pair_copy(n, h).start()

    def pair_sum(n, h, k):
        mine = pair_out[n, h, c_own, part_rows(k), :].astype(f32)
        return mine + pair_in[n, h, part_rows(k), :].astype(f32)

    def across(n):
        for h in range(halves):
            pair_copy(n, h).wait_recv()
            for i in range(1, pairs):
                k = lax.rem(k_own + i, pairs)
                y_out[n, h, k] = pair_sum(n, h, k).astype(bf16)
                y_copy(n, h, k, k_own).start()

    far = 2 if team == 4 else 0
    near_slot = g + 1 - 2 * lax.rem(g, 2)
    inner = (g == 1) | (g == 2)

    def along(n, h, merging):
        at = slice(h * half, (h + 1) * half)
        total = pair_sum(n, h, k_own)
        for i in range(1, pairs):
            k = lax.rem(k_own + i, pairs)
            y_copy(n, h, k_own, k).wait_recv()
            total = total + y_in[n, h, k].astype(f32)
        if merging and n in (1, 2):
            z_copy(n, h, 1 + n, near_slot).wait_recv()
            z_out[n, h] = (total + z_in[1 + n, h].astype(f32)).astype(bf16)
            z_copy(n, h, 1, slot_of(n)).start()
        elif n < far and not merging:
            z_out[n, h] = total.astype(bf16)
            z_copy(n, h, 2 + n, near_slot).start()
        elif n < team - 1:
            z_out[n, h] = total.astype(bf16)
            z_copy(n, h, 0, near_slot).start()
        else:
            stream[:, at] += total

    for n in range(team + 1):
        if n < team:
            front(n)
        if n > 0:
            across(n - 1)
        if far and n == team - 1:

            @pl.when(inner)
            def _():
                for h in range(halves):
                    along(0, h, True)

            @pl.when(jnp.logical_not(inner))
            def _():
                for h in range(halves):
                    along(0, h, False)

        if n < team:
            back(n)
    @pl.when((lax.rem(z, 2) == 0) & (z + 2 < lines))
    def _():
        sent_all(kv_rows(s), kvz_send.at[z + 2])

    @pl.when(z + 1 < lines)
    def _():
        sent_all(kv_rows(s), kvz_send.at[z + 1])

    @pl.loop(0, z)
    def _(line):
        @pl.when(relays(line))
        def _():
            sent_all(kv_rows(s), relay_send.at[line])

    @pl.loop(0, z + 1)
    def _(line):
        sent_all(kv_rows(s), kvx_send.at[line])

    @pl.loop(1, lines)
    def _(i):
        to = lax.rem(z + i, lines)

        def act(skip):
            at = pl.ds(pl.multiple_of(columns(to) + skip, 128), piece - skip)
            sent_all(w_own.at[:, :, at], wz_send.at[to])

        by_width(to, act)

    by_width(z, lambda skip: sent_all(w_lines(skip), wx_send.at[0]))

    sent_all(part_out.at[pl.ds(0, tp_count - 1)], rs_send.at[0])

    def sent(at):
        for slot in range(team):
            if slot == at:
                continue
            if (team, at) not in targets or slot in targets[team, at]:
                sent_all(some_rows(1), team_send.at[slot])
            to = relay_to(slot, at)
            if to is not None:
                sent_all(some_rows(1), up_send.at[slot])

    at_own(sent)
    for slot in range(team):
        halos(slot, lambda copy: copy.wait_send())
    sent_all(some_rows(team * (pairs - 1)), gy_send.at[0])
    sent_all(some_rows(team * pairs), gc_send.at[0])
    def leave(h):
        at = pl.ds(h * half, half)
        return pltpu.make_async_copy(out.at[:, at], result.at[:, at], local.at[16 + h])

    def finish(merging):
        rest = [(n, h) for n in range(1 if far else 0, team) for h in range(halves)]
        for n, h in rest:
            along(n, h, merging)

    if far:

        @pl.when(inner)
        def _():
            finish(True)

        @pl.when(jnp.logical_not(inner))
        def _():
            finish(False)

    else:
        finish(False)
    sent_all(pair_in, pair_send.at[0])
    if pairs > 1:
        sent_all(y_in.at[:, :, pl.ds(0, pairs - 1)], y_send.at[0])
    if team > 1:
        sent_all(z_out.at[pl.ds(0, team - 1)], z_send.at[0])
    for h in range(halves):
        at = slice(h * half, (h + 1) * half)
        total = stream[:, at]
        for kind in range(min(2, team - 1) if far else team - 1):
            z_copy(0, h, kind, near_slot).wait_recv()
            total = total + z_in[kind, h].astype(f32)
        out[:, at] = total.astype(bf16)
        leave(h).start()
    for h in range(halves):
        leave(h).wait()


def shards(sp_count, tp_count, *args):
    (q_a, _, _, _, vals, lambdas, head_gain, out_weight, residual, mix_gain, gate, _, _, _, down) = args
    rows = q_a.shape[0]
    width = residual.shape[1]
    w_rows, ff = gate.shape
    part = rows // tp_count
    lines = sp_count // lanes
    team = next(n for n in (4, 2, 1) if lines % n == 0)
    pairs = tp_count // 2
    piece = -(-ff // (team * 128)) * 128
    halves = 4 if width % 512 == 0 else 1
    kv_parts = 2 if rows % 32 == 0 else 1
    w_parts = 2 if w_rows % 32 == 0 else 1
    row_parts = part // 16 if part % 16 == 0 else 1
    half = width // halves
    args = list(args)
    args[6] = head_gain.reshape(1, -1)
    args[9] = mix_gain.reshape(1, -1)
    hbm = pl.BlockSpec(memory_space=pl.ANY)
    smem = pl.BlockSpec(memory_space=pltpu.SMEM)
    dma = pltpu.SemaphoreType.DMA
    in_specs = [hbm] * 5 + [smem] + [hbm] * 9
    return pl.pallas_call(
        functools.partial(layer, sp_count, tp_count, team),
        out_shape=jax.ShapeDtypeStruct((part, width), bf16),
        in_specs=in_specs,
        out_specs=hbm,
        scratch_shapes=[
            pltpu.VMEM((sp_count * rows, 2 * q_a.shape[1] + vals.shape[1]), bf16),
            pltpu.VMEM((2, w_rows, ff), bf16),
            pltpu.VMEM((2, sp_count * w_rows, piece), bf16),
            pltpu.VMEM((piece, width), bf16),
            pltpu.VMEM(out_weight.shape, bf16),
            pltpu.VMEM((part, width), bf16),
            pltpu.VMEM((rows, vals.shape[1]), bf16),
            pltpu.VMEM((tp_count, part, width), bf16),
            pltpu.VMEM((tp_count, part, width), bf16),
            pltpu.VMEM((part, width), f32),
            pltpu.VMEM((team * (halo + rows), width), bf16),
            pltpu.VMEM((2, halo + rows, piece), f32),
            pltpu.VMEM((rows, piece), bf16),
            pltpu.VMEM((team, halves, 2, pairs * part, half), bf16),
            pltpu.VMEM((team, halves, pairs * part, half), bf16),
            pltpu.VMEM((team, halves, pairs, part, half), bf16),
            pltpu.VMEM((team, halves, pairs, part, half), bf16),
            pltpu.VMEM((team, halves, part, half), bf16),
            pltpu.VMEM((4, halves, part, half), bf16),
            pltpu.VMEM(q_a.shape, bf16),
            pltpu.VMEM(q_a.shape, bf16),
            pltpu.VMEM(args[6].shape, f32),
            pltpu.VMEM(args[9].shape, f32),
            pltpu.VMEM(args[12].shape, f32),
            pltpu.VMEM(args[12].shape, f32),
            pltpu.VMEM((part, width), bf16),
            dma((16 + halves,)),
            dma((lines,)),
            dma((lines, kv_parts)),
            dma((lines,)),
            dma((lines,)),
            dma((lines,)),
            dma((lines,)),
            dma((2, lines, w_parts)),
            dma((1,)),
            dma((1,)),
            dma((1,)),
            dma((tp_count,)),
            dma((1,)),
            dma((team, pairs)),
            dma((1,)),
            dma((team,)),
            dma((team,)),
            dma((team,)),
            dma((1,)),
            dma((team, halves)),
            dma((1,)),
            dma((team, halves, max(pairs - 1, 1))),
            dma((1,)),
            dma((4, halves)),
            dma((team,)),
            dma((team, row_parts)),
            dma((team,)),
        ],
        compiler_params=pltpu.CompilerParams(
            collective_id=0, has_side_effects=True, vmem_limit_bytes=60 * 1024 * 1024
        ),
    )(*args)


def solution(mesh):
    in_specs = (
        P("sp", "tp"),
        P("sp", "tp"),
        P("sp", "tp"),
        P("sp", "tp"),
        P("sp", "tp"),
        P("tp"),
        P(),
        P("tp", None),
        P("sp", None),
        P(),
        P("sp", "tp"),
        P("sp", "tp"),
        P(None, "tp"),
        P(None, "tp"),
        P("tp", None),
    )
    body = functools.partial(shards, mesh.shape["sp"], mesh.shape["tp"])
    return jax.shard_map(
        body, mesh=mesh, in_specs=in_specs, out_specs=P(("sp", "tp"), None), check_vma=False
    )
```
